512 devices in a mesh: sp: 64 (over z, y), tp: 8 (over x, core).
Axes of the slice: x: 4, y: 4, z: 16, core: 2. Of those that a mesh axis runs over, the one named last changes fastest.
Arguments:
- hidden_in: bfloat16 [16384, 2048], P('sp'), may hold values from -16 to 16
- query_one: bfloat16 [2048, 512], P(None, 'tp'), may hold values from -0.13258252 to 0.13258252
- query_two: bfloat16 [2048, 512], P(None, 'tp'), may hold values from -0.13258252 to 0.13258252
- key_one: bfloat16 [2048, 512], P(None, 'tp'), may hold values from -0.13258252 to 0.13258252
- key_two: bfloat16 [2048, 512], P(None, 'tp'), may hold values from -0.13258252 to 0.13258252
- value_proj: bfloat16 [2048, 1024], P(None, 'tp'), may hold values from -0.125 to 0.125
- lambdas: float32 [8], P('tp'), may hold values from 0.3 to 0.8
- norm_gain: float32 [128], replicated, may hold values from 0.1 to 1.9
- out_proj: bfloat16 [1024, 2048], P('tp'), may hold values from -0.1875 to 0.1875
Outputs:
- attended: bfloat16 [16384, 2048], P('sp')
The draws below stay inside these ranges and needn't reach their ends.
All inputs are finite; a program needn't handle non-finite values.
Results may differ from the reference program's by a relative error of at most 0.015.
Values may be sent and summed in bfloat16 or wider, within the bound.
A program may use at most 64 MiB of HBM per device.

```python
import math
import jax
import jax.numpy as jnp
from jax import lax

D = 2048
HEADS = 8
HEAD_QK = 64
HEAD_V = 128
TOK_DEV = 256
TOKENS = 16384
N_TP = 8


def draw_hidden_in(key, part):
    blocks = TOKENS // TOK_DEV
    noise_key = jax.random.fold_in(key, 101)
    shift_key = jax.random.fold_in(key, 102)
    offsets = 0.6 * jax.random.normal(shift_key, (blocks, 1, D), jnp.float32)
    base = 0.8 * jax.random.normal(noise_key, (blocks, TOK_DEV, D), jnp.float32)
    field = base + offsets
    return jnp.clip(field.reshape(TOKENS, D), -16.0, 16.0).astype(jnp.bfloat16)


def plain_weight(key, salt):
    base = jax.random.normal(jax.random.fold_in(key, salt), (D, HEADS * HEAD_QK), jnp.float32)
    return jnp.clip(base, -6.0, 6.0) * D ** (-0.5)


def draw_query_one(key, part):
    return plain_weight(key, 201).astype(jnp.bfloat16)


def draw_query_two(key, part):
    return plain_weight(key, 301).astype(jnp.bfloat16)


def draw_key_one(key, part):
    return plain_weight(key, 211).astype(jnp.bfloat16)


def draw_key_two(key, part):
    return plain_weight(key, 311).astype(jnp.bfloat16)


def shard_levels(rng, dims, split, least, high):
    loudness = 1.0
    for dim, blocks in split:
        draws = jax.random.uniform(jax.random.fold_in(jax.random.fold_in(rng, 6), dim), (blocks,), jnp.float32, least / len(split), high / len(split))
        loudness = loudness * jnp.repeat(jnp.exp(draws), dims[dim] // blocks).reshape((-1,) + (1,) * (len(dims) - 1 - dim))
    return loudness


def scatter_about(key, dims, spread, bound, split=(), held_as=jnp.bfloat16):
    array = jax.random.normal(key, dims, jnp.float32) * spread
    if len(split) > 0:
        array = shard_levels(key, dims, split, -0.22, 0.18) * array
    return jnp.clip(array, min=-bound, max=bound).astype(held_as)


def setup_inputs(seed: int = 0) -> dict:
    key_list = jax.random.split(jax.random.key(seed), 10)
    hidden_in = draw_hidden_in(jax.random.fold_in(key_list[9], 71), 0)
    query_one = draw_query_one(jax.random.fold_in(key_list[9], 71), 0)
    query_two = draw_query_two(jax.random.fold_in(key_list[9], 71), 0)
    key_one = draw_key_one(jax.random.fold_in(key_list[9], 71), 0)
    key_two = draw_key_two(jax.random.fold_in(key_list[9], 71), 0)
    value_proj = scatter_about(key_list[5], (D, HEADS * HEAD_V), D ** -0.5, 0.125, ((1, 8),))
    lambdas = jnp.clip(0.3 + 0.5 * jax.random.uniform(key_list[6], (HEADS,), jnp.float32) ** shard_levels(key_list[6], (HEADS,), ((0, 8),), -0.2, 0.2), 0.3, 0.8)
    norm_gain = jnp.clip(1.0 + 0.18 * jax.random.normal(key_list[7], (HEAD_V,), jnp.float32), 0.1, 1.9)
    out_proj = scatter_about(key_list[8], (HEADS * HEAD_V, D), (HEADS * HEAD_V) ** -0.5, 0.1875, ((0, 8),))
    return {"hidden_in": hidden_in, "query_one": query_one, "query_two": query_two, "key_one": key_one, "key_two": key_two, "value_proj": value_proj, "lambdas": lambdas, "norm_gain": norm_gain, "out_proj": out_proj}


epsilon = 1e-06
masked_score = -1e+30

def reference(hidden_in, query_one, query_two, key_one, key_two, value_proj, lambdas, norm_gain, out_proj):

    def project(weight, width):
        product = jnp.dot(hidden_in, weight, preferred_element_type=jnp.float32)
        return product.astype(jnp.bfloat16).reshape(TOKENS, HEADS, width)
    query_a = project(query_one, HEAD_QK)
    query_b = project(query_two, HEAD_QK)
    keys_a = project(key_one, HEAD_QK).astype(jnp.float32)
    keys_b = project(key_two, HEAD_QK).astype(jnp.float32)
    value_rows = project(value_proj, HEAD_V).astype(jnp.float32)
    score_scale = 1.75 * HEAD_QK ** (-0.5)
    key_pos = jnp.arange(TOKENS, dtype=jnp.int32)
    query_rows = math.gcd(TOKENS, 512)

    def one_block(block_index):
        begin = block_index * query_rows
        row_pos = begin + jnp.arange(query_rows, dtype=jnp.int32)
        allowed = key_pos[None, :] <= row_pos[:, None]

        def attend(queries, keys):
            chosen = lax.dynamic_slice_in_dim(queries, begin, query_rows, 0).astype(jnp.float32)
            scores = jnp.einsum('qhd,khd->hqk', chosen, keys) * score_scale
            scores = jnp.where(allowed[None], scores, masked_score)
            highest = lax.optimization_barrier(jnp.max(scores, axis=-1, keepdims=True))
            expos = jnp.where(allowed[None], jnp.exp(scores - highest), 0.0)
            summed = lax.optimization_barrier(jnp.sum(expos, axis=-1))
            rounded = lax.optimization_barrier(expos.astype(jnp.bfloat16))
            accum = jnp.einsum('hqk,khe->hqe', rounded.astype(jnp.float32), value_rows)
            return accum / summed[..., None]
        mixed_out = attend(query_a, keys_a) - lambdas[:, None, None] * attend(query_b, keys_b)
        scale_rows = lax.rsqrt(lax.optimization_barrier(jnp.mean(mixed_out * mixed_out, axis=-1, keepdims=True)) + epsilon)
        normed = (mixed_out * scale_rows * norm_gain).astype(jnp.bfloat16)
        return jnp.transpose(normed, (1, 0, 2)).reshape(query_rows, HEADS * HEAD_V)
    normed = lax.map(one_block, jnp.arange(TOKENS // query_rows, dtype=jnp.int32))
    normed = normed.reshape(TOKENS, HEADS * HEAD_V)
    group_cols = HEADS * HEAD_V // N_TP
    summed = jnp.zeros((TOKENS, D), jnp.float32)
    for group_index in range(N_TP):
        lower = group_index * group_cols
        part = jnp.dot(normed[:, lower:lower + group_cols], out_proj[lower:lower + group_cols], preferred_element_type=jnp.float32).astype(jnp.bfloat16)
        part = lax.optimization_barrier(part)
        summed = summed + part.astype(jnp.float32)
    return summed.astype(jnp.bfloat16)
```

```python
import math

import jax
import jax.numpy as jnp
from jax import lax
from jax.experimental import pallas as pl
from jax.experimental.pallas import tpu as pltpu
from jax.sharding import Mesh
from jax.sharding import PartitionSpec as P

SP = ("sp_0", "sp_1")
F32 = jnp.float32
BF16 = jnp.bfloat16
MESH = pl.DeviceIdType.MESH

epsilon = 1e-06
masked_score = -1e30

NZ = 16
NY = 4
NX = 4
HALF = NZ // 2
CHUNKS = 4
FAR = 2


def kernel(
    hidden_hbm, wq1_hbm, wq2_hbm, wk1_hbm, wk2_hbm, wv_hbm, lam_ref, gain_ref, wo_hbm,
    out_hbm,
    hid, wq, wk, wv, load_sem,
    kv, kv_send, kv_recv,
    qbuf, qz, q_send, q_recv,
    m_ref, l_ref, acc_ref,
    opart, stats, orecv, strecv, relay, o_send, o_recv, rel_send, rel_recv, st_send, st_recv,
    wo, wo_send, wo_recv, wo_dsend, wo_drecv,
    nb, nb_send, nb_recv, nb_dsend, nb_drecv,
    out_v, out_sem,
):
    z = lax.axis_index("sp_0")
    y = lax.axis_index("sp_1")
    t = lax.axis_index("tp")
    x = t // 2
    core = t % 2
    rows = hid.shape[0]
    head_qk = wq.shape[1]
    head_v = wv.shape[1]
    half_rows = rows // 2
    scale = 1.75 * head_qk ** (-0.5) * math.log2(math.e)

    z_up, z_down = (z + 1) % NZ, (z + NZ - 1) % NZ
    y_at = [y, (y + 1) % NY, (y + 2) % NY, (y + 3) % NY]
    x_at = [x, (x + 1) % NX, (x + 2) % NX, (x + 3) % NX]
    tp_at = [2 * xx + core for xx in x_at]
    sibling = 2 * x + (1 - core)

    loads = [
        pltpu.make_async_copy(hidden_hbm, hid, load_sem.at[0]),
        pltpu.make_async_copy(wk1_hbm, wk.at[0], load_sem.at[1]),
        pltpu.make_async_copy(wk2_hbm, wk.at[1], load_sem.at[2]),
        pltpu.make_async_copy(wv_hbm, wv, load_sem.at[3]),
        pltpu.make_async_copy(wq1_hbm, wq.at[0], load_sem.at[4]),
        pltpu.make_async_copy(wq2_hbm, wq.at[1], load_sem.at[5]),
        pltpu.make_async_copy(wo_hbm, wo.at[t], load_sem.at[6]),
    ]
    for load in loads:
        load.start()

    barrier = pltpu.get_barrier_semaphore()
    partners = [
        {"sp_0": z_up}, {"sp_0": z_down},
        {"sp_1": y_at[1]}, {"sp_1": y_at[2]}, {"sp_1": y_at[3]},
        {"tp": tp_at[1]}, {"tp": tp_at[3]}, {"tp": sibling},
    ]
    for partner in partners:
        pl.semaphore_signal(barrier, inc=1, device_id=partner, device_id_type=MESH)

    def remote(src, dst, send_sem, recv_sem, device):
        return pltpu.make_async_remote_copy(
            src_ref=src, dst_ref=dst, send_sem=send_sem, recv_sem=recv_sem,
            device_id=device, device_id_type=MESH,
        )

    def project(h, pair):
        both = pair[...].reshape(2 * head_qk, pair.shape[2])
        return lax.dot_general(h, both, (((1,), (1,)), ((), ())), preferred_element_type=F32)

    for load in loads[:4]:
        load.wait()
    h = hid[...]
    k = project(h, wk)
    v = jnp.dot(h, wv[...], preferred_element_type=F32)
    own = jnp.concatenate((k, v), axis=1).astype(BF16)
    kv[z] = own.reshape(kv.shape[1:])

    pl.semaphore_wait(barrier, len(partners))

    def up(step, chunk, slot):
        ref = kv.at[slot, chunk]
        return remote(
            ref, ref, kv_send.at[0, step - 1, chunk], kv_recv.at[0, step - 1, chunk], {"sp_0": z_up}
        )

    def down(step, chunk, slot):
        ref = kv.at[slot, chunk]
        return remote(
            ref, ref, kv_send.at[1, step - 1, chunk], kv_recv.at[1, step - 1, chunk], {"sp_0": z_down}
        )

    for chunk in range(CHUNKS):
        up(1, chunk, z).start()
        down(1, chunk, z).start()

    loads[4].wait()
    loads[5].wait()
    qbuf[y] = project(h, wq).astype(BF16)

    def q_copy(off, slot):
        return remote(
            qbuf.at[slot], qbuf.at[slot], q_send.at[off], q_recv.at[off], {"sp_1": y_at[off]}
        )

    for off in (2, 1, 3):
        q_copy(off, y).start()

    def gather_ops(buf, send, recv, dsend, drecv):
        first = {0: 0, 1: 1}

        def hop(direction, order, slot):
            piece = first[direction] if order != 1 else 1 - first[direction]
            ref = buf.at[slot, piece]
            to = tp_at[1] if direction == 0 else tp_at[3]
            return remote(ref, ref, send.at[direction, order], recv.at[direction, order], {"tp": to})

        def across(index, piece, slot):
            ref = buf.at[slot, piece]
            return remote(ref, ref, dsend.at[index, piece], drecv.at[index, piece], {"tp": sibling})

        def start_own():
            for order in range(2):
                for direction in range(2):
                    hop(direction, order, t).start()
            for piece in range(2):
                across(0, piece, t).start()

        def came(direction):
            return tp_at[3] if direction == 0 else tp_at[1]

        def take(order):
            for direction in range(2):
                slot = tp_at[2] if order == 2 else came(direction)
                arrived = hop(direction, order, slot)
                arrived.wait_recv()
                piece = first[direction] if order != 1 else 1 - first[direction]
                if order == 0:
                    hop(direction, 2, slot).start()
                index = 2 if order == 2 else (3 if direction == 0 else 1)
                across(index, piece, slot).start()

        def take_across():
            for index in range(4):
                slot = 2 * x_at[index] + (1 - core)
                for piece in range(2):
                    across(index, piece, slot).wait_recv()

        def drain():
            for direction in range(2):
                for order in range(3):
                    slot = came(direction) if order == 2 else t
                    hop(direction, order, slot).wait_send()
            for index in range(4):
                for piece in range(2):
                    across(index, piece, tp_at[index]).wait_send()

        return start_own, take, take_across, drain

    wo_start, wo_take, wo_take_across, wo_drain = gather_ops(wo, wo_send, wo_recv, wo_dsend, wo_drecv)
    nb_start, nb_take, nb_take_across, nb_drain = gather_ops(nb, nb_send, nb_recv, nb_dsend, nb_drecv)

    loads[6].wait()
    wo_start()

    for off in (1, 3, 2):
        q_copy(off, y_at[(NY - off) % NY]).wait_recv()
    lane = lax.broadcasted_iota(jnp.int32, (rows, 2 * head_qk), 1)
    in_first = (lane < head_qk).astype(F32)

    def split_queries(block, _):
        q = qbuf[block].astype(F32)
        qz[0, block] = (q * in_first).astype(BF16)
        qz[1, block] = (q * (1.0 - in_first)).astype(BF16)
        return 0

    lax.fori_loop(0, NY, split_queries, 0)

    def block_of(slot):
        whole = kv[slot].reshape(rows, 2 * head_qk + head_v)
        return whole[:, : 2 * head_qk], whole[:, 2 * head_qk :]

    def attend(block, keys, vals, allowed=None):
        for pick in range(2):
            scores = scale * lax.dot_general(
                qz[pick, block], keys, (((1,), (1,)), ((), ())), preferred_element_type=F32
            )
            if allowed is not None:
                scores = jnp.where(allowed, scores, masked_score)
            highest = jnp.max(scores, axis=1, keepdims=True)
            if allowed is None:
                before = m_ref[pick, block]
                now = jnp.maximum(before, highest)
                rescale = jnp.exp2(before - now)
            else:
                now = jnp.broadcast_to(highest, (rows, 128))
            parts = []
            total = None
            for left in range(0, scores.shape[1], 128):
                part = jnp.exp2(scores[:, left : left + 128] - now)
                if allowed is not None:
                    part = jnp.where(allowed[:, left : left + 128], part, 0.0)
                total = part if total is None else total + part
                parts.append(part.astype(BF16))
            added = jnp.dot(jnp.concatenate(parts, axis=1), vals, preferred_element_type=F32)
            m_ref[pick, block] = now
            if allowed is None:
                l_ref[pick, block] = l_ref[pick, block] * rescale + total
                acc_ref[pick, block] = acc_ref[pick, block] * rescale + added
            else:
                l_ref[pick, block] = total
                acc_ref[pick, block] = added

    def pass_on(step, chunk):
        low, high = (z + NZ - step) % NZ, (z + step) % NZ
        up(step, chunk, low).wait_recv()

        @pl.when((step < HALF - 1) | (chunk < CHUNKS // 2))
        def _():
            up(step + 1, chunk, low).start()

        down(step, chunk, high).wait_recv()

        @pl.when((step < HALF - 1) | (chunk >= CHUNKS // 2))
        def _():
            down(step + 1, chunk, high).start()

    def attend_pair(step, block):
        low, high = (z + NZ - step) % NZ, (z + step) % NZ

        @pl.when(z >= NZ - step)
        def _():
            keys_low, vals_low = block_of(low)
            keys_high, vals_high = block_of(high)
            attend(
                block,
                jnp.concatenate((keys_low, keys_high), axis=0),
                jnp.concatenate((vals_low, vals_high), axis=0),
            )

        @pl.when((z >= step) & (z < NZ - step))
        def _():
            attend(block, *block_of(low))

    def first_step(block, _):
        pass_on(1, block)
        q_pos = block * rows + lax.broadcasted_iota(jnp.int32, (rows, rows), 0)
        k_pos = y * rows + lax.broadcasted_iota(jnp.int32, (rows, rows), 1)
        attend(block, *block_of(z), allowed=k_pos <= q_pos)
        return 0

    lax.fori_loop(0, NY, first_step, 0)

    def ring_step(index, _):
        step, block = index // CHUNKS, index % CHUNKS
        pass_on(step, block)

        @pl.when(index == 4 * CHUNKS)
        def _():
            wo_take(0)

        @pl.when(index == 6 * CHUNKS)
        def _():
            wo_take(1)

        attend_pair(step - 1, block)
        return 0

    lax.fori_loop(2 * CHUNKS, HALF * CHUNKS, ring_step, 0)

    def last_pair(block, _):
        attend_pair(HALF - 1, block)
        return 0

    lax.fori_loop(0, NY, last_pair, 0)

    opposite = (z + HALF) % NZ
    for chunk in range(CHUNKS):
        if chunk < CHUNKS // 2:
            up(HALF, chunk, opposite).wait_recv()
        else:
            down(HALF, chunk, opposite).wait_recv()

    def o_copy(direction, piece, slot):
        to = y_at[1] if direction == 0 else y_at[3]
        return remote(
            opart.at[slot, piece], orecv.at[direction, piece],
            o_send.at[direction, piece], o_recv.at[direction, piece], {"sp_1": to},
        )

    def rel_copy(direction, slot):
        to = y_at[1] if direction == 0 else y_at[3]
        return remote(
            opart.at[slot, direction], relay.at[direction],
            rel_send.at[direction, 0], rel_recv.at[direction, 0], {"sp_1": to},
        )

    def rel_forward(direction):
        to = y_at[1] if direction == 0 else y_at[3]
        return remote(
            relay.at[direction], orecv.at[2, direction],
            rel_send.at[direction, 1], rel_recv.at[direction, 1], {"sp_1": to},
        )

    def st_copy(off, slot):
        return remote(
            stats.at[slot], strecv.at[off], st_send.at[off], st_recv.at[off], {"sp_1": y_at[off]}
        )

    lane_128 = lax.broadcasted_iota(jnp.int32, (rows, 128), 1)

    def finish(block):
        @pl.when(z >= HALF)
        def _():
            attend(block, *block_of(opposite))

        table = jnp.zeros((rows, 128), F32)
        for pick in range(2):
            total = jnp.sum(l_ref[pick, block], axis=1, keepdims=True)
            table = jnp.where(lane_128 == 2 * pick, m_ref[pick, block], table)
            table = jnp.where(lane_128 == 2 * pick + 1, total, table)
        stats[block] = table.T[:8]
        packed = jnp.concatenate((acc_ref[0, block], acc_ref[1, block]), axis=1).astype(BF16)
        opart[block] = packed.reshape(opart.shape[1:])

    finish(y_at[2])
    rel_copy(0, y_at[2]).start()
    rel_copy(1, y_at[2]).start()
    st_copy(2, y_at[2]).start()
    finish(y_at[1])
    o_copy(0, 0, y_at[1]).start()
    o_copy(0, 1, y_at[1]).start()
    st_copy(1, y_at[1]).start()
    finish(y_at[3])
    o_copy(1, 0, y_at[3]).start()
    o_copy(1, 1, y_at[3]).start()
    st_copy(3, y_at[3]).start()
    finish(y_at[0])

    wo_take(2)

    for direction in range(2):
        rel_copy(direction, y_at[2]).wait_recv()
        rel_forward(direction).start()

    for off in range(1, NY):
        st_copy(off, y_at[0]).wait_recv()

    lam = lam_ref[0]
    tables = [stats[y], strecv[1], strecv[3], strecv[2]]
    coefs = []
    for pick in range(2):
        maxima = [table[2 * pick : 2 * pick + 1] for table in tables]
        sums = [table[2 * pick + 1 : 2 * pick + 2] for table in tables]
        highest = maxima[0]
        for other in maxima[1:]:
            highest = jnp.maximum(highest, other)
        shares = [jnp.exp2(one - highest) for one in maxima]
        total = shares[0] * sums[0]
        for share, one in zip(shares[1:], sums[1:]):
            total = total + share * one
        factor = (1.0 if pick == 0 else -lam) / total
        coefs.extend(share * factor for share in shares)
    coef_rows = jnp.concatenate(coefs, axis=0)
    coef_cols = jnp.concatenate([coef_rows] * 16, axis=0).T

    gain = gain_ref[...].reshape(1, head_v)
    for piece in range(2):
        o_copy(0, piece, y_at[1]).wait_recv()
        o_copy(1, piece, y_at[3]).wait_recv()
        rel_forward(piece).wait_recv()
        part = slice(piece * half_rows, (piece + 1) * half_rows)
        cols = coef_cols[part]
        arrived = [None] + [orecv[source, piece].astype(F32) for source in (0, 1, 2)]
        mixed = acc_ref[0, y, part] * cols[:, 0:1] + acc_ref[1, y, part] * cols[:, 4:5]
        for source in (1, 2, 3):
            mixed = mixed + arrived[source][:, :head_v] * cols[:, source : source + 1]
            mixed = mixed + arrived[source][:, head_v:] * cols[:, 4 + source : 5 + source]
        spread = lax.rsqrt(jnp.mean(mixed * mixed, axis=1, keepdims=True) + epsilon)
        nb[t, piece] = (mixed * spread * gain).astype(BF16)

    nb_start()
    wo_take_across()
    nb_take(0)
    nb_take(1)
    nb_take(2)
    nb_take_across()

    lhs = jnp.concatenate([nb[head].reshape(rows, head_v) for head in range(2 * NX)], axis=1)
    width = 256
    out_copies = []
    for left in range(0, out_v.shape[1], width):
        rhs = wo[:, :, :, left : left + width].reshape(2 * NX * head_v, width)
        out_v[:, left : left + width] = jnp.dot(lhs, rhs, preferred_element_type=F32).astype(BF16)
        copy = pltpu.make_async_copy(
            out_v.at[:, left : left + width], out_hbm.at[:, left : left + width],
            out_sem.at[left // width],
        )
        copy.start()
        out_copies.append(copy)

    def drain_ring(index, _):
        step, chunk = index // CHUNKS, index % CHUNKS

        @pl.when((step < HALF) | (chunk < CHUNKS // 2))
        def _():
            up(step, chunk, z).wait_send()

        @pl.when((step < HALF) | (chunk >= CHUNKS // 2))
        def _():
            down(step, chunk, z).wait_send()

        return 0

    lax.fori_loop(CHUNKS, (HALF + 1) * CHUNKS, drain_ring, 0)
    for off in range(1, NY):
        q_copy(off, y).wait_send()
        st_copy(off, y).wait_send()
    for direction in range(2):
        for piece in range(2):
            o_copy(direction, piece, y).wait_send()
        rel_copy(direction, y).wait_send()
        rel_forward(direction).wait_send()
    wo_drain()
    nb_drain()
    for copy in out_copies:
        copy.wait()


def shards(
    hidden_in, query_one, query_two, key_one, key_two, value_proj, lambdas, norm_gain, out_proj
):
    rows, depth = hidden_in.shape
    head_qk = query_one.shape[1]
    head_v = value_proj.shape[1]
    wide = 2 * head_qk + head_v
    half = rows // 2
    heads = 2 * NX
    dma = pltpu.SemaphoreType.DMA
    anywhere = pl.BlockSpec(memory_space=pl.ANY)
    scratch = [
        pltpu.VMEM((rows, depth), BF16),
        pltpu.VMEM((2, head_qk, depth), BF16),
        pltpu.VMEM((2, head_qk, depth), BF16),
        pltpu.VMEM((depth, head_v), BF16),
        dma((7,)),
        pltpu.VMEM((NZ, CHUNKS, rows // CHUNKS, wide), BF16),
        dma((2, HALF, CHUNKS)),
        dma((2, HALF, CHUNKS)),
        pltpu.VMEM((NY, rows, 2 * head_qk), BF16),
        pltpu.VMEM((2, NY, rows, 2 * head_qk), BF16),
        dma((NY,)),
        dma((NY,)),
        pltpu.VMEM((2, NY, rows, 128), F32),
        pltpu.VMEM((2, NY, rows, 128), F32),
        pltpu.VMEM((2, NY, rows, head_v), F32),
        pltpu.VMEM((NY, 2, half, 2 * head_v), BF16),
        pltpu.VMEM((NY, 8, rows), F32),
        pltpu.VMEM((3, 2, half, 2 * head_v), BF16),
        pltpu.VMEM((NY, 8, rows), F32),
        pltpu.VMEM((2, half, 2 * head_v), BF16),
        dma((2, 2)),
        dma((2, 2)),
        dma((2, 2)),
        dma((2, 2)),
        dma((NY,)),
        dma((NY,)),
        pltpu.VMEM((heads, 2, head_v // 2, out_proj.shape[1]), BF16),
        dma((2, 3)),
        dma((2, 3)),
        dma((4, 2)),
        dma((4, 2)),
        pltpu.VMEM((heads, 2, half, head_v), BF16),
        dma((2, 3)),
        dma((2, 3)),
        dma((4, 2)),
        dma((4, 2)),
        pltpu.VMEM((rows, out_proj.shape[1]), BF16),
        dma((out_proj.shape[1] // 256,)),
    ]
    return pl.pallas_call(
        kernel,
        out_shape=jax.ShapeDtypeStruct((rows, out_proj.shape[1]), BF16),
        in_specs=[anywhere] * 6
        + [
            pl.BlockSpec(memory_space=pltpu.SMEM),
            pl.BlockSpec(memory_space=pltpu.VMEM),
            anywhere,
        ],
        out_specs=anywhere,
        scratch_shapes=scratch,
        compiler_params=pltpu.CompilerParams(
            collective_id=0, has_side_effects=True, vmem_limit_bytes=62 * 1024 * 1024
        ),
    )(
        hidden_in, query_one.T, query_two.T, key_one.T, key_two.T, value_proj, lambdas, norm_gain,
        out_proj.reshape(2, head_v // 2, out_proj.shape[1]),
    )


def solution(mesh):
    torus = Mesh(mesh.devices.reshape(NZ, NY, mesh.shape["tp"]), ("sp_0", "sp_1", "tp"))
    placed = (
        P(SP, None),
        P(None, "tp"),
        P(None, "tp"),
        P(None, "tp"),
        P(None, "tp"),
        P(None, "tp"),
        P("tp"),
        P(),
        P("tp", None),
    )
    return jax.shard_map(
        shards, mesh=torus, in_specs=placed, out_specs=P(SP, None), check_vma=False
    )
```

```python
import math

import jax
import jax.numpy as jnp
from jax import lax
from jax.experimental import pallas as pl
from jax.experimental.pallas import tpu as pltpu
from jax.sharding import Mesh
from jax.sharding import PartitionSpec as P

SP = ("sp_0", "sp_1")
F32 = jnp.float32
BF16 = jnp.bfloat16
MESH = pl.DeviceIdType.MESH

epsilon = 1e-06
masked_score = -1e30

NZ = 16
NY = 4
NX = 4
HALF = NZ // 2
CHUNKS = 4
FAR = 2


def kernel(
    hidden_hbm, wq1_hbm, wq2_hbm, wk1_hbm, wk2_hbm, wv_hbm, lam_hbm, gain_hbm, wo_hbm,
    out_ref,
    hid, wq, wk, wv, lam_ref, gain_ref, load_sem,
    kv, kv_send, kv_recv,
    qbuf, qz, q_send, q_recv,
    m_ref, l_ref, acc_ref,
    opart, stats, orecv, strecv, relay, o_send, o_recv, rel_send, rel_recv, st_send, st_recv,
    wo, wo_send, wo_recv, wo_dsend, wo_drecv,
    nb, nb_send, nb_recv, nb_dsend, nb_drecv,
):
    z = lax.axis_index("sp_0")
    y = lax.axis_index("sp_1")
    t = lax.axis_index("tp")
    x = t // 2
    core = t % 2
    rows = hid.shape[0]
    head_qk = wq.shape[1]
    head_v = wv.shape[1]
    half_rows = rows // 2
    scale = 1.75 * head_qk ** (-0.5) * math.log2(math.e)

    z_up, z_down = (z + 1) % NZ, (z + NZ - 1) % NZ
    y_at = [y, (y + 1) % NY, (y + 2) % NY, (y + 3) % NY]
    x_at = [x, (x + 1) % NX, (x + 2) % NX, (x + 3) % NX]
    tp_at = [2 * xx + core for xx in x_at]
    sibling = 2 * x + (1 - core)

    loads = [
        pltpu.make_async_copy(hidden_hbm, hid, load_sem.at[0]),
        pltpu.make_async_copy(wk1_hbm, wk.at[0], load_sem.at[1]),
        pltpu.make_async_copy(wk2_hbm, wk.at[1], load_sem.at[2]),
        pltpu.make_async_copy(wv_hbm, wv, load_sem.at[3]),
        pltpu.make_async_copy(wq1_hbm, wq.at[0], load_sem.at[4]),
        pltpu.make_async_copy(wq2_hbm, wq.at[1], load_sem.at[5]),
        pltpu.make_async_copy(wo_hbm, wo.at[t], load_sem.at[6]),
        pltpu.make_async_copy(gain_hbm, gain_ref, load_sem.at[7]),
        pltpu.make_async_copy(lam_hbm, lam_ref, load_sem.at[8]),
    ]
    for load in loads:
        load.start()

    barrier = pltpu.get_barrier_semaphore()
    partners = [
        {"sp_0": z_up}, {"sp_0": z_down},
        {"sp_1": y_at[1]}, {"sp_1": y_at[2]}, {"sp_1": y_at[3]},
        {"tp": tp_at[1]}, {"tp": tp_at[3]}, {"tp": sibling},
    ]
    for partner in partners:
        pl.semaphore_signal(barrier, inc=1, device_id=partner, device_id_type=MESH)

    def remote(src, dst, send_sem, recv_sem, device):
        return pltpu.make_async_remote_copy(
            src_ref=src, dst_ref=dst, send_sem=send_sem, recv_sem=recv_sem,
            device_id=device, device_id_type=MESH,
        )

    def dot(a, b, dims=((1,), (0,))):
        return lax.dot_general(a, b, (dims, ((), ())), preferred_element_type=F32)

    with jax.named_scope("load_kv"):
        for load in loads[:4]:
            load.wait()
    with jax.named_scope("proj_kv"):
        h = hid[...]
        k = dot(h, wk[...].reshape(2 * head_qk, wk.shape[2]), ((1,), (1,))).astype(BF16)
        v = dot(h, wv[...]).T.astype(BF16)
        kv[z, 0] = k[:half_rows]
        kv[z, 1] = k[half_rows:]
        kv[z, 2] = v[:, :half_rows]
        kv[z, 3] = v[:, half_rows:]

    with jax.named_scope("entry_barrier"):
        pl.semaphore_wait(barrier, len(partners))

    def up(step, chunk, slot):
        ref = kv.at[slot, chunk]
        return remote(
            ref, ref, kv_send.at[0, step - 1, chunk], kv_recv.at[0, step - 1, chunk], {"sp_0": z_up}
        )

    def down(step, chunk, slot):
        ref = kv.at[slot, chunk]
        return remote(
            ref, ref, kv_send.at[1, step - 1, chunk], kv_recv.at[1, step - 1, chunk], {"sp_0": z_down}
        )

    @pl.when(z < NZ - 1)
    def _():
        for chunk in range(CHUNKS):
            up(1, chunk, z).start()

    @pl.when(z < HALF)
    def _():
        for chunk in range(CHUNKS):
            down(1, chunk, z).start()

    with jax.named_scope("proj_q"):
        loads[4].wait()
        loads[5].wait()
        qbuf[y] = dot(wq[...].reshape(2 * head_qk, wq.shape[2]), h, ((1,), (1,))).astype(BF16)

    def q_copy(off, slot):
        return remote(
            qbuf.at[slot], qbuf.at[slot], q_send.at[off], q_recv.at[off], {"sp_1": y_at[off]}
        )

    for off in (2, 1, 3):
        q_copy(off, y).start()

    def gather_ops(buf, send, recv, dsend, drecv):
        def piece_of(direction, order):
            return direction if order != 1 else 1 - direction

        def hop(direction, order, slot):
            ref = buf.at[slot, piece_of(direction, order)]
            to = tp_at[1] if direction == 0 else tp_at[3]
            return remote(ref, ref, send.at[direction, order], recv.at[direction, order], {"tp": to})

        def across(index, piece, slot):
            ref = buf.at[slot, piece]
            return remote(ref, ref, dsend.at[index, piece], drecv.at[index, piece], {"tp": sibling})

        def came(direction):
            return tp_at[3] if direction == 0 else tp_at[1]

        def start_own():
            for order in range(2):
                for direction in range(2):
                    hop(direction, order, t).start()
            for piece in range(2):
                across(0, piece, t).start()

        def take(order):
            for direction in range(2):
                slot = tp_at[2] if order == 2 else came(direction)
                hop(direction, order, slot).wait_recv()
                if order == 0:
                    hop(direction, 2, slot).start()
                index = 2 if order == 2 else (3 if direction == 0 else 1)
                across(index, piece_of(direction, order), slot).start()

        def take_across():
            for index in range(4):
                slot = 2 * x_at[index] + (1 - core)
                for piece in range(2):
                    across(index, piece, slot).wait_recv()

        def drain():
            for direction in range(2):
                for order in range(3):
                    slot = came(direction) if order == 2 else t
                    hop(direction, order, slot).wait_send()
            for index in range(4):
                for piece in range(2):
                    across(index, piece, tp_at[index]).wait_send()

        return start_own, take, take_across, drain

    wo_start, wo_take, wo_take_across, wo_drain = gather_ops(wo, wo_send, wo_recv, wo_dsend, wo_drecv)
    nb_start, nb_take, nb_take_across, nb_drain = gather_ops(nb, nb_send, nb_recv, nb_dsend, nb_drecv)

    loads[6].wait()
    wo_start()

    def pass_on(step, chunk):
        low, high = (z + NZ - step) % NZ, (z + step) % NZ

        @pl.when(z >= step)
        def _():
            up(step, chunk, low).wait_recv()

            @pl.when((z < NZ - 1) & ((step < HALF - 1) | (chunk < CHUNKS // 2)))
            def _():
                up(step + 1, chunk, low).start()

        @pl.when(high < HALF)
        def _():
            down(step, chunk, high).wait_recv()

            @pl.when((step < HALF - 1) | (chunk >= CHUNKS // 2))
            def _():
                down(step + 1, chunk, high).start()

    with jax.named_scope("first_pass"):
        for chunk in range(CHUNKS):
            pass_on(1, chunk)

    with jax.named_scope("wait_q"):
        for off in (1, 3, 2):
            q_copy(off, y_at[(NY - off) % NY]).wait_recv()

    def split_queries(block, _):
        q = qbuf[block].astype(F32) * scale
        high = q.astype(BF16)
        low = (q - high.astype(F32)).astype(BF16)
        nothing = jnp.zeros((head_qk, rows), BF16)
        qz[0, block] = jnp.concatenate((high[:head_qk], nothing, low[:head_qk], nothing), axis=0)
        qz[1, block] = jnp.concatenate((nothing, high[head_qk:], nothing, low[head_qk:]), axis=0)
        return 0

    with jax.named_scope("split_q"):
        lax.fori_loop(0, NY, split_queries, 0)

    def block_of(slot):
        keys = jnp.concatenate((kv[slot, 0], kv[slot, 1]), axis=0)
        return (
            jnp.concatenate((keys, keys), axis=1),
            jnp.concatenate((kv[slot, 2], kv[slot, 3]), axis=1),
        )

    def attend(blocks, slots, own=False):
        keys, vals = zip(*[block_of(slot) for slot in slots])
        vals = jnp.concatenate(vals, axis=1)
        units = [(pick, block) for block in blocks for pick in range(2)]
        groups = rows // 8

        def allowed(block):
            k_pos = y * rows + lax.broadcasted_iota(jnp.int32, (rows, rows), 0)
            q_pos = block * rows + lax.broadcasted_iota(jnp.int32, (rows, rows), 1)
            return k_pos <= q_pos

        def score(unit):
            pick, block = unit
            found = [dot(one, qz[pick, block]) for one in keys]
            if own:
                found = [jnp.where(allowed(block), one, masked_score) for one in found]
            highest = None
            for one in found:
                top = jnp.max(one.reshape(groups, 8, rows), axis=0)
                highest = top if highest is None else jnp.maximum(highest, top)
            return found, highest

        def absorb(unit, found, highest):
            pick, block = unit
            now = jnp.broadcast_to(jnp.max(highest, axis=0, keepdims=True), (8, rows))
            if not own:
                before = m_ref[pick, block]
                now = jnp.maximum(before, now)
                rescale = jnp.exp2(before - now)
            total = None
            parts = []
            for one in found:
                part = jnp.exp2(one.reshape(groups, 8, rows) - now[None])
                if own:
                    part = jnp.where(allowed(block).reshape(groups, 8, rows), part, 0.0)
                summed = jnp.sum(part, axis=0)
                total = summed if total is None else total + summed
                parts.append(part.reshape(rows, rows).astype(BF16))
            added = dot(vals, jnp.concatenate(parts, axis=0))
            m_ref[pick, block] = now
            if own:
                l_ref[pick, block] = total
                acc_ref[pick, block] = added
            else:
                l_ref[pick, block] = l_ref[pick, block] * rescale + total
                kept = acc_ref[pick, block].reshape(head_v // 8, 8, rows) * rescale[None]
                acc_ref[pick, block] = kept.reshape(head_v, rows) + added

        ahead = score(units[0])
        for index, unit in enumerate(units):
            here = ahead
            if index + 1 < len(units):
                ahead = score(units[index + 1])
            absorb(unit, *here)

    def attend_pair(step, part):
        low, high = (z + NZ - step) % NZ, (z + step) % NZ
        blocks = (2 * part, 2 * part + 1)

        @pl.when(z >= NZ - step)
        def _():
            attend(blocks, (low, high))

        @pl.when((z >= step) & (z < NZ - step))
        def _():
            attend(blocks, (low,))

    opposite = (z + HALF) % NZ

    def o_copy(direction, piece, slot):
        to = y_at[1] if direction == 0 else y_at[3]
        return remote(
            opart.at[slot, piece], orecv.at[direction, piece],
            o_send.at[direction, piece], o_recv.at[direction, piece], {"sp_1": to},
        )

    def rel_copy(direction, slot):
        to = y_at[1] if direction == 0 else y_at[3]
        return remote(
            opart.at[slot, direction], relay.at[direction],
            rel_send.at[direction, 0], rel_recv.at[direction, 0], {"sp_1": to},
        )

    def rel_forward(direction):
        to = y_at[1] if direction == 0 else y_at[3]
        return remote(
            relay.at[direction], orecv.at[2, direction],
            rel_send.at[direction, 1], rel_recv.at[direction, 1], {"sp_1": to},
        )

    def st_copy(off, slot):
        return remote(
            stats.at[slot], strecv.at[off], st_send.at[off], st_recv.at[off], {"sp_1": y_at[off]}
        )

    def pack(block):
        table = []
        for pick in range(2):
            table.append(m_ref[pick, block][:1])
            table.append(jnp.sum(l_ref[pick, block], axis=0, keepdims=True))
            part = acc_ref[pick, block].astype(BF16)
            for piece in range(2):
                span = slice(piece * half_rows, (piece + 1) * half_rows)
                opart[block, piece, pick * head_v : (pick + 1) * head_v] = part[:, span]
        table.append(jnp.zeros((4, rows), F32))
        stats[block] = jnp.concatenate(table, axis=0)

    def finish_send(late):
        if late:

            @pl.when(z >= HALF)
            def _():
                attend((y_at[2], y_at[1]), (opposite,))

        pack(y_at[2])
        rel_copy(0, y_at[2]).start()
        rel_copy(1, y_at[2]).start()
        st_copy(2, y_at[2]).start()
        pack(y_at[1])
        o_copy(0, 0, y_at[1]).start()
        o_copy(0, 1, y_at[1]).start()
        st_copy(1, y_at[1]).start()
        if late:

            @pl.when(z >= HALF)
            def _():
                attend((y_at[3], y_at[0]), (opposite,))

        pack(y_at[3])
        o_copy(1, 0, y_at[3]).start()
        o_copy(1, 1, y_at[3]).start()
        st_copy(3, y_at[3]).start()
        pack(y_at[0])

    def finish_relay():
        for direction in range(2):
            rel_copy(direction, y_at[2]).wait_recv()
            rel_forward(direction).start()

    def finish_combine():
        for off in range(1, NY):
            st_copy(off, y_at[0]).wait_recv()
        lam = lam_ref[0]
        tables = [stats[y], strecv[1], strecv[3], strecv[2]]
        coefs = []
        for pick in range(2):
            maxima = [table[2 * pick : 2 * pick + 1] for table in tables]
            sums = [table[2 * pick + 1 : 2 * pick + 2] for table in tables]
            highest = maxima[0]
            for other in maxima[1:]:
                highest = jnp.maximum(highest, other)
            shares = [jnp.exp2(one - highest) for one in maxima]
            total = shares[0] * sums[0]
            for share, one in zip(shares[1:], sums[1:]):
                total = total + share * one
            factor = (1.0 if pick == 0 else -lam) / total
            coefs.append([share * factor for share in shares])
        gain = gain_ref[...].reshape(1, head_v)
        for piece in range(2):
            o_copy(0, piece, y_at[1]).wait_recv()
            o_copy(1, piece, y_at[3]).wait_recv()
            rel_forward(piece).wait_recv()
            span = slice(piece * half_rows, (piece + 1) * half_rows)
            mixed = None
            for pick in range(2):
                parts = [acc_ref[pick, y][:, span]]
                for source in range(3):
                    one = orecv[source, piece, pick * head_v : (pick + 1) * head_v]
                    parts.append(one.astype(F32))
                for part, coef in zip(parts, coefs[pick]):
                    term = part * coef[:, span]
                    mixed = term if mixed is None else mixed + term
            spread = lax.rsqrt(jnp.mean(mixed * mixed, axis=0, keepdims=True) + epsilon)
            nb[t, piece] = ((mixed * spread).T * gain).astype(BF16)
        nb_start()

    def finish_gather():
        nb_take(0)
        nb_take(1)
        nb_take(2)

    loads[7].wait()
    loads[8].wait()

    def ring_step(index, _):
        step, part = index // 2, index % 2

        def pass_one(chunk):
            @pl.when(step < HALF)
            def _():
                with jax.named_scope("pass_on"):
                    pass_on(step, chunk)

        pass_one(2 * part)

        @pl.when(step == 2)
        def _():
            attend((2 * part, 2 * part + 1), (z,), own=True)

        pass_one(2 * part + 1)
        with jax.named_scope("attend_pair"):
            attend_pair(step - 1, part)

        @pl.when(index == 8)
        def _():
            wo_take(0)

        @pl.when(index == 12)
        def _():
            wo_take(1)

        for at, phase in ((5, lambda: finish_send(False)), (7, finish_relay), (10, finish_combine), (14, finish_gather)):

            @pl.when((z == 0) & (index == at))
            def _(phase=phase):
                phase()

        return 0

    with jax.named_scope("ring"):
        lax.fori_loop(4, 2 * HALF + 2, ring_step, 0)

    with jax.named_scope("last_wait"):

        @pl.when(z >= HALF)
        def _():
            for chunk in range(CHUNKS):
                if chunk < CHUNKS // 2:
                    up(HALF, chunk, opposite).wait_recv()
                else:
                    down(HALF, chunk, opposite).wait_recv()

    @pl.when(z > 0)
    def _():
        with jax.named_scope("finish_send"):
            finish_send(True)
        with jax.named_scope("finish_relay"):
            finish_relay()

    with jax.named_scope("wo_far"):
        wo_take(2)

    @pl.when(z > 0)
    def _():
        with jax.named_scope("finish_combine"):
            finish_combine()
        with jax.named_scope("finish_gather"):
            finish_gather()

    with jax.named_scope("take_across"):
        wo_take_across()
        nb_take_across()

    with jax.named_scope("out_proj"):
        lhs = jnp.concatenate([nb[head].reshape(rows, head_v) for head in range(2 * NX)], axis=1)
        width = 256
        for left in range(0, out_ref.shape[1], width):
            rhs = wo[:, :, :, left : left + width].reshape(2 * NX * head_v, width)
            out_ref[:, left : left + width] = dot(lhs, rhs).astype(BF16)

    def drain_ring(index, _):
        step, chunk = index // CHUNKS, index % CHUNKS

        @pl.when((z < NZ - 1) & (z + 1 >= step) & ((step < HALF) | (chunk < CHUNKS // 2)))
        def _():
            up(step, chunk, z).wait_send()

        @pl.when(((z + step - 1) % NZ < HALF) & ((step < HALF) | (chunk >= CHUNKS // 2)))
        def _():
            down(step, chunk, z).wait_send()

        return 0

    with jax.named_scope("drain"):
        lax.fori_loop(CHUNKS, (HALF + 1) * CHUNKS, drain_ring, 0)
        for off in range(1, NY):
            q_copy(off, y).wait_send()
            st_copy(off, y).wait_send()
        for direction in range(2):
            for piece in range(2):
                o_copy(direction, piece, y).wait_send()
            rel_copy(direction, y).wait_send()
            rel_forward(direction).wait_send()
        wo_drain()
        nb_drain()


def shards(
    hidden_in, query_one, query_two, key_one, key_two, value_proj, lambdas, norm_gain, out_proj
):
    rows, depth = hidden_in.shape
    head_qk = query_one.shape[1]
    head_v = value_proj.shape[1]
    half = rows // 2
    heads = 2 * NX
    dma = pltpu.SemaphoreType.DMA
    scratch = [
        pltpu.VMEM((rows, depth), BF16),
        pltpu.VMEM((2, head_qk, depth), BF16),
        pltpu.VMEM((2, head_qk, depth), BF16),
        pltpu.VMEM((depth, head_v), BF16),
        pltpu.SMEM((1,), F32),
        pltpu.VMEM((head_v,), F32),
        dma((9,)),
        pltpu.VMEM((NZ, CHUNKS, half, head_v), BF16),
        dma((2, HALF, CHUNKS)),
        dma((2, HALF, CHUNKS)),
        pltpu.VMEM((NY, 2 * head_qk, rows), BF16),
        pltpu.VMEM((2, NY, 4 * head_qk, rows), BF16),
        dma((NY,)),
        dma((NY,)),
        pltpu.VMEM((2, NY, 8, rows), F32),
        pltpu.VMEM((2, NY, 8, rows), F32),
        pltpu.VMEM((2, NY, head_v, rows), F32),
        pltpu.VMEM((NY, 2, 2 * head_v, half), BF16),
        pltpu.VMEM((NY, 8, rows), F32),
        pltpu.VMEM((3, 2, 2 * head_v, half), BF16),
        pltpu.VMEM((NY, 8, rows), F32),
        pltpu.VMEM((2, 2 * head_v, half), BF16),
        dma((2, 2)),
        dma((2, 2)),
        dma((2, 2)),
        dma((2, 2)),
        dma((NY,)),
        dma((NY,)),
        pltpu.VMEM((heads, 2, head_v // 2, out_proj.shape[1]), BF16),
        dma((2, 3)),
        dma((2, 3)),
        dma((4, 2)),
        dma((4, 2)),
        pltpu.VMEM((heads, 2, half, head_v), BF16),
        dma((2, 3)),
        dma((2, 3)),
        dma((4, 2)),
        dma((4, 2)),
    ]
    return pl.pallas_call(
        kernel,
        out_shape=pltpu.VMEM((rows, out_proj.shape[1]), BF16),
        in_specs=[pl.BlockSpec(memory_space=pltpu.HBM)] * 9,
        out_specs=pl.BlockSpec(memory_space=pltpu.VMEM),
        scratch_shapes=scratch,
        compiler_params=pltpu.CompilerParams(
            collective_id=0, has_side_effects=True, vmem_limit_bytes=60 * 1024 * 1024
        ),
    )(
        hidden_in, query_one.T, query_two.T, key_one.T, key_two.T, value_proj, lambdas, norm_gain,
        out_proj.reshape(2, head_v // 2, out_proj.shape[1]),
    )


def solution(mesh):
    torus = Mesh(mesh.devices.reshape(NZ, NY, mesh.shape["tp"]), ("sp_0", "sp_1", "tp"))
    placed = (
        P(SP, None),
        P(None, "tp"),
        P(None, "tp"),
        P(None, "tp"),
        P(None, "tp"),
        P(None, "tp"),
        P("tp"),
        P(),
        P("tp", None),
    )
    return jax.shard_map(
        shards, mesh=torus, in_specs=placed, out_specs=P(SP, None), check_vma=False
    )
```

```python
import math

import jax
import jax.numpy as jnp
from jax import lax
from jax.experimental import pallas as pl
from jax.experimental.pallas import tpu as pltpu
from jax.sharding import Mesh
from jax.sharding import PartitionSpec as P

SP = ("sp_0", "sp_1")
F32 = jnp.float32
BF16 = jnp.bfloat16
MESH = pl.DeviceIdType.MESH

epsilon = 1e-06
masked_score = -1e30

NZ = 16
NY = 4
NX = 4
HALF = NZ // 2
CHUNKS = 4
FAR = 2


def kernel(
    hidden_hbm, wq1_hbm, wq2_hbm, wk1_hbm, wk2_hbm, wv_hbm, lam_hbm, gain_hbm, wo_hbm,
    out_ref,
    hid, wq, wk, wv, lam_ref, gain_ref, load_sem,
    kv, kv_send, kv_recv, own_send, own_recv, give_send, give_recv,
    qbuf, qz, q_send, q_recv,
    m_ref, l_ref, acc_ref,
    opart, stats, orecv, strecv, relay, o_send, o_recv, rel_send, rel_recv, st_send, st_recv,
    wo, wo_send, wo_recv, wo_dsend, wo_drecv,
    nb, nb_send, nb_recv, nb_dsend, nb_drecv,
    out_v, out_sem,
):
    z = lax.axis_index("sp_0")
    y = lax.axis_index("sp_1")
    t = lax.axis_index("tp")
    x = t // 2
    core = t % 2
    rows = hid.shape[0]
    head_qk = wq.shape[1]
    head_v = wv.shape[1]
    half_rows = rows // 2
    scale = 1.75 * head_qk ** (-0.5) * math.log2(math.e)

    z_up, z_down = (z + 1) % NZ, (z + NZ - 1) % NZ
    y_at = [y, (y + 1) % NY, (y + 2) % NY, (y + 3) % NY]
    x_at = [x, (x + 1) % NX, (x + 2) % NX, (x + 3) % NX]
    tp_at = [2 * xx + core for xx in x_at]
    sibling = 2 * x + (1 - core)

    loads = [
        pltpu.make_async_copy(hidden_hbm, hid, load_sem.at[0]),
        pltpu.make_async_copy(wk1_hbm, wk.at[0], load_sem.at[1]),
        pltpu.make_async_copy(wk2_hbm, wk.at[1], load_sem.at[2]),
        pltpu.make_async_copy(wv_hbm, wv, load_sem.at[3]),
        pltpu.make_async_copy(wq1_hbm, wq.at[0], load_sem.at[4]),
        pltpu.make_async_copy(wq2_hbm, wq.at[1], load_sem.at[5]),
        pltpu.make_async_copy(wo_hbm, wo.at[t], load_sem.at[6]),
        pltpu.make_async_copy(gain_hbm, gain_ref, load_sem.at[7]),
        pltpu.make_async_copy(lam_hbm, lam_ref, load_sem.at[8]),
    ]
    for load in loads:
        load.start()

    barrier = pltpu.get_barrier_semaphore()
    partners = [
        {"sp_0": z_up}, {"sp_0": z_down},
        {"sp_1": y_at[1]}, {"sp_1": y_at[2]}, {"sp_1": y_at[3]},
        {"tp": tp_at[1]}, {"tp": tp_at[3]}, {"tp": sibling},
    ]
    for partner in partners:
        pl.semaphore_signal(barrier, inc=1, device_id=partner, device_id_type=MESH)

    def remote(src, dst, send_sem, recv_sem, device):
        return pltpu.make_async_remote_copy(
            src_ref=src, dst_ref=dst, send_sem=send_sem, recv_sem=recv_sem,
            device_id=device, device_id_type=MESH,
        )

    def dot(a, b, dims=((1,), (0,))):
        return lax.dot_general(a, b, (dims, ((), ())), preferred_element_type=F32)

    with jax.named_scope("load_kv"):
        for load in loads[:4]:
            load.wait()
    with jax.named_scope("proj_kv"):
        h = hid[...]
        k = dot(h, wk[...].reshape(2 * head_qk, wk.shape[2]), ((1,), (1,))).astype(BF16)
        v = dot(h, wv[...]).T.astype(BF16)
        for chunk, piece in enumerate((k[:half_rows], k[half_rows:], v[:, :half_rows], v[:, half_rows:])):
            kv[z, chunk, core] = piece

    with jax.named_scope("entry_barrier"):
        pl.semaphore_wait(barrier, len(partners))

    def up(step, chunk, slot):
        ref = kv.at[slot, chunk]
        return remote(
            ref, ref, kv_send.at[0, step - 1, chunk], kv_recv.at[0, step - 1, chunk], {"sp_0": z_up}
        )

    def down(step, chunk, slot):
        ref = kv.at[slot, chunk]
        return remote(
            ref, ref, kv_send.at[1, step - 1, chunk], kv_recv.at[1, step - 1, chunk], {"sp_0": z_down}
        )

    def own_over(chunk):
        ref = kv.at[z, chunk, 0]
        return remote(ref, ref, own_send.at[chunk], own_recv.at[chunk], {"tp": sibling})

    def give(direction, step, chunk, slot):
        ref = kv.at[slot, chunk, 0]
        return remote(
            ref, ref, give_send.at[direction, step - 1, chunk], give_recv.at[direction, step - 1, chunk],
            {"tp": sibling},
        )

    @pl.when(core == 0)
    def _():
        for chunk in range(CHUNKS):
            own_over(chunk).start()

    with jax.named_scope("proj_q"):
        loads[4].wait()
        loads[5].wait()
        qbuf[y] = dot(wq[...].reshape(2 * head_qk, wq.shape[2]), h, ((1,), (1,))).astype(BF16)

    def q_copy(off, slot):
        return remote(
            qbuf.at[slot], qbuf.at[slot], q_send.at[off], q_recv.at[off], {"sp_1": y_at[off]}
        )

    for off in (2, 1, 3):
        q_copy(off, y).start()

    @pl.when(core == 1)
    def _():
        for chunk in range(CHUNKS):
            own_over(chunk).wait_recv()

            @pl.when(z < NZ - 1)
            def _(chunk=chunk):
                up(1, chunk, z).start()

            @pl.when(z < HALF)
            def _(chunk=chunk):
                down(1, chunk, z).start()


    def gather_ops(buf, send, recv, dsend, drecv):
        def piece_of(direction, order):
            return direction if order != 1 else 1 - direction

        def hop(direction, order, slot):
            ref = buf.at[slot, piece_of(direction, order)]
            to = tp_at[1] if direction == 0 else tp_at[3]
            return remote(ref, ref, send.at[direction, order], recv.at[direction, order], {"tp": to})

        def across(index, piece, slot):
            ref = buf.at[slot, piece]
            return remote(ref, ref, dsend.at[index, piece], drecv.at[index, piece], {"tp": sibling})

        def came(direction):
            return tp_at[3] if direction == 0 else tp_at[1]

        def start_own():
            for order in range(2):
                for direction in range(2):
                    hop(direction, order, t).start()
            for piece in range(2):
                across(0, piece, t).start()

        def take(order):
            for direction in range(2):
                slot = tp_at[2] if order == 2 else came(direction)
                hop(direction, order, slot).wait_recv()
                if order == 0:
                    hop(direction, 2, slot).start()
                index = 2 if order == 2 else (3 if direction == 0 else 1)
                across(index, piece_of(direction, order), slot).start()

        def take_across():
            for index in range(4):
                slot = 2 * x_at[index] + (1 - core)
                for piece in range(2):
                    across(index, piece, slot).wait_recv()

        def drain():
            for direction in range(2):
                for order in range(3):
                    slot = came(direction) if order == 2 else t
                    hop(direction, order, slot).wait_send()
            for index in range(4):
                for piece in range(2):
                    across(index, piece, tp_at[index]).wait_send()

        return start_own, take, take_across, drain

    wo_start, wo_take, wo_take_across, wo_drain = gather_ops(wo, wo_send, wo_recv, wo_dsend, wo_drecv)

    def nb_hop(direction, order, head, chip):
        piece = direction if order != 1 else 1 - direction
        ref = nb.at[2 * chip + head, piece]
        to = 2 * (x_at[1] if direction == 0 else x_at[3]) + 1
        return remote(
            ref, ref, nb_send.at[direction, order, head], nb_recv.at[direction, order, head], {"tp": to}
        )

    def nb_across(index, head, piece, chip):
        ref = nb.at[2 * chip + head, piece]
        return remote(
            ref, ref, nb_dsend.at[index, head, piece], nb_drecv.at[index, head, piece], {"tp": sibling}
        )

    def nb_start():
        for piece in range(2):
            nb_across(0, core, piece, x).start()

    def nb_gather():
        @pl.when(core == 1)
        def _():
            for head in (1, 0):
                for order in range(2):
                    for direction in range(2):
                        piece = direction if order != 1 else 1 - direction
                        if head == 0 and order == 0:
                            nb_across(0, 0, piece, x).wait_recv()
                        nb_hop(direction, order, head, x).start()
            for head in (1, 0):
                for order in range(3):
                    for direction in range(2):
                        piece = direction if order != 1 else 1 - direction
                        index = 2 if order == 2 else (3 if direction == 0 else 1)
                        nb_hop(direction, order, head, x_at[index]).wait_recv()
                        if order == 0:
                            nb_hop(direction, 2, head, x_at[index]).start()
                        nb_across(index, head, piece, x_at[index]).start()

        @pl.when(core == 0)
        def _():
            nb_across(0, 1, 0, x).wait_recv()
            nb_across(0, 1, 1, x).wait_recv()
            for head in (1, 0):
                for index in (1, 3, 2):
                    for piece in range(2):
                        nb_across(index, head, piece, x_at[index]).wait_recv()

    def nb_drain():
        for piece in range(2):
            nb_across(0, core, piece, x).wait_send()

        @pl.when(core == 1)
        def _():
            for head in (1, 0):
                for direction in range(2):
                    for order in range(3):
                        nb_hop(direction, order, head, x).wait_send()
                for index in (1, 3, 2):
                    for piece in range(2):
                        nb_across(index, head, piece, x).wait_send()

    loads[6].wait()
    wo_start()

    def pass_on(step, chunk):
        low, high = (z + NZ - step) % NZ, (z + step) % NZ

        @pl.when(core == 1)
        def _():
            @pl.when(z >= step)
            def _():
                up(step, chunk, low).wait_recv()

                @pl.when((z < NZ - 1) & ((step < HALF - 1) | (chunk < CHUNKS // 2)))
                def _():
                    up(step + 1, chunk, low).start()

                give(0, step, chunk, low).start()

            @pl.when(high < HALF)
            def _():
                down(step, chunk, high).wait_recv()

                @pl.when((step < HALF - 1) | (chunk >= CHUNKS // 2))
                def _():
                    down(step + 1, chunk, high).start()

                @pl.when(z >= NZ - step)
                def _():
                    give(1, step, chunk, high).start()

        @pl.when(core == 0)
        def _():
            @pl.when(z >= step)
            def _():
                give(0, step, chunk, low).wait_recv()

            @pl.when(z >= NZ - step)
            def _():
                give(1, step, chunk, high).wait_recv()

    with jax.named_scope("first_pass"):
        for chunk in range(CHUNKS):
            pass_on(1, chunk)

    with jax.named_scope("wait_q"):
        for off in (1, 3, 2):
            q_copy(off, y_at[(NY - off) % NY]).wait_recv()

    def split_queries(block, _):
        q = qbuf[block].astype(F32) * scale
        high = q.astype(BF16)
        low = (q - high.astype(F32)).astype(BF16)
        nothing = jnp.zeros((head_qk, rows), BF16)
        qz[0, block] = jnp.concatenate((high[:head_qk], nothing, low[:head_qk], nothing), axis=0)
        qz[1, block] = jnp.concatenate((nothing, high[head_qk:], nothing, low[head_qk:]), axis=0)
        return 0

    with jax.named_scope("split_q"):
        lax.fori_loop(0, NY, split_queries, 0)

    def block_of(slot):
        keys = jnp.concatenate((kv[slot, 0, core], kv[slot, 1, core]), axis=0)
        return (
            jnp.concatenate((keys, keys), axis=1),
            jnp.concatenate((kv[slot, 2, core], kv[slot, 3, core]), axis=1),
        )

    def attend(blocks, slots, own=False):
        keys, vals = zip(*[block_of(slot) for slot in slots])
        vals = jnp.concatenate(vals, axis=1)
        units = [(pick, block) for block in blocks for pick in range(2)]
        groups = rows // 8

        def allowed(block):
            k_pos = y * rows + lax.broadcasted_iota(jnp.int32, (rows, rows), 0)
            q_pos = block * rows + lax.broadcasted_iota(jnp.int32, (rows, rows), 1)
            return k_pos <= q_pos

        def score(unit):
            pick, block = unit
            found = [dot(one, qz[pick, block]) for one in keys]
            if own:
                found = [jnp.where(allowed(block), one, masked_score) for one in found]
            highest = None
            for one in found:
                top = jnp.max(one.reshape(groups, 8, rows), axis=0)
                highest = top if highest is None else jnp.maximum(highest, top)
            return found, highest

        def absorb(unit, found, highest):
            pick, block = unit
            now = jnp.broadcast_to(jnp.max(highest, axis=0, keepdims=True), (8, rows))
            if not own:
                before = m_ref[pick, block]
                now = jnp.maximum(before, now)
                rescale = jnp.exp2(before - now)
            total = None
            parts = []
            for one in found:
                part = jnp.exp2(one.reshape(groups, 8, rows) - now[None])
                if own:
                    part = jnp.where(allowed(block).reshape(groups, 8, rows), part, 0.0)
                summed = jnp.sum(part, axis=0)
                total = summed if total is None else total + summed
                parts.append(part.reshape(rows, rows).astype(BF16))
            added = dot(vals, jnp.concatenate(parts, axis=0))
            m_ref[pick, block] = now
            if own:
                l_ref[pick, block] = total
                acc_ref[pick, block] = added
            else:
                l_ref[pick, block] = l_ref[pick, block] * rescale + total
                kept = acc_ref[pick, block].reshape(head_v // 8, 8, rows) * rescale[None]
                acc_ref[pick, block] = kept.reshape(head_v, rows) + added

        ahead = score(units[0])
        for index, unit in enumerate(units):
            here = ahead
            if index + 1 < len(units):
                ahead = score(units[index + 1])
            absorb(unit, *here)

    def attend_pair(step, part):
        low, high = (z + NZ - step) % NZ, (z + step) % NZ
        blocks = (2 * part, 2 * part + 1)

        @pl.when(z >= NZ - step)
        def _():
            attend(blocks, (low, high))

        @pl.when((z >= step) & (z < NZ - step))
        def _():
            attend(blocks, (low,))

    opposite = (z + HALF) % NZ

    def o_copy(direction, piece, slot):
        to = y_at[1] if direction == 0 else y_at[3]
        return remote(
            opart.at[slot, piece], orecv.at[direction, piece],
            o_send.at[direction, piece], o_recv.at[direction, piece], {"sp_1": to},
        )

    def rel_copy(direction, slot):
        to = y_at[1] if direction == 0 else y_at[3]
        return remote(
            opart.at[slot, direction], relay.at[direction],
            rel_send.at[direction, 0], rel_recv.at[direction, 0], {"sp_1": to},
        )

    def rel_forward(direction):
        to = y_at[1] if direction == 0 else y_at[3]
        return remote(
            relay.at[direction], orecv.at[2, direction],
            rel_send.at[direction, 1], rel_recv.at[direction, 1], {"sp_1": to},
        )

    def st_copy(off, slot):
        return remote(
            stats.at[slot], strecv.at[off], st_send.at[off], st_recv.at[off], {"sp_1": y_at[off]}
        )

    def pack(block):
        table = []
        for pick in range(2):
            table.append(m_ref[pick, block][:1])
            table.append(jnp.sum(l_ref[pick, block], axis=0, keepdims=True))
            part = acc_ref[pick, block].astype(BF16)
            for piece in range(2):
                span = slice(piece * half_rows, (piece + 1) * half_rows)
                opart[block, piece, pick * head_v : (pick + 1) * head_v] = part[:, span]
        table.append(jnp.zeros((4, rows), F32))
        stats[block] = jnp.concatenate(table, axis=0)

    def finish_send(late):
        if late:

            @pl.when(z >= HALF)
            def _():
                attend((y_at[2], y_at[1]), (opposite,))

        pack(y_at[2])
        rel_copy(0, y_at[2]).start()
        rel_copy(1, y_at[2]).start()
        st_copy(2, y_at[2]).start()
        pack(y_at[1])
        o_copy(0, 0, y_at[1]).start()
        o_copy(0, 1, y_at[1]).start()
        st_copy(1, y_at[1]).start()
        if late:

            @pl.when(z >= HALF)
            def _():
                attend((y_at[3], y_at[0]), (opposite,))

        pack(y_at[3])
        o_copy(1, 0, y_at[3]).start()
        o_copy(1, 1, y_at[3]).start()
        st_copy(3, y_at[3]).start()
        pack(y_at[0])

    def finish_relay():
        for direction in range(2):
            rel_copy(direction, y_at[2]).wait_recv()
            rel_forward(direction).start()

    def finish_combine():
        for off in range(1, NY):
            st_copy(off, y_at[0]).wait_recv()
        lam = lam_ref[0]
        tables = [stats[y], strecv[1], strecv[3], strecv[2]]
        coefs = []
        for pick in range(2):
            maxima = [table[2 * pick : 2 * pick + 1] for table in tables]
            sums = [table[2 * pick + 1 : 2 * pick + 2] for table in tables]
            highest = maxima[0]
            for other in maxima[1:]:
                highest = jnp.maximum(highest, other)
            shares = [jnp.exp2(one - highest) for one in maxima]
            total = shares[0] * sums[0]
            for share, one in zip(shares[1:], sums[1:]):
                total = total + share * one
            factor = (1.0 if pick == 0 else -lam) / total
            coefs.append([share * factor for share in shares])
        gain = gain_ref[...].reshape(1, head_v)
        for piece in range(2):
            o_copy(0, piece, y_at[1]).wait_recv()
            o_copy(1, piece, y_at[3]).wait_recv()
            rel_forward(piece).wait_recv()
            span = slice(piece * half_rows, (piece + 1) * half_rows)
            mixed = None
            for pick in range(2):
                parts = [acc_ref[pick, y][:, span]]
                for source in range(3):
                    one = orecv[source, piece, pick * head_v : (pick + 1) * head_v]
                    parts.append(one.astype(F32))
                for part, coef in zip(parts, coefs[pick]):
                    term = part * coef[:, span]
                    mixed = term if mixed is None else mixed + term
            spread = lax.rsqrt(jnp.mean(mixed * mixed, axis=0, keepdims=True) + epsilon)
            nb[t, piece] = ((mixed * spread).T * gain).astype(BF16)
        nb_start()

    def finish_gather():
        nb_gather()

    loads[7].wait()
    loads[8].wait()

    def ring_step(index, _):
        step, part = index // 2, index % 2

        def pass_one(chunk):
            @pl.when(step < HALF)
            def _():
                with jax.named_scope("pass_on"):
                    pass_on(step, chunk)

        pass_one(2 * part)

        @pl.when(step == 2)
        def _():
            attend((2 * part, 2 * part + 1), (z,), own=True)

        pass_one(2 * part + 1)
        with jax.named_scope("attend_pair"):
            attend_pair(step - 1, part)

        @pl.when(index == 8)
        def _():
            wo_take(0)

        @pl.when(index == 12)
        def _():
            wo_take(1)

        for at, phase in ((5, lambda: finish_send(False)), (7, finish_relay), (10, finish_combine), (14, finish_gather)):

            @pl.when((z == 0) & (index == at))
            def _(phase=phase):
                phase()

        return 0

    with jax.named_scope("ring"):
        lax.fori_loop(4, 2 * HALF + 2, ring_step, 0)

    with jax.named_scope("last_wait"):

        @pl.when(z >= HALF)
        def _():
            for chunk in range(CHUNKS):
                direction = 0 if chunk < CHUNKS // 2 else 1
                last = (up, down)[direction](HALF, chunk, opposite)
                handed = give(direction, HALF, chunk, opposite)

                @pl.when(core == 1)
                def _(last=last, handed=handed):
                    last.wait_recv()
                    handed.start()

                @pl.when(core == 0)
                def _(handed=handed):
                    handed.wait_recv()

    @pl.when(z > 0)
    def _():
        with jax.named_scope("finish_send"):
            finish_send(True)

    def drain_ring(index, _):
        step, chunk = index // CHUNKS, index % CHUNKS

        @pl.when((z < NZ - 1) & (z + 1 >= step) & ((step < HALF) | (chunk < CHUNKS // 2)))
        def _():
            up(step, chunk, z).wait_send()

        @pl.when(((z + step - 1) % NZ < HALF) & ((step < HALF) | (chunk >= CHUNKS // 2)))
        def _():
            down(step, chunk, z).wait_send()

        @pl.when((z >= step) & ((step < HALF) | (chunk < CHUNKS // 2)))
        def _():
            give(0, step, chunk, z).wait_send()

        @pl.when((z >= NZ - step) & ((step < HALF) | (chunk >= CHUNKS // 2)))
        def _():
            give(1, step, chunk, z).wait_send()

        return 0

    with jax.named_scope("drain_ring"):

        @pl.when(core == 1)
        def _():
            lax.fori_loop(CHUNKS, (HALF + 1) * CHUNKS, drain_ring, 0)

        @pl.when(core == 0)
        def _():
            for chunk in range(CHUNKS):
                own_over(chunk).wait_send()

        for off in range(1, NY):
            q_copy(off, y).wait_send()

    @pl.when(z > 0)
    def _():
        with jax.named_scope("finish_relay"):
            finish_relay()

    with jax.named_scope("wo_far"):
        wo_take(2)

    @pl.when(z > 0)
    def _():
        with jax.named_scope("finish_combine"):
            finish_combine()
    with jax.named_scope("drain_parts"):
        for off in range(1, NY):
            st_copy(off, y).wait_send()
        for direction in range(2):
            for piece in range(2):
                o_copy(direction, piece, y).wait_send()
            rel_copy(direction, y).wait_send()
            rel_forward(direction).wait_send()

    @pl.when(z > 0)
    def _():
        with jax.named_scope("finish_gather"):
            finish_gather()

    with jax.named_scope("take_across"):
        wo_take_across()

    with jax.named_scope("out_proj"):
        lhs = jnp.concatenate([nb[head].reshape(rows, head_v) for head in range(2 * NX)], axis=1)
        width = 256
        tiles = []
        for left in range(0, out_ref.shape[1], width):
            rhs = wo[:, :, :, left : left + width].reshape(2 * NX * head_v, width)
            out_v[:, left : left + width] = dot(lhs, rhs).astype(BF16)
            tile = pltpu.make_async_copy(
                out_v.at[:, left : left + width], out_ref.at[:, left : left + width],
                out_sem.at[left // width],
            )
            tile.start()
            tiles.append(tile)

    with jax.named_scope("drain"):
        for tile in tiles:
            tile.wait()
        wo_drain()
        nb_drain()


def shards(
    hidden_in, query_one, query_two, key_one, key_two, value_proj, lambdas, norm_gain, out_proj
):
    rows, depth = hidden_in.shape
    head_qk = query_one.shape[1]
    head_v = value_proj.shape[1]
    half = rows // 2
    heads = 2 * NX
    dma = pltpu.SemaphoreType.DMA
    scratch = [
        pltpu.VMEM((rows, depth), BF16),
        pltpu.VMEM((2, head_qk, depth), BF16),
        pltpu.VMEM((2, head_qk, depth), BF16),
        pltpu.VMEM((depth, head_v), BF16),
        pltpu.SMEM((1,), F32),
        pltpu.VMEM((head_v,), F32),
        dma((9,)),
        pltpu.VMEM((NZ, CHUNKS, 2, half, head_v), BF16),
        dma((2, HALF, CHUNKS)),
        dma((2, HALF, CHUNKS)),
        dma((CHUNKS,)),
        dma((CHUNKS,)),
        dma((2, HALF, CHUNKS)),
        dma((2, HALF, CHUNKS)),
        pltpu.VMEM((NY, 2 * head_qk, rows), BF16),
        pltpu.VMEM((2, NY, 4 * head_qk, rows), BF16),
        dma((NY,)),
        dma((NY,)),
        pltpu.VMEM((2, NY, 8, rows), F32),
        pltpu.VMEM((2, NY, 8, rows), F32),
        pltpu.VMEM((2, NY, head_v, rows), F32),
        pltpu.VMEM((NY, 2, 2 * head_v, half), BF16),
        pltpu.VMEM((NY, 8, rows), F32),
        pltpu.VMEM((3, 2, 2 * head_v, half), BF16),
        pltpu.VMEM((NY, 8, rows), F32),
        pltpu.VMEM((2, 2 * head_v, half), BF16),
        dma((2, 2)),
        dma((2, 2)),
        dma((2, 2)),
        dma((2, 2)),
        dma((NY,)),
        dma((NY,)),
        pltpu.VMEM((heads, 2, head_v // 2, out_proj.shape[1]), BF16),
        dma((2, 3)),
        dma((2, 3)),
        dma((4, 2)),
        dma((4, 2)),
        pltpu.VMEM((heads, 2, half, head_v), BF16),
        dma((2, 3, 2)),
        dma((2, 3, 2)),
        dma((4, 2, 2)),
        dma((4, 2, 2)),
        pltpu.VMEM((rows, out_proj.shape[1]), BF16),
        dma((out_proj.shape[1] // 256,)),
    ]
    return pl.pallas_call(
        kernel,
        out_shape=pltpu.VMEM((rows, out_proj.shape[1]), BF16),
        in_specs=[pl.BlockSpec(memory_space=pltpu.HBM)] * 9,
        out_specs=pl.BlockSpec(memory_space=pl.ANY),
        scratch_shapes=scratch,
        compiler_params=pltpu.CompilerParams(
            collective_id=0, has_side_effects=True, vmem_limit_bytes=60 * 1024 * 1024
        ),
    )(
        hidden_in, query_one.T, query_two.T, key_one.T, key_two.T, value_proj, lambdas, norm_gain,
        out_proj.reshape(2, head_v // 2, out_proj.shape[1]),
    )


def solution(mesh):
    torus = Mesh(mesh.devices.reshape(NZ, NY, mesh.shape["tp"]), ("sp_0", "sp_1", "tp"))
    placed = (
        P(SP, None),
        P(None, "tp"),
        P(None, "tp"),
        P(None, "tp"),
        P(None, "tp"),
        P(None, "tp"),
        P("tp"),
        P(),
        P("tp", None),
    )
    return jax.shard_map(
        shards, mesh=torus, in_specs=placed, out_specs=P(SP, None), check_vma=False
    )
```

```python
import math

import jax
import jax.numpy as jnp
from jax import lax
from jax.experimental import pallas as pl
from jax.experimental.pallas import tpu as pltpu
from jax.sharding import Mesh
from jax.sharding import PartitionSpec as P

SP = ("sp_0", "sp_1")
F32 = jnp.float32
BF16 = jnp.bfloat16
MESH = pl.DeviceIdType.MESH

epsilon = 1e-06
masked_score = -1e30

NZ = 16
NY = 4
NX = 4
HALF = NZ // 2
CHUNKS = 4
FAR = 2


def kernel(
    hidden_hbm, wq1_hbm, wq2_hbm, wk1_hbm, wk2_hbm, wv_hbm, lam_hbm, gain_hbm, wo_hbm,
    out_ref,
    hid, wq, wk, wv, lam_ref, gain_ref, load_sem,
    kv, kv_send, kv_recv,
    qbuf, qz, q_send, q_recv,
    m_ref, l_ref, acc_ref, ahead_ref, ahead_max,
    opart, stats, orecv, strecv, relay, o_send, o_recv, rel_recv, st_send, st_recv,
    wo, wo_send, wo_recv, wo_dsend, wo_drecv,
    nb, nb_send, nb_recv, nb_dsend, nb_drecv,
):
    z = lax.axis_index("sp_0")
    y = lax.axis_index("sp_1")
    t = lax.axis_index("tp")
    x = t // 2
    core = t % 2
    rows = hid.shape[0]
    head_qk = wq.shape[1]
    head_v = wv.shape[1]
    half_rows = rows // 2
    scale = 1.75 * head_qk ** (-0.5) * math.log2(math.e)

    z_up, z_down = (z + 1) % NZ, (z + NZ - 1) % NZ
    y_at = [y, (y + 1) % NY, (y + 2) % NY, (y + 3) % NY]
    x_at = [x, (x + 1) % NX, (x + 2) % NX, (x + 3) % NX]
    tp_at = [2 * xx + core for xx in x_at]
    sibling = 2 * x + (1 - core)

    loads = [
        pltpu.make_async_copy(hidden_hbm, hid, load_sem.at[0]),
        pltpu.make_async_copy(wk1_hbm, wk.at[0], load_sem.at[1]),
        pltpu.make_async_copy(wk2_hbm, wk.at[1], load_sem.at[2]),
        pltpu.make_async_copy(wv_hbm, wv, load_sem.at[3]),
        pltpu.make_async_copy(wq1_hbm, wq.at[0], load_sem.at[4]),
        pltpu.make_async_copy(wq2_hbm, wq.at[1], load_sem.at[5]),
        pltpu.make_async_copy(wo_hbm, wo.at[t], load_sem.at[6]),
        pltpu.make_async_copy(gain_hbm, gain_ref, load_sem.at[7]),
        pltpu.make_async_copy(lam_hbm, lam_ref, load_sem.at[8]),
    ]
    for load in loads:
        load.start()

    barrier = pltpu.get_barrier_semaphore()
    partners = [
        {"sp_0": z_up}, {"sp_0": z_down},
        {"sp_1": y_at[1]}, {"sp_1": y_at[2]}, {"sp_1": y_at[3]},
        {"tp": tp_at[1]}, {"tp": tp_at[2]}, {"tp": tp_at[3]}, {"tp": sibling},
    ]
    for partner in partners:
        pl.semaphore_signal(barrier, inc=1, device_id=partner, device_id_type=MESH)

    def remote(src, dst, send_sem, recv_sem, device):
        return pltpu.make_async_remote_copy(
            src_ref=src, dst_ref=dst, send_sem=send_sem, recv_sem=recv_sem,
            device_id=device, device_id_type=MESH,
        )

    def dot(a, b, dims=((1,), (0,))):
        return lax.dot_general(a, b, (dims, ((), ())), preferred_element_type=F32)

    with jax.named_scope("load_kv"):
        for load in loads[:4]:
            load.wait()
    with jax.named_scope("proj_kv"):
        h = hid[...]
        k = dot(h, wk[...].reshape(2 * head_qk, wk.shape[2]), ((1,), (1,))).astype(BF16)
        v = dot(h, wv[...]).T.astype(BF16)
        kv[z, 0] = k[:half_rows]
        kv[z, 1] = k[half_rows:]
        kv[z, 2] = v[:, :half_rows]
        kv[z, 3] = v[:, half_rows:]

    with jax.named_scope("entry_barrier"):
        pl.semaphore_wait(barrier, len(partners))

    def up(step, chunk, slot):
        ref = kv.at[slot, chunk]
        return remote(
            ref, ref, kv_send.at[0, chunk], kv_recv.at[0, step - 1, chunk], {"sp_0": z_up}
        )

    def down(step, chunk, slot):
        ref = kv.at[slot, chunk]
        return remote(
            ref, ref, kv_send.at[1, chunk], kv_recv.at[1, step - 1, chunk], {"sp_0": z_down}
        )

    @pl.when(z < NZ - 1)
    def _():
        for chunk in range(CHUNKS):
            up(1, chunk, z).start()

    @pl.when(z < HALF)
    def _():
        for chunk in range(CHUNKS):
            down(1, chunk, z).start()

    with jax.named_scope("proj_q"):
        loads[4].wait()
        loads[5].wait()
        qbuf[y] = dot(wq[...].reshape(2 * head_qk, wq.shape[2]), h, ((1,), (1,))).astype(BF16)

    def q_copy(off, slot):
        return remote(
            qbuf.at[slot], qbuf.at[slot], q_send.at[0], q_recv.at[0], {"sp_1": y_at[off]}
        )

    def all_of(ref, send_sem, recv_sem):
        return remote(ref, ref, send_sem, recv_sem, {"tp": sibling})

    for off in (2, 1, 3):
        q_copy(off, y).start()

    def gather_ops(buf, send, recv, dsend, drecv):
        def piece_of(direction, order):
            return direction if order != 1 else 1 - direction

        def hop(direction, order, slot):
            ref = buf.at[slot, piece_of(direction, order)]
            to = tp_at[1] if direction == 0 else tp_at[3]
            return remote(ref, ref, send.at[0], recv.at[order], {"tp": to})

        def across(piece, slot):
            ref = buf.at[slot, piece]
            return remote(ref, ref, dsend.at[0], drecv.at[0], {"tp": sibling})

        def came(direction):
            return tp_at[3] if direction == 0 else tp_at[1]

        def start_own():
            for order in range(2):
                for direction in range(2):
                    hop(direction, order, t).start()
            for piece in range(2):
                across(piece, t).start()

        def take(order):
            all_of(buf.at[0], send.at[0], recv.at[order]).wait_recv()
            for direction in range(2):
                slot = tp_at[2] if order == 2 else came(direction)
                if order == 0:
                    hop(direction, 2, slot).start()
                across(piece_of(direction, order), slot).start()

        def take_across():
            all_of(buf.at[0:4], dsend.at[0], drecv.at[0]).wait_recv()

        def drain():
            all_of(buf.at[0:3], send.at[0], recv.at[0]).wait_send()
            all_of(buf.at[0:4], dsend.at[0], drecv.at[0]).wait_send()

        return start_own, take, take_across, drain

    wo_start, wo_take, wo_take_across, wo_drain = gather_ops(wo, wo_send, wo_recv, wo_dsend, wo_drecv)

    def nb_copy(off, slot):
        ref = nb.at[slot]
        return remote(ref, ref, nb_send.at[0], nb_recv.at[off - 1], {"tp": tp_at[off]})

    def nb_across(slot):
        ref = nb.at[slot]
        return remote(ref, ref, nb_dsend.at[0], nb_drecv.at[0], {"tp": sibling})

    def nb_start():
        for off in (2, 1, 3):
            nb_copy(off, t).start()
        nb_across(t).start()

    def nb_take():
        for off in (1, 3, 2):
            slot = tp_at[(NX - off) % NX]
            nb_copy(off, slot).wait_recv()
            nb_across(slot).start()

    loads[6].wait()
    wo_start()

    def pass_on(step, chunk):
        low, high = (z + NZ - step) % NZ, (z + step) % NZ

        @pl.when(z >= step)
        def _():
            up(step, chunk, low).wait_recv()

            @pl.when((z < NZ - 1) & ((step < HALF - 1) | (chunk < CHUNKS // 2)))
            def _():
                up(step, chunk, low).wait_send()
                up(step + 1, chunk, low).start()

        @pl.when(high < HALF)
        def _():
            down(step, chunk, high).wait_recv()

            @pl.when((step < HALF - 1) | (chunk >= CHUNKS // 2))
            def _():
                @pl.when((z + step - 1) % NZ < HALF)
                def _():
                    down(step, chunk, high).wait_send()

                down(step + 1, chunk, high).start()

    with jax.named_scope("first_pass"):
        for chunk in range(CHUNKS):
            pass_on(1, chunk)

    with jax.named_scope("wait_q"):
        all_of(qbuf.at[0 : NY - 1], q_send.at[0], q_recv.at[0]).wait_recv()

    def split_queries(block, _):
        q = qbuf[block].astype(F32) * scale
        high = q.astype(BF16)
        low = (q - high.astype(F32)).astype(BF16)
        nothing = jnp.zeros((head_qk, rows), BF16)
        qz[0, block] = jnp.concatenate((high[:head_qk], nothing, low[:head_qk], nothing), axis=0)
        qz[1, block] = jnp.concatenate((nothing, high[head_qk:], nothing, low[head_qk:]), axis=0)
        return 0

    with jax.named_scope("split_q"):
        lax.fori_loop(0, NY, split_queries, 0)

    def block_of(slot):
        keys = jnp.concatenate((kv[slot, 0], kv[slot, 1]), axis=0)
        return (
            jnp.concatenate((keys, keys), axis=1),
            jnp.concatenate((kv[slot, 2], kv[slot, 3]), axis=1),
        )

    groups = rows // 8

    def allowed(block):
        k_pos = y * rows + lax.broadcasted_iota(jnp.int32, (rows, rows), 0)
        q_pos = block * rows + lax.broadcasted_iota(jnp.int32, (rows, rows), 1)
        return k_pos <= q_pos

    def score(unit, keys, own=False):
        pick, block = unit
        found = [dot(one, qz[pick, block]) for one in keys]
        if own:
            found = [jnp.where(allowed(block), one, masked_score) for one in found]
        highest = None
        for one in found:
            top = jnp.max(one.reshape(groups, 8, rows), axis=0)
            highest = top if highest is None else jnp.maximum(highest, top)
        return found, highest

    def keep(ahead):
        found, highest = ahead
        for index, one in enumerate(found):
            ahead_ref[index] = one
        ahead_max[...] = highest

    def absorb(unit, vals, found, highest, own=False):
        pick, block = unit
        now = jnp.broadcast_to(jnp.max(highest, axis=0, keepdims=True), (8, rows))
        if not own:
            before = m_ref[pick, block]
            now = jnp.maximum(before, now)
            rescale = jnp.exp2(before - now)
        total = None
        parts = []
        for one in found:
            part = jnp.exp2(one.reshape(groups, 8, rows) - now[None])
            if own:
                part = jnp.where(allowed(block).reshape(groups, 8, rows), part, 0.0)
            summed = jnp.sum(part, axis=0)
            total = summed if total is None else total + summed
            parts.append(part.reshape(rows, rows).astype(BF16))
        added = dot(vals, jnp.concatenate(parts, axis=0))
        m_ref[pick, block] = now
        if own:
            l_ref[pick, block] = total
            acc_ref[pick, block] = added
        else:
            l_ref[pick, block] = l_ref[pick, block] * rescale + total
            kept = acc_ref[pick, block].reshape(head_v // 8, 8, rows) * rescale[None]
            acc_ref[pick, block] = kept.reshape(head_v, rows) + added

    def attend(blocks, slots, own=False, carried=False, then=None):
        keys, vals = zip(*[block_of(slot) for slot in slots])
        vals = jnp.concatenate(vals, axis=1)
        units = [(pick, block) for block in blocks for pick in range(2)]
        if carried:
            ahead = ([ahead_ref[index] for index in range(len(slots))], ahead_max[...])
        else:
            ahead = score(units[0], keys, own)
        for index, unit in enumerate(units):
            here = ahead
            if index + 1 < len(units):
                ahead = score(units[index + 1], keys, own)
            elif then is not None:
                next_block, next_slots = then
                keep(score((0, next_block), [block_of(slot)[0] for slot in next_slots]))
            absorb(unit, vals, *here, own)

    def attend_pair(step, part):
        low, high = (z + NZ - step) % NZ, (z + step) % NZ
        blocks = (2 * part, 2 * part + 1)
        final = (step == HALF - 1) & (part == 1)

        @pl.when(z >= NZ - step)
        def _():
            @pl.when((z == NZ - step) & (part == 0))
            def _():
                keep(score((0, blocks[0]), [block_of(low)[0], block_of(high)[0]]))

            @pl.when(jnp.logical_not(final))
            def _():
                next_slots = ((z + NZ - step - part) % NZ, (z + step + part) % NZ)
                attend(blocks, (low, high), carried=True, then=(2 - 2 * part, next_slots))

            @pl.when(final)
            def _():
                attend(blocks, (low, high), carried=True)

        @pl.when((z >= step) & (z < NZ - step))
        def _():
            attend(blocks, (low,))

    opposite = (z + HALF) % NZ

    def o_copy(direction, piece, slot):
        to = y_at[1] if direction == 0 else y_at[3]
        return remote(
            opart.at[slot, piece], orecv.at[piece, direction],
            o_send.at[0], o_recv.at[piece], {"sp_1": to},
        )

    def rel_copy(direction, slot):
        to = y_at[1] if direction == 0 else y_at[3]
        return remote(
            opart.at[slot, direction], relay.at[direction],
            o_send.at[0], rel_recv.at[direction], {"sp_1": to},
        )

    def rel_forward(direction):
        to = y_at[1] if direction == 0 else y_at[3]
        return remote(
            relay.at[direction], orecv.at[direction, 2],
            o_send.at[0], o_recv.at[direction], {"sp_1": to},
        )

    def st_copy(off, slot):
        return remote(
            stats.at[slot], strecv.at[off], st_send.at[0], st_recv.at[0], {"sp_1": y_at[off]}
        )

    def pack(block):
        table = []
        for pick in range(2):
            table.append(m_ref[pick, block][:1])
            table.append(jnp.sum(l_ref[pick, block], axis=0, keepdims=True))
            part = acc_ref[pick, block].astype(BF16)
            for piece in range(2):
                span = slice(piece * half_rows, (piece + 1) * half_rows)
                opart[block, piece, pick * head_v : (pick + 1) * head_v] = part[:, span]
        table.append(jnp.zeros((4, rows), F32))
        stats[block] = jnp.concatenate(table, axis=0)

    def finish_send(late):
        if late:

            @pl.when(z >= HALF)
            def _():
                attend((y_at[2], y_at[1]), (opposite,))

        pack(y_at[2])
        rel_copy(0, y_at[2]).start()
        rel_copy(1, y_at[2]).start()
        st_copy(2, y_at[2]).start()
        pack(y_at[1])
        o_copy(0, 0, y_at[1]).start()
        o_copy(0, 1, y_at[1]).start()
        st_copy(1, y_at[1]).start()
        if late:

            @pl.when(z >= HALF)
            def _():
                attend((y_at[3], y_at[0]), (opposite,))

        pack(y_at[3])
        o_copy(1, 0, y_at[3]).start()
        o_copy(1, 1, y_at[3]).start()
        st_copy(3, y_at[3]).start()
        pack(y_at[0])

    def finish_relay():
        for direction in range(2):
            rel_copy(direction, y_at[2]).wait_recv()
            rel_forward(direction).start()

    def finish_combine():
        all_of(strecv.at[1:NY], st_send.at[0], st_recv.at[0]).wait_recv()
        lam = lam_ref[0]
        tables = [stats[y], strecv[1], strecv[3], strecv[2]]
        coefs = []
        for pick in range(2):
            maxima = [table[2 * pick : 2 * pick + 1] for table in tables]
            sums = [table[2 * pick + 1 : 2 * pick + 2] for table in tables]
            highest = maxima[0]
            for other in maxima[1:]:
                highest = jnp.maximum(highest, other)
            shares = [jnp.exp2(one - highest) for one in maxima]
            total = shares[0] * sums[0]
            for share, one in zip(shares[1:], sums[1:]):
                total = total + share * one
            factor = (1.0 if pick == 0 else -lam) / total
            coefs.append([share * factor for share in shares])
        gain = gain_ref[...].reshape(1, head_v)
        for piece in range(2):
            all_of(orecv.at[piece], o_send.at[0], o_recv.at[piece]).wait_recv()
            span = slice(piece * half_rows, (piece + 1) * half_rows)
            mixed = None
            for pick in range(2):
                parts = [acc_ref[pick, y][:, span]]
                for source in range(3):
                    one = orecv[piece, source, pick * head_v : (pick + 1) * head_v]
                    parts.append(one.astype(F32))
                for part, coef in zip(parts, coefs[pick]):
                    term = part * coef[:, span]
                    mixed = term if mixed is None else mixed + term
            spread = lax.rsqrt(jnp.mean(mixed * mixed, axis=0, keepdims=True) + epsilon)
            nb[t, piece] = ((mixed * spread).T * gain).astype(BF16)
        nb_start()

    def finish_gather():
        nb_take()

    loads[7].wait()
    loads[8].wait()

    def ring_step(index, _):
        step, part = index // 2, index % 2

        def pass_one(chunk):
            @pl.when(step < HALF)
            def _():
                with jax.named_scope("pass_on"):
                    pass_on(step, chunk)

        pass_one(2 * part)

        @pl.when(step == 2)
        def _():
            attend((2 * part, 2 * part + 1), (z,), own=True)

        pass_one(2 * part + 1)
        with jax.named_scope("attend_pair"):
            attend_pair(step - 1, part)

        @pl.when(index == 8)
        def _():
            wo_take(0)

        @pl.when(index == 12)
        def _():
            wo_take(1)

        for at, phase in ((5, lambda: finish_send(False)), (7, finish_relay), (10, finish_combine), (14, finish_gather)):

            @pl.when((z == 0) & (index == at))
            def _(phase=phase):
                phase()

        return 0

    with jax.named_scope("ring"):
        lax.fori_loop(4, 2 * HALF + 2, ring_step, 0)

    with jax.named_scope("last_wait"):

        @pl.when(z >= HALF)
        def _():
            for chunk in range(CHUNKS):
                if chunk < CHUNKS // 2:
                    up(HALF, chunk, opposite).wait_recv()
                else:
                    down(HALF, chunk, opposite).wait_recv()

    @pl.when(z > 0)
    def _():
        with jax.named_scope("finish_send"):
            finish_send(True)
        with jax.named_scope("finish_relay"):
            finish_relay()

    with jax.named_scope("drain_ring"):
        for chunk in range(CHUNKS):

            @pl.when(z < NZ - 1)
            def _(chunk=chunk):
                up(1, chunk, z).wait_send()

            @pl.when((z < HALF) | (z > HALF + 1) | ((z == HALF + 1) & (chunk >= CHUNKS // 2)))
            def _(chunk=chunk):
                down(1, chunk, z).wait_send()

        all_of(qbuf.at[0 : NY - 1], q_send.at[0], q_recv.at[0]).wait_send()

    with jax.named_scope("wo_far"):
        wo_take(2)

    @pl.when(z > 0)
    def _():
        with jax.named_scope("finish_combine"):
            finish_combine()

    with jax.named_scope("drain_parts"):
        all_of(stats.at[0 : NY - 1], st_send.at[0], st_recv.at[0]).wait_send()
        all_of(opart, o_send.at[0], o_recv.at[0]).wait_send()
        wo_take_across()
        wo_drain()

    @pl.when(z > 0)
    def _():
        with jax.named_scope("finish_gather"):
            finish_gather()

    with jax.named_scope("take_across"):
        all_of(nb.at[0:4], nb_dsend.at[0], nb_drecv.at[0]).wait_recv()

    with jax.named_scope("out_proj"):
        lhs = jnp.concatenate([nb[head].reshape(rows, head_v) for head in range(2 * NX)], axis=1)
        width = 256
        for left in range(0, out_ref.shape[1], width):
            rhs = wo[:, :, :, left : left + width].reshape(2 * NX * head_v, width)
            out_ref[:, left : left + width] = dot(lhs, rhs).astype(BF16)

    with jax.named_scope("drain"):
        all_of(nb.at[0:3], nb_send.at[0], nb_recv.at[0]).wait_send()
        all_of(nb.at[0:4], nb_dsend.at[0], nb_drecv.at[0]).wait_send()


def shards(
    hidden_in, query_one, query_two, key_one, key_two, value_proj, lambdas, norm_gain, out_proj
):
    rows, depth = hidden_in.shape
    head_qk = query_one.shape[1]
    head_v = value_proj.shape[1]
    half = rows // 2
    heads = 2 * NX
    dma = pltpu.SemaphoreType.DMA
    scratch = [
        pltpu.VMEM((rows, depth), BF16),
        pltpu.VMEM((2, head_qk, depth), BF16),
        pltpu.VMEM((2, head_qk, depth), BF16),
        pltpu.VMEM((depth, head_v), BF16),
        pltpu.SMEM((1,), F32),
        pltpu.VMEM((head_v,), F32),
        dma((9,)),
        pltpu.VMEM((NZ, CHUNKS, half, head_v), BF16),
        dma((2, CHUNKS)),
        dma((2, HALF, CHUNKS)),
        pltpu.VMEM((NY, 2 * head_qk, rows), BF16),
        pltpu.VMEM((2, NY, 4 * head_qk, rows), BF16),
        dma((1,)),
        dma((1,)),
        pltpu.VMEM((2, NY, 8, rows), F32),
        pltpu.VMEM((2, NY, 8, rows), F32),
        pltpu.VMEM((2, NY, head_v, rows), F32),
        pltpu.VMEM((2, rows, rows), F32),
        pltpu.VMEM((8, rows), F32),
        pltpu.VMEM((NY, 2, 2 * head_v, half), BF16),
        pltpu.VMEM((NY, 8, rows), F32),
        pltpu.VMEM((2, 3, 2 * head_v, half), BF16),
        pltpu.VMEM((NY, 8, rows), F32),
        pltpu.VMEM((2, 2 * head_v, half), BF16),
        dma((1,)),
        dma((2,)),
        dma((2,)),
        dma((1,)),
        dma((1,)),
        pltpu.VMEM((heads, 2, head_v // 2, out_proj.shape[1]), BF16),
        dma((1,)),
        dma((3,)),
        dma((1,)),
        dma((1,)),
        pltpu.VMEM((heads, 2, half, head_v), BF16),
        dma((1,)),
        dma((3,)),
        dma((1,)),
        dma((1,)),
    ]
    return pl.pallas_call(
        kernel,
        out_shape=pltpu.VMEM((rows, out_proj.shape[1]), BF16),
        in_specs=[pl.BlockSpec(memory_space=pltpu.HBM)] * 9,
        out_specs=pl.BlockSpec(memory_space=pltpu.VMEM),
        scratch_shapes=scratch,
        compiler_params=pltpu.CompilerParams(
            collective_id=0, has_side_effects=True, vmem_limit_bytes=60 * 1024 * 1024
        ),
    )(
        hidden_in, query_one.T, query_two.T, key_one.T, key_two.T, value_proj, lambdas, norm_gain,
        out_proj.reshape(2, head_v // 2, out_proj.shape[1]),
    )


def solution(mesh):
    torus = Mesh(mesh.devices.reshape(NZ, NY, mesh.shape["tp"]), ("sp_0", "sp_1", "tp"))
    placed = (
        P(SP, None),
        P(None, "tp"),
        P(None, "tp"),
        P(None, "tp"),
        P(None, "tp"),
        P(None, "tp"),
        P("tp"),
        P(),
        P("tp", None),
    )
    return jax.shard_map(
        shards, mesh=torus, in_specs=placed, out_specs=P(SP, None), check_vma=False
    )
```

```python
import math

import jax
import jax.numpy as jnp
from jax import lax
from jax.experimental import pallas as pl
from jax.experimental.pallas import tpu as pltpu
from jax.sharding import Mesh
from jax.sharding import PartitionSpec as P

SP = ("sp_0", "sp_1")
F32 = jnp.float32
BF16 = jnp.bfloat16
MESH = pl.DeviceIdType.MESH

epsilon = 1e-06
masked_score = -1e30

NZ = 16
NY = 4
NX = 4
HALF = NZ // 2
CHUNKS = 4
FAR = 2


def kernel(
    hidden_hbm, wq1_hbm, wq2_hbm, wk1_hbm, wk2_hbm, wv_hbm, lam_hbm, gain_hbm, wo_hbm,
    out_ref,
    hid, wq, wk, wv, lam_ref, gain_ref, load_sem,
    kv, kv_send, kv_recv,
    qbuf, qz, q_send, q_recv,
    m_ref, l_ref, acc_ref, ahead_ref, ahead_max,
    opart, stats, orecv, strecv, relay, o_send, o_recv, rel_send, rel_recv, st_send, st_recv,
    wo, wo_send, wo_recv, wo_dsend, wo_drecv,
    nb, nb_send, nb_recv, nb_dsend, nb_drecv,
    out_acc,
):
    z = lax.axis_index("sp_0")
    y = lax.axis_index("sp_1")
    t = lax.axis_index("tp")
    x = t // 2
    core = t % 2
    rows = hid.shape[0]
    head_qk = wq.shape[1]
    head_v = wv.shape[1]
    half_rows = rows // 2
    scale = 1.75 * head_qk ** (-0.5) * math.log2(math.e)

    z_up, z_down = (z + 1) % NZ, (z + NZ - 1) % NZ
    y_at = [y, (y + 1) % NY, (y + 2) % NY, (y + 3) % NY]
    x_at = [x, (x + 1) % NX, (x + 2) % NX, (x + 3) % NX]
    tp_at = [2 * xx + core for xx in x_at]
    sibling = 2 * x + (1 - core)

    loads = [
        pltpu.make_async_copy(hidden_hbm, hid, load_sem.at[0]),
        pltpu.make_async_copy(wk1_hbm, wk.at[0], load_sem.at[1]),
        pltpu.make_async_copy(wk2_hbm, wk.at[1], load_sem.at[2]),
        pltpu.make_async_copy(wv_hbm, wv, load_sem.at[3]),
        pltpu.make_async_copy(wq1_hbm, wq.at[0], load_sem.at[4]),
        pltpu.make_async_copy(wq2_hbm, wq.at[1], load_sem.at[5]),
        pltpu.make_async_copy(wo_hbm, wo.at[t], load_sem.at[6]),
        pltpu.make_async_copy(gain_hbm, gain_ref, load_sem.at[7]),
        pltpu.make_async_copy(lam_hbm, lam_ref, load_sem.at[8]),
    ]
    for load in loads:
        load.start()

    barrier = pltpu.get_barrier_semaphore()
    partners = [
        {"sp_0": z_up}, {"sp_0": z_down},
        {"sp_1": y_at[1]}, {"sp_1": y_at[2]}, {"sp_1": y_at[3]},
        {"sp_1": y_at[1], "tp": sibling}, {"sp_1": y_at[3], "tp": sibling},
        {"tp": tp_at[1]}, {"tp": tp_at[2]}, {"tp": tp_at[3]}, {"tp": sibling},
    ]
    for partner in partners:
        pl.semaphore_signal(barrier, inc=1, device_id=partner, device_id_type=MESH)

    def remote(src, dst, send_sem, recv_sem, device):
        return pltpu.make_async_remote_copy(
            src_ref=src, dst_ref=dst, send_sem=send_sem, recv_sem=recv_sem,
            device_id=device, device_id_type=MESH,
        )

    def dot(a, b, dims=((1,), (0,))):
        return lax.dot_general(a, b, (dims, ((), ())), preferred_element_type=F32)

    def up(step, chunk, slot):
        ref = kv.at[slot, chunk]
        return remote(
            ref, ref, kv_send.at[0, chunk], kv_recv.at[0, step - 1, chunk], {"sp_0": z_up}
        )

    def down(step, chunk, slot):
        ref = kv.at[slot, chunk]
        return remote(
            ref, ref, kv_send.at[1, chunk], kv_recv.at[1, step - 1, chunk], {"sp_0": z_down}
        )

    def start_ring(chunks):
        @pl.when(z < NZ - 1)
        def _():
            for chunk in chunks:
                up(1, chunk, z).start()

        @pl.when(z < HALF)
        def _():
            for chunk in chunks:
                down(1, chunk, z).start()

    with jax.named_scope("load_kv"):
        for load in loads[:3]:
            load.wait()
    with jax.named_scope("proj_k"):
        h = hid[...]
        k = dot(h, wk[...].reshape(2 * head_qk, wk.shape[2]), ((1,), (1,))).astype(BF16)
        kv[z, 0] = k[:half_rows]
        kv[z, 1] = k[half_rows:]
    with jax.named_scope("entry_barrier"):
        pl.semaphore_wait(barrier, len(partners))
    start_ring((0, 1))
    with jax.named_scope("proj_v"):
        loads[3].wait()
        v = dot(h, wv[...]).T.astype(BF16)
        kv[z, 2] = v[:, :half_rows]
        kv[z, 3] = v[:, half_rows:]
    start_ring((2, 3))

    with jax.named_scope("proj_q"):
        loads[4].wait()
        loads[5].wait()
        qbuf[y] = dot(wq[...].reshape(2 * head_qk, wq.shape[2]), h, ((1,), (1,))).astype(BF16)

    def q_copy(off, slot):
        return remote(
            qbuf.at[slot], qbuf.at[slot], q_send.at[0], q_recv.at[off - 1], {"sp_1": y_at[off]}
        )

    def all_of(ref, send_sem, recv_sem):
        return remote(ref, ref, send_sem, recv_sem, {"tp": sibling})

    for off in (3, 2, 1):
        q_copy(off, y).start()

    def gather_ops(buf, send, recv, dsend, drecv):
        def piece_of(direction, order):
            return direction if order != 1 else 1 - direction

        def hop(direction, order, slot):
            ref = buf.at[slot, piece_of(direction, order)]
            to = tp_at[1] if direction == 0 else tp_at[3]
            return remote(ref, ref, send.at[0], recv.at[order], {"tp": to})

        def across(piece, slot):
            ref = buf.at[slot, piece]
            return remote(ref, ref, dsend.at[0], drecv.at[0], {"tp": sibling})

        def came(direction):
            return tp_at[3] if direction == 0 else tp_at[1]

        def start_own():
            for order in range(2):
                for direction in range(2):
                    hop(direction, order, t).start()
            for piece in range(2):
                across(piece, t).start()

        def take(order):
            all_of(buf.at[0], send.at[0], recv.at[order]).wait_recv()
            for direction in range(2):
                slot = tp_at[2] if order == 2 else came(direction)
                if order == 0:
                    hop(direction, 2, slot).start()
                across(piece_of(direction, order), slot).start()

        def take_across():
            all_of(buf.at[0:4], dsend.at[0], drecv.at[0]).wait_recv()

        def drain():
            all_of(buf.at[0:3], send.at[0], recv.at[0]).wait_send()
            all_of(buf.at[0:4], dsend.at[0], drecv.at[0]).wait_send()

        return start_own, take, take_across, drain

    wo_start, wo_take, wo_take_across, wo_drain = gather_ops(wo, wo_send, wo_recv, wo_dsend, wo_drecv)

    def nb_copy(off, slot):
        ref = nb.at[slot]
        return remote(ref, ref, nb_send.at[0], nb_recv.at[off - 1], {"tp": tp_at[off]})

    def nb_across(slot):
        ref = nb.at[slot]
        return remote(ref, ref, nb_dsend.at[0], nb_drecv.at[0], {"tp": sibling})

    def nb_start():
        for off in (2, 1, 3):
            nb_copy(off, t).start()
        nb_across(t).start()

    def nb_take():
        for off in (1, 3, 2):
            slot = tp_at[(NX - off) % NX]
            nb_copy(off, slot).wait_recv()
            nb_across(slot).start()

    loads[6].wait()
    wo_start()

    def pass_on(step, chunk):
        low, high = (z + NZ - step) % NZ, (z + step) % NZ

        @pl.when(z >= step)
        def _():
            up(step, chunk, low).wait_recv()

            @pl.when((z < NZ - 1) & ((step < HALF - 1) | (chunk < CHUNKS // 2)))
            def _():
                up(step, chunk, low).wait_send()
                up(step + 1, chunk, low).start()

        @pl.when(high < HALF)
        def _():
            down(step, chunk, high).wait_recv()

            @pl.when((step < HALF - 1) | (chunk >= CHUNKS // 2))
            def _():
                @pl.when((z + step - 1) % NZ < HALF)
                def _():
                    down(step, chunk, high).wait_send()

                down(step + 1, chunk, high).start()

    with jax.named_scope("first_pass"):
        for chunk in range(CHUNKS):
            pass_on(1, chunk)

    def split_queries(block):
        q = qbuf[block].astype(F32) * scale
        high = q.astype(BF16)
        low = (q - high.astype(F32)).astype(BF16)
        nothing = jnp.zeros((head_qk, rows), BF16)
        qz[0, block] = jnp.concatenate((high[:head_qk], nothing, low[:head_qk], nothing), axis=0)
        qz[1, block] = jnp.concatenate((nothing, high[head_qk:], nothing, low[head_qk:]), axis=0)

    def take_queries(first):
        if first:
            q_copy(3, y_at[1]).wait_recv()
        else:
            q_copy(2, y_at[2]).wait_recv()
            q_copy(1, y_at[3]).wait_recv()
        for off in (0, 1) if first else (2, 3):
            split_queries(y_at[off])


    def block_of(slot):
        keys = jnp.concatenate((kv[slot, 0], kv[slot, 1]), axis=0)
        return (
            jnp.concatenate((keys, keys), axis=1),
            jnp.concatenate((kv[slot, 2], kv[slot, 3]), axis=1),
        )

    groups = rows // 8

    def allowed(block):
        k_pos = y * rows + lax.broadcasted_iota(jnp.int32, (rows, rows), 0)
        q_pos = block * rows + lax.broadcasted_iota(jnp.int32, (rows, rows), 1)
        return k_pos <= q_pos

    def score(unit, keys, own=False):
        pick, block = unit
        found = [dot(one, qz[pick, block]) for one in keys]
        if own:
            found = [jnp.where(allowed(block), one, masked_score) for one in found]
        highest = None
        for one in found:
            top = jnp.max(one.reshape(groups, 8, rows), axis=0)
            highest = top if highest is None else jnp.maximum(highest, top)
        return found, highest

    def keep(ahead):
        found, highest = ahead
        for index, one in enumerate(found):
            ahead_ref[index] = one
        ahead_max[...] = highest

    def absorb(unit, vals, found, highest, own=False):
        pick, block = unit
        now = jnp.broadcast_to(jnp.max(highest, axis=0, keepdims=True), (8, rows))
        if not own:
            before = m_ref[pick, block]
            now = jnp.maximum(before, now)
            rescale = jnp.exp2(before - now)
        total = None
        parts = []
        for one in found:
            part = jnp.exp2(one.reshape(groups, 8, rows) - now[None])
            if own:
                part = jnp.where(allowed(block).reshape(groups, 8, rows), part, 0.0)
            summed = jnp.sum(part, axis=0)
            total = summed if total is None else total + summed
            parts.append(part.reshape(rows, rows).astype(BF16))
        added = dot(vals, jnp.concatenate(parts, axis=0))
        m_ref[pick, block] = now
        if own:
            l_ref[pick, block] = total
            acc_ref[pick, block] = added
        else:
            l_ref[pick, block] = l_ref[pick, block] * rescale + total
            kept = acc_ref[pick, block].reshape(head_v // 8, 8, rows) * rescale[None]
            acc_ref[pick, block] = kept.reshape(head_v, rows) + added

    def attend(blocks, slots, own=False, carried=False, then=None):
        keys, vals = zip(*[block_of(slot) for slot in slots])
        vals = jnp.concatenate(vals, axis=1)
        units = [(pick, block) for block in blocks for pick in range(2)]
        if carried:
            ahead = ([ahead_ref[index] for index in range(len(slots))], ahead_max[...])
        else:
            ahead = score(units[0], keys, own)
        for index, unit in enumerate(units):
            here = ahead
            if index + 1 < len(units):
                ahead = score(units[index + 1], keys, own)
            elif then is not None:
                next_block, next_slots = then
                keep(score((0, next_block), [block_of(slot)[0] for slot in next_slots]))
            absorb(unit, vals, *here, own)

    def attend_pair(step, part):
        low, high = (z + NZ - step) % NZ, (z + step) % NZ
        blocks = ((y + 2 * part) % NY, (y + 2 * part + 1) % NY)
        final = (step == HALF - 1) & (part == 1)

        @pl.when(z >= NZ - step)
        def _():
            @pl.when((z == NZ - step) & (part == 0))
            def _():
                keep(score((0, blocks[0]), [block_of(low)[0], block_of(high)[0]]))

            @pl.when(jnp.logical_not(final))
            def _():
                next_slots = ((z + NZ - step - part) % NZ, (z + step + part) % NZ)
                attend(blocks, (low, high), carried=True, then=((y + 2 - 2 * part) % NY, next_slots))

            @pl.when(final)
            def _():
                attend(blocks, (low, high), carried=True)

        @pl.when((z >= step) & (z < NZ - step))
        def _():
            attend(blocks, (low,))

    opposite = (z + HALF) % NZ

    def o_copy(direction, piece, slot):
        to = y_at[1] if direction == 0 else y_at[3]
        return remote(
            opart.at[slot, piece], orecv.at[piece, direction],
            o_send.at[0], o_recv.at[piece], {"sp_1": to},
        )

    def rel_copy(head, direction, slot):
        to = y_at[1] if direction == 0 else y_at[3]
        return remote(
            opart.at[slot, direction], relay.at[head, direction],
            o_send.at[0], rel_recv.at[head, direction], {"sp_1": to, "tp": 2 * x + 1},
        )

    def rel_forward(head, direction):
        to = y_at[1] if direction == 0 else y_at[3]
        return remote(
            relay.at[head, direction], orecv.at[direction, 2],
            rel_send.at[head], o_recv.at[direction], {"sp_1": to, "tp": 2 * x + head},
        )

    def st_copy(off, slot):
        return remote(
            stats.at[slot], strecv.at[off], st_send.at[0], st_recv.at[0], {"sp_1": y_at[off]}
        )

    def pack(block):
        table = []
        for pick in range(2):
            table.append(m_ref[pick, block][:1])
            table.append(jnp.sum(l_ref[pick, block], axis=0, keepdims=True))
            part = acc_ref[pick, block].astype(BF16)
            for piece in range(2):
                span = slice(piece * half_rows, (piece + 1) * half_rows)
                opart[block, piece, pick * head_v : (pick + 1) * head_v] = part[:, span]
        table.append(jnp.zeros((4, rows), F32))
        stats[block] = jnp.concatenate(table, axis=0)

    def finish_send(late):
        if late:

            @pl.when(z >= HALF)
            def _():
                attend((y_at[2], y_at[1]), (opposite,))

        pack(y_at[2])
        rel_copy(core, 0, y_at[2]).start()
        rel_copy(core, 1, y_at[2]).start()
        st_copy(2, y_at[2]).start()
        pack(y_at[1])
        o_copy(0, 0, y_at[1]).start()
        o_copy(0, 1, y_at[1]).start()
        st_copy(1, y_at[1]).start()
        if late:

            @pl.when(z >= HALF)
            def _():
                attend((y_at[3], y_at[0]), (opposite,))

        pack(y_at[3])
        o_copy(1, 0, y_at[3]).start()
        o_copy(1, 1, y_at[3]).start()
        st_copy(3, y_at[3]).start()
        pack(y_at[0])

    def finish_relay(head):
        @pl.when(core == 1)
        def _():
            for direction in range(2):
                rel_copy(head, direction, y_at[2]).wait_recv()
                rel_forward(head, direction).start()

    def finish_combine():
        all_of(strecv.at[1:NY], st_send.at[0], st_recv.at[0]).wait_recv()
        lam = lam_ref[0]
        tables = [stats[y], strecv[1], strecv[3], strecv[2]]
        coefs = []
        for pick in range(2):
            maxima = [table[2 * pick : 2 * pick + 1] for table in tables]
            sums = [table[2 * pick + 1 : 2 * pick + 2] for table in tables]
            highest = maxima[0]
            for other in maxima[1:]:
                highest = jnp.maximum(highest, other)
            shares = [jnp.exp2(one - highest) for one in maxima]
            total = shares[0] * sums[0]
            for share, one in zip(shares[1:], sums[1:]):
                total = total + share * one
            factor = (1.0 if pick == 0 else -lam) / total
            coefs.append([share * factor for share in shares])
        gain = gain_ref[...].reshape(1, head_v)
        for piece in range(2):
            all_of(orecv.at[piece], o_send.at[0], o_recv.at[piece]).wait_recv()
            span = slice(piece * half_rows, (piece + 1) * half_rows)
            mixed = None
            for pick in range(2):
                parts = [acc_ref[pick, y][:, span]]
                for source in range(3):
                    one = orecv[piece, source, pick * head_v : (pick + 1) * head_v]
                    parts.append(one.astype(F32))
                for part, coef in zip(parts, coefs[pick]):
                    term = part * coef[:, span]
                    mixed = term if mixed is None else mixed + term
            spread = lax.rsqrt(jnp.mean(mixed * mixed, axis=0, keepdims=True) + epsilon)
            nb[t, piece] = ((mixed * spread).T * gain).astype(BF16)
        nb_start()

    loads[7].wait()
    loads[8].wait()

    def ring_step(index, _):
        step, part = index // 2, index % 2

        def pass_one(chunk):
            @pl.when(step < HALF)
            def _():
                with jax.named_scope("pass_on"):
                    pass_on(step, chunk)

        pass_one(2 * part)

        @pl.when(step == 2)
        def _():
            @pl.when(part == 0)
            def _():
                with jax.named_scope("take_q"):
                    take_queries(True)

            attend(((y + 2 * part) % NY, (y + 2 * part + 1) % NY), (z,), own=True)

        pass_one(2 * part + 1)

        @pl.when(index == 4)
        def _():
            with jax.named_scope("take_more_q"):
                take_queries(False)

        with jax.named_scope("attend_pair"):
            attend_pair(step - 1, part)

        @pl.when(index == 8)
        def _():
            wo_take(0)

        @pl.when(index == 12)
        def _():
            wo_take(1)

        @pl.when(index == 16)
        def _():
            wo_take(2)

        @pl.when((z == 0) & (index == 6))
        def _():
            finish_send(False)

        @pl.when((z == 0) & (index == 15))
        def _():
            finish_relay(1)
            finish_relay(0)

        return 0

    with jax.named_scope("ring"):
        lax.fori_loop(4, 2 * HALF + 2, ring_step, 0)

    with jax.named_scope("last_wait"):

        @pl.when(z >= HALF)
        def _():
            for chunk in range(CHUNKS):
                if chunk < CHUNKS // 2:
                    up(HALF, chunk, opposite).wait_recv()
                else:
                    down(HALF, chunk, opposite).wait_recv()

    @pl.when(z > 0)
    def _():
        with jax.named_scope("finish_send"):
            finish_send(True)
        with jax.named_scope("finish_relay"):
            finish_relay(1)

    with jax.named_scope("drain_ring"):
        for chunk in range(CHUNKS):

            @pl.when(z < NZ - 1)
            def _(chunk=chunk):
                up(1, chunk, z).wait_send()

            @pl.when((z < HALF) | (z > HALF + 1) | ((z == HALF + 1) & (chunk >= CHUNKS // 2)))
            def _(chunk=chunk):
                down(1, chunk, z).wait_send()

        all_of(qbuf.at[0 : NY - 1], q_send.at[0], q_recv.at[0]).wait_send()

    with jax.named_scope("finish_combine"):
        finish_combine()

    @pl.when(z > 0)
    def _():
        with jax.named_scope("relay_other"):
            finish_relay(0)

    with jax.named_scope("drain_parts"):
        all_of(stats.at[0 : NY - 1], st_send.at[0], st_recv.at[0]).wait_send()
        all_of(opart.at[0:3], o_send.at[0], o_recv.at[0]).wait_send()

        @pl.when(core == 1)
        def _():
            for head in range(2):
                all_of(relay.at[head], rel_send.at[head], o_recv.at[0]).wait_send()

        wo_take_across()
        wo_drain()

    def heads_across():
        all_of(nb.at[0:4], nb_dsend.at[0], nb_drecv.at[0]).wait_recv()

    def project_out(which):
        heads = [2 * chip + which for chip in range(NX)]
        lhs = jnp.concatenate([nb[head].reshape(rows, head_v) for head in heads], axis=1)
        width = 256
        for left in range(0, out_ref.shape[1], width):
            span = slice(left, left + width)
            rhs = jnp.concatenate([wo[head, :, :, span].reshape(head_v, width) for head in heads], axis=0)
            found = dot(lhs, rhs)
            if which == 1:
                out_acc[:, span] = found
            else:
                out_ref[:, span] = (out_acc[:, span] + found).astype(BF16)

    with jax.named_scope("gather_ones"):

        @pl.when(core == 1)
        def _():
            nb_take()

        @pl.when(core == 0)
        def _():
            heads_across()

    with jax.named_scope("out_ones"):
        project_out(1)

    with jax.named_scope("gather_zeros"):

        @pl.when(core == 0)
        def _():
            nb_take()

        @pl.when(core == 1)
        def _():
            heads_across()

    with jax.named_scope("out_zeros"):
        project_out(0)

    with jax.named_scope("drain"):
        all_of(nb.at[0:3], nb_send.at[0], nb_recv.at[0]).wait_send()
        all_of(nb.at[0:4], nb_dsend.at[0], nb_drecv.at[0]).wait_send()


def shards(
    hidden_in, query_one, query_two, key_one, key_two, value_proj, lambdas, norm_gain, out_proj
):
    rows, depth = hidden_in.shape
    head_qk = query_one.shape[1]
    head_v = value_proj.shape[1]
    half = rows // 2
    heads = 2 * NX
    dma = pltpu.SemaphoreType.DMA
    scratch = [
        pltpu.VMEM((rows, depth), BF16),
        pltpu.VMEM((2, head_qk, depth), BF16),
        pltpu.VMEM((2, head_qk, depth), BF16),
        pltpu.VMEM((depth, head_v), BF16),
        pltpu.SMEM((1,), F32),
        pltpu.VMEM((head_v,), F32),
        dma((9,)),
        pltpu.VMEM((NZ, CHUNKS, half, head_v), BF16),
        dma((2, CHUNKS)),
        dma((2, HALF, CHUNKS)),
        pltpu.VMEM((NY, 2 * head_qk, rows), BF16),
        pltpu.VMEM((2, NY, 4 * head_qk, rows), BF16),
        dma((1,)),
        dma((3,)),
        pltpu.VMEM((2, NY, 8, rows), F32),
        pltpu.VMEM((2, NY, 8, rows), F32),
        pltpu.VMEM((2, NY, head_v, rows), F32),
        pltpu.VMEM((2, rows, rows), F32),
        pltpu.VMEM((8, rows), F32),
        pltpu.VMEM((NY, 2, 2 * head_v, half), BF16),
        pltpu.VMEM((NY, 8, rows), F32),
        pltpu.VMEM((2, 3, 2 * head_v, half), BF16),
        pltpu.VMEM((NY, 8, rows), F32),
        pltpu.VMEM((2, 2, 2 * head_v, half), BF16),
        dma((1,)),
        dma((2,)),
        dma((2,)),
        dma((2, 2)),
        dma((1,)),
        dma((1,)),
        pltpu.VMEM((heads, 2, head_v // 2, out_proj.shape[1]), BF16),
        dma((1,)),
        dma((3,)),
        dma((1,)),
        dma((1,)),
        pltpu.VMEM((heads, 2, half, head_v), BF16),
        dma((1,)),
        dma((3,)),
        dma((1,)),
        dma((1,)),
        pltpu.VMEM((rows, out_proj.shape[1]), F32),
    ]
    return pl.pallas_call(
        kernel,
        out_shape=pltpu.VMEM((rows, out_proj.shape[1]), BF16),
        in_specs=[pl.BlockSpec(memory_space=pltpu.HBM)] * 9,
        out_specs=pl.BlockSpec(memory_space=pltpu.VMEM),
        scratch_shapes=scratch,
        compiler_params=pltpu.CompilerParams(
            collective_id=0, has_side_effects=True, vmem_limit_bytes=60 * 1024 * 1024
        ),
    )(
        hidden_in, query_one.T, query_two.T, key_one.T, key_two.T, value_proj, lambdas, norm_gain,
        out_proj.reshape(2, head_v // 2, out_proj.shape[1]),
    )


def solution(mesh):
    torus = Mesh(mesh.devices.reshape(NZ, NY, mesh.shape["tp"]), ("sp_0", "sp_1", "tp"))
    placed = (
        P(SP, None),
        P(None, "tp"),
        P(None, "tp"),
        P(None, "tp"),
        P(None, "tp"),
        P(None, "tp"),
        P("tp"),
        P(),
        P("tp", None),
    )
    return jax.shard_map(
        shards, mesh=torus, in_specs=placed, out_specs=P(SP, None), check_vma=False
    )
```

```python
import math

import jax
import jax.numpy as jnp
from jax import lax
from jax.experimental import pallas as pl
from jax.experimental.pallas import tpu as pltpu
from jax.sharding import Mesh
from jax.sharding import PartitionSpec as P

SP = ("sp_0", "sp_1")
F32 = jnp.float32
BF16 = jnp.bfloat16
MESH = pl.DeviceIdType.MESH

epsilon = 1e-06
masked_score = -1e30

NZ = 16
NY = 4
NX = 4
HALF = NZ // 2
CHUNKS = 4
FAR = 2


def kernel(
    hidden_hbm, wq1_hbm, wq2_hbm, wk1_hbm, wk2_hbm, wv_hbm, lam_hbm, gain_hbm, wo_hbm,
    out_ref,
    hid, wq, wk, wv, lam_ref, gain_ref, load_sem,
    kv, kv_send, kv_recv, give_send, give_recv,
    qbuf, qz, q_send, q_recv,
    m_ref, l_ref, acc_ref, ahead_ref, ahead_max,
    opart, stats, orecv, strecv, relay, o_send, o_recv, rel_send, rel_recv, st_send, st_recv,
    wo, wo_send, wo_recv, wo_dsend, wo_drecv,
    nb, nb_send, nb_recv, nb_dsend, nb_drecv,
    out_acc,
):
    z = lax.axis_index("sp_0")
    y = lax.axis_index("sp_1")
    t = lax.axis_index("tp")
    x = t // 2
    core = t % 2
    rows = hid.shape[0]
    head_qk = wq.shape[1]
    head_v = wv.shape[1]
    half_rows = rows // 2
    scale = 1.75 * head_qk ** (-0.5) * math.log2(math.e)

    z_up, z_down = (z + 1) % NZ, (z + NZ - 1) % NZ
    y_at = [y, (y + 1) % NY, (y + 2) % NY, (y + 3) % NY]
    x_at = [x, (x + 1) % NX, (x + 2) % NX, (x + 3) % NX]
    tp_at = [2 * xx + core for xx in x_at]
    sibling = 2 * x + (1 - core)

    loads = [
        pltpu.make_async_copy(hidden_hbm, hid, load_sem.at[0]),
        pltpu.make_async_copy(wk1_hbm, wk.at[0], load_sem.at[1]),
        pltpu.make_async_copy(wk2_hbm, wk.at[1], load_sem.at[2]),
        pltpu.make_async_copy(wv_hbm, wv, load_sem.at[3]),
        pltpu.make_async_copy(wq1_hbm, wq.at[0], load_sem.at[4]),
        pltpu.make_async_copy(wq2_hbm, wq.at[1], load_sem.at[5]),
        pltpu.make_async_copy(wo_hbm, wo.at[t], load_sem.at[6]),
        pltpu.make_async_copy(gain_hbm, gain_ref, load_sem.at[7]),
        pltpu.make_async_copy(lam_hbm, lam_ref, load_sem.at[8]),
    ]
    for load in loads[:3]:
        load.start()

    barrier = pltpu.get_barrier_semaphore()
    partners = [
        {"sp_0": z_up, "tp": sibling}, {"sp_0": z_down, "tp": sibling},
        {"sp_1": y_at[1]}, {"sp_1": y_at[2]}, {"sp_1": y_at[3]},
        {"sp_1": y_at[1], "tp": sibling}, {"sp_1": y_at[3], "tp": sibling},
        {"tp": tp_at[1]}, {"tp": tp_at[2]}, {"tp": tp_at[3]}, {"tp": sibling},
    ]
    for partner in partners:
        pl.semaphore_signal(barrier, inc=1, device_id=partner, device_id_type=MESH)
    for load in loads[3:]:
        load.start()

    def remote(src, dst, send_sem, recv_sem, device):
        return pltpu.make_async_remote_copy(
            src_ref=src, dst_ref=dst, send_sem=send_sem, recv_sem=recv_sem,
            device_id=device, device_id_type=MESH,
        )

    def dot(a, b, dims=((1,), (0,))):
        return lax.dot_general(a, b, (dims, ((), ())), preferred_element_type=F32)

    def hop_copy(direction, step, chunk, slot, to):
        return remote(
            kv.at[(step - 1) % 2, slot, chunk], kv.at[step % 2, slot, chunk],
            kv_send.at[direction, chunk], kv_recv.at[direction, step - 1, chunk],
            {"sp_0": to, "tp": sibling},
        )

    def up(step, chunk, slot):
        return hop_copy(0, step, chunk, slot, z_up)

    def down(step, chunk, slot):
        return hop_copy(1, step, chunk, slot, z_down)

    def give(direction, step, chunk, slot):
        return remote(
            kv.at[1, slot, chunk], kv.at[0, slot, chunk],
            give_send.at[direction, chunk], give_recv.at[direction, step // 2, chunk], {"tp": sibling},
        )

    def start_ring(chunks):
        @pl.when(z < NZ - 1)
        def _():
            for chunk in chunks:
                up(1, chunk, z).start()

        @pl.when(z < HALF)
        def _():
            for chunk in chunks:
                down(1, chunk, z).start()

    with jax.named_scope("load_kv"):
        for load in loads[:3]:
            load.wait()
    with jax.named_scope("proj_k"):
        h = hid[...]
        k = dot(h, wk[...].reshape(2 * head_qk, wk.shape[2]), ((1,), (1,))).astype(BF16)
        kv[0, z, 0] = k[:half_rows]
        kv[0, z, 1] = k[half_rows:]
    with jax.named_scope("entry_barrier"):
        pl.semaphore_wait(barrier, len(partners))
    start_ring((0, 1))
    with jax.named_scope("proj_v"):
        loads[3].wait()
        v = dot(h, wv[...]).T.astype(BF16)
        kv[0, z, 2] = v[:, :half_rows]
        kv[0, z, 3] = v[:, half_rows:]
    start_ring((2, 3))

    with jax.named_scope("proj_q"):
        loads[4].wait()
        loads[5].wait()
        qbuf[y] = dot(wq[...].reshape(2 * head_qk, wq.shape[2]), h, ((1,), (1,))).astype(BF16)

    def q_copy(off, slot):
        return remote(
            qbuf.at[slot], qbuf.at[slot], q_send.at[0], q_recv.at[off - 1], {"sp_1": y_at[off]}
        )

    def all_of(ref, send_sem, recv_sem):
        return remote(ref, ref, send_sem, recv_sem, {"tp": sibling})

    for off in (3, 2, 1):
        q_copy(off, y).start()

    def gather_ops(buf, send, recv, dsend, drecv):
        def piece_of(direction, order):
            return direction if order != 1 else 1 - direction

        def hop(direction, order, slot):
            ref = buf.at[slot, piece_of(direction, order)]
            to = tp_at[1] if direction == 0 else tp_at[3]
            return remote(ref, ref, send.at[0], recv.at[order], {"tp": to})

        def across(piece, slot):
            ref = buf.at[slot, piece]
            return remote(ref, ref, dsend.at[0], drecv.at[0], {"tp": sibling})

        def came(direction):
            return tp_at[3] if direction == 0 else tp_at[1]

        def start_own():
            for order in range(2):
                for direction in range(2):
                    hop(direction, order, t).start()
            for piece in range(2):
                across(piece, t).start()

        def take(order):
            all_of(buf.at[0], send.at[0], recv.at[order]).wait_recv()
            for direction in range(2):
                slot = tp_at[2] if order == 2 else came(direction)
                if order == 0:
                    hop(direction, 2, slot).start()
                across(piece_of(direction, order), slot).start()

        def take_across():
            all_of(buf.at[0:4], dsend.at[0], drecv.at[0]).wait_recv()

        def drain():
            all_of(buf.at[0:3], send.at[0], recv.at[0]).wait_send()
            all_of(buf.at[0:4], dsend.at[0], drecv.at[0]).wait_send()

        return start_own, take, take_across, drain

    wo_start, wo_take, wo_take_across, wo_drain = gather_ops(wo, wo_send, wo_recv, wo_dsend, wo_drecv)

    def nb_copy(off, slot):
        ref = nb.at[slot]
        return remote(ref, ref, nb_send.at[0], nb_recv.at[off - 1], {"tp": tp_at[off]})

    def nb_across(slot):
        ref = nb.at[slot]
        return remote(ref, ref, nb_dsend.at[0], nb_drecv.at[0], {"tp": sibling})

    def nb_start():
        for off in (2, 1, 3):
            nb_copy(off, t).start()
        nb_across(t).start()

    def nb_take():
        for off in (1, 3, 2):
            slot = tp_at[(NX - off) % NX]
            nb_copy(off, slot).wait_recv()
            nb_across(slot).start()

    loads[6].wait()
    wo_start()

    def pass_on(step, chunk):
        low, high = (z + NZ - step) % NZ, (z + step) % NZ

        @pl.when(z >= step)
        def _():
            up(step, chunk, low).wait_recv()

            @pl.when((z < NZ - 1) & ((step < HALF - 1) | (chunk < CHUNKS // 2)))
            def _():
                up(step, chunk, low).wait_send()
                up(step + 1, chunk, low).start()

            @pl.when(step % 2 == 1)
            def _():
                @pl.when(step > 2)
                def _():
                    give(0, step, chunk, low).wait_send()

                give(0, step, chunk, low).start()

        @pl.when(high < HALF)
        def _():
            down(step, chunk, high).wait_recv()

            @pl.when((step < HALF - 1) | (chunk >= CHUNKS // 2))
            def _():
                @pl.when((z + step - 1) % NZ < HALF)
                def _():
                    down(step, chunk, high).wait_send()

                down(step + 1, chunk, high).start()

            @pl.when((step % 2 == 1) & (z >= NZ - step))
            def _():
                @pl.when(z >= NZ - step + 2)
                def _():
                    give(1, step, chunk, high).wait_send()

                give(1, step, chunk, high).start()

    def take_given(step):
        low, high = (z + NZ - step) % NZ, (z + step) % NZ
        for chunk in range(CHUNKS):

            @pl.when(z >= step)
            def _(chunk=chunk):
                give(0, step, chunk, low).wait_recv()

            @pl.when(z >= NZ - step)
            def _(chunk=chunk):
                give(1, step, chunk, high).wait_recv()

    with jax.named_scope("first_pass"):
        for chunk in range(CHUNKS):
            pass_on(1, chunk)

    def split_queries(block):
        q = qbuf[block].astype(F32) * scale
        high = q.astype(BF16)
        low = (q - high.astype(F32)).astype(BF16)
        nothing = jnp.zeros((head_qk, rows), BF16)
        qz[0, block] = jnp.concatenate((high[:head_qk], nothing, low[:head_qk], nothing), axis=0)
        qz[1, block] = jnp.concatenate((nothing, high[head_qk:], nothing, low[head_qk:]), axis=0)

    def take_queries(first):
        if first:
            q_copy(3, y_at[1]).wait_recv()
        else:
            q_copy(2, y_at[2]).wait_recv()
            q_copy(1, y_at[3]).wait_recv()
        for off in (0, 1) if first else (2, 3):
            split_queries(y_at[off])


    def block_of(slot):
        keys = jnp.concatenate((kv[0, slot, 0], kv[0, slot, 1]), axis=0)
        return (
            jnp.concatenate((keys, keys), axis=1),
            jnp.concatenate((kv[0, slot, 2], kv[0, slot, 3]), axis=1),
        )

    groups = rows // 8

    def allowed(block):
        k_pos = y * rows + lax.broadcasted_iota(jnp.int32, (rows, rows), 0)
        q_pos = block * rows + lax.broadcasted_iota(jnp.int32, (rows, rows), 1)
        return k_pos <= q_pos

    def score(unit, keys, own=False):
        pick, block = unit
        found = [dot(one, qz[pick, block]) for one in keys]
        if own:
            found = [jnp.where(allowed(block), one, masked_score) for one in found]
        highest = None
        for one in found:
            top = jnp.max(one.reshape(groups, 8, rows), axis=0)
            highest = top if highest is None else jnp.maximum(highest, top)
        return found, highest

    def keep(ahead):
        found, highest = ahead
        for index, one in enumerate(found):
            ahead_ref[index] = one
        ahead_max[...] = highest

    def absorb(unit, vals, found, highest, own=False):
        pick, block = unit
        now = jnp.broadcast_to(jnp.max(highest, axis=0, keepdims=True), (8, rows))
        if not own:
            before = m_ref[pick, block]
            now = jnp.maximum(before, now)
            rescale = jnp.exp2(before - now)
        total = None
        parts = []
        for one in found:
            part = jnp.exp2(one.reshape(groups, 8, rows) - now[None])
            if own:
                part = jnp.where(allowed(block).reshape(groups, 8, rows), part, 0.0)
            summed = jnp.sum(part, axis=0)
            total = summed if total is None else total + summed
            parts.append(part.reshape(rows, rows).astype(BF16))
        added = dot(vals, jnp.concatenate(parts, axis=0))
        m_ref[pick, block] = now
        if own:
            l_ref[pick, block] = total
            acc_ref[pick, block] = added
        else:
            l_ref[pick, block] = l_ref[pick, block] * rescale + total
            kept = acc_ref[pick, block].reshape(head_v // 8, 8, rows) * rescale[None]
            acc_ref[pick, block] = kept.reshape(head_v, rows) + added

    def attend(blocks, slots, own=False, carried=False, then=None):
        keys, vals = zip(*[block_of(slot) for slot in slots])
        vals = jnp.concatenate(vals, axis=1)
        units = [(pick, block) for block in blocks for pick in range(2)]
        if carried:
            ahead = ([ahead_ref[index] for index in range(len(slots))], ahead_max[...])
        else:
            ahead = score(units[0], keys, own)
        for index, unit in enumerate(units):
            here = ahead
            if index + 1 < len(units):
                ahead = score(units[index + 1], keys, own)
            elif then is not None:
                next_block, next_slots = then
                keep(score((0, next_block), [block_of(slot)[0] for slot in next_slots]))
            absorb(unit, vals, *here, own)

    def attend_pair(step, part):
        low, high = (z + NZ - step) % NZ, (z + step) % NZ
        blocks = ((y + 2 * part) % NY, (y + 2 * part + 1) % NY)
        leads = (part == 0) | ((step % 2 == 1) & (step < HALF - 1))

        @pl.when(z >= NZ - step)
        def _():
            @pl.when(((z == NZ - step) | (step % 2 == 1)) & (part == 0))
            def _():
                keep(score((0, blocks[0]), [block_of(low)[0], block_of(high)[0]]))

            @pl.when(leads)
            def _():
                next_slots = ((z + NZ - step - part) % NZ, (z + step + part) % NZ)
                attend(blocks, (low, high), carried=True, then=((y + 2 - 2 * part) % NY, next_slots))

            @pl.when(jnp.logical_not(leads))
            def _():
                attend(blocks, (low, high), carried=True)

        @pl.when((z >= step) & (z < NZ - step))
        def _():
            attend(blocks, (low,))

    opposite = (z + HALF) % NZ

    def o_copy(direction, piece, slot):
        to = y_at[1] if direction == 0 else y_at[3]
        return remote(
            opart.at[slot, piece], orecv.at[piece, direction],
            o_send.at[0], o_recv.at[piece], {"sp_1": to},
        )

    def rel_copy(head, direction, slot):
        to = y_at[1] if direction == 0 else y_at[3]
        return remote(
            opart.at[slot, direction], relay.at[head, direction],
            o_send.at[0], rel_recv.at[head, direction], {"sp_1": to, "tp": 2 * x + 1},
        )

    def rel_forward(head, direction):
        to = y_at[1] if direction == 0 else y_at[3]
        return remote(
            relay.at[head, direction], orecv.at[direction, 2],
            rel_send.at[head], o_recv.at[direction], {"sp_1": to, "tp": 2 * x + head},
        )

    def st_copy(off, slot):
        return remote(
            stats.at[slot], strecv.at[off], st_send.at[0], st_recv.at[0], {"sp_1": y_at[off]}
        )

    def pack(block):
        table = []
        for pick in range(2):
            table.append(m_ref[pick, block][:1])
            table.append(jnp.sum(l_ref[pick, block], axis=0, keepdims=True))
            part = acc_ref[pick, block].astype(BF16)
            for piece in range(2):
                span = slice(piece * half_rows, (piece + 1) * half_rows)
                opart[block, piece, pick * head_v : (pick + 1) * head_v] = part[:, span]
        table.append(jnp.zeros((4, rows), F32))
        stats[block] = jnp.concatenate(table, axis=0)

    def finish_send(late):
        if late:

            @pl.when(z >= HALF)
            def _():
                attend((y_at[2], y_at[1]), (opposite,))

        pack(y_at[2])
        rel_copy(core, 0, y_at[2]).start()
        rel_copy(core, 1, y_at[2]).start()
        st_copy(2, y_at[2]).start()
        pack(y_at[1])
        o_copy(0, 0, y_at[1]).start()
        o_copy(0, 1, y_at[1]).start()
        st_copy(1, y_at[1]).start()
        if late:

            @pl.when(z >= HALF)
            def _():
                attend((y_at[3], y_at[0]), (opposite,))

        pack(y_at[3])
        o_copy(1, 0, y_at[3]).start()
        o_copy(1, 1, y_at[3]).start()
        st_copy(3, y_at[3]).start()
        pack(y_at[0])

    def finish_relay(head):
        @pl.when(core == 1)
        def _():
            for direction in range(2):
                rel_copy(head, direction, y_at[2]).wait_recv()
                rel_forward(head, direction).start()

    def finish_combine():
        all_of(strecv.at[1:NY], st_send.at[0], st_recv.at[0]).wait_recv()
        lam = lam_ref[0]
        tables = [stats[y], strecv[1], strecv[3], strecv[2]]
        coefs = []
        for pick in range(2):
            maxima = [table[2 * pick : 2 * pick + 1] for table in tables]
            sums = [table[2 * pick + 1 : 2 * pick + 2] for table in tables]
            highest = maxima[0]
            for other in maxima[1:]:
                highest = jnp.maximum(highest, other)
            shares = [jnp.exp2(one - highest) for one in maxima]
            total = shares[0] * sums[0]
            for share, one in zip(shares[1:], sums[1:]):
                total = total + share * one
            factor = (1.0 if pick == 0 else -lam) / total
            coefs.append([share * factor for share in shares])
        gain = gain_ref[...].reshape(1, head_v)
        for piece in range(2):
            all_of(orecv.at[piece], o_send.at[0], o_recv.at[piece]).wait_recv()
            span = slice(piece * half_rows, (piece + 1) * half_rows)
            mixed = None
            for pick in range(2):
                parts = [acc_ref[pick, y][:, span]]
                for source in range(3):
                    one = orecv[piece, source, pick * head_v : (pick + 1) * head_v]
                    parts.append(one.astype(F32))
                for part, coef in zip(parts, coefs[pick]):
                    term = part * coef[:, span]
                    mixed = term if mixed is None else mixed + term
            spread = lax.rsqrt(jnp.mean(mixed * mixed, axis=0, keepdims=True) + epsilon)
            nb[t, piece] = ((mixed * spread).T * gain).astype(BF16)
        nb_start()

    loads[7].wait()
    loads[8].wait()

    def ring_step(index, _):
        step, part = index // 2, index % 2

        def pass_one(chunk):
            @pl.when(step < HALF)
            def _():
                with jax.named_scope("pass_on"):
                    pass_on(step, chunk)

        pass_one(2 * part)

        @pl.when(step == 2)
        def _():
            @pl.when(part == 0)
            def _():
                with jax.named_scope("take_q"):
                    take_queries(True)

            attend(((y + 2 * part) % NY, (y + 2 * part + 1) % NY), (z,), own=True)

        pass_one(2 * part + 1)

        @pl.when(index == 4)
        def _():
            with jax.named_scope("take_more_q"):
                take_queries(False)

        @pl.when((step % 2 == 0) & (part == 0))
        def _():
            with jax.named_scope("take_given"):
                take_given(step - 1)

        with jax.named_scope("attend_pair"):
            attend_pair(step - 1, part)

        @pl.when(index == 8)
        def _():
            wo_take(0)

        @pl.when(index == 12)
        def _():
            wo_take(1)

        @pl.when(index == 16)
        def _():
            wo_take(2)

        @pl.when((z == 0) & (index == 6))
        def _():
            finish_send(False)

        @pl.when((z == 0) & (index == 15))
        def _():
            finish_relay(1)
            finish_relay(0)

        return 0

    with jax.named_scope("ring"):
        lax.fori_loop(4, 2 * HALF + 2, ring_step, 0)

    with jax.named_scope("last_wait"):

        @pl.when(z >= HALF)
        def _():
            for chunk in range(CHUNKS):
                if chunk < CHUNKS // 2:
                    up(HALF, chunk, opposite).wait_recv()
                else:
                    down(HALF, chunk, opposite).wait_recv()

    @pl.when(z > 0)
    def _():
        with jax.named_scope("finish_send"):
            finish_send(True)
        with jax.named_scope("finish_relay"):
            finish_relay(1)

    with jax.named_scope("drain_ring"):
        for chunk in range(CHUNKS):

            @pl.when(z < NZ - 1)
            def _(chunk=chunk):
                up(1, chunk, z).wait_send()

            @pl.when((z < HALF) | (z > HALF + 1) | ((z == HALF + 1) & (chunk >= CHUNKS // 2)))
            def _(chunk=chunk):
                down(1, chunk, z).wait_send()

            @pl.when(z >= 1)
            def _(chunk=chunk):
                give(0, 1, chunk, z).wait_send()

            @pl.when(z >= NZ - HALF + 1)
            def _(chunk=chunk):
                give(1, 1, chunk, z).wait_send()

        all_of(qbuf.at[0 : NY - 1], q_send.at[0], q_recv.at[0]).wait_send()

    with jax.named_scope("finish_combine"):
        finish_combine()

    @pl.when(z > 0)
    def _():
        with jax.named_scope("relay_other"):
            finish_relay(0)

    with jax.named_scope("drain_parts"):
        all_of(stats.at[0 : NY - 1], st_send.at[0], st_recv.at[0]).wait_send()
        all_of(opart.at[0:3], o_send.at[0], o_recv.at[0]).wait_send()

        @pl.when(core == 1)
        def _():
            for head in range(2):
                all_of(relay.at[head], rel_send.at[head], o_recv.at[0]).wait_send()

        wo_take_across()
        wo_drain()

    def heads_across():
        all_of(nb.at[0:4], nb_dsend.at[0], nb_drecv.at[0]).wait_recv()

    def project_out(which):
        heads = [2 * chip + which for chip in range(NX)]
        lhs = jnp.concatenate([nb[head].reshape(rows, head_v) for head in heads], axis=1)
        width = 256
        for left in range(0, out_ref.shape[1], width):
            span = slice(left, left + width)
            rhs = jnp.concatenate([wo[head, :, :, span].reshape(head_v, width) for head in heads], axis=0)
            found = dot(lhs, rhs)
            if which == 1:
                out_acc[:, span] = found
            else:
                out_ref[:, span] = (out_acc[:, span] + found).astype(BF16)

    with jax.named_scope("gather_ones"):

        @pl.when(core == 1)
        def _():
            nb_take()

        @pl.when(core == 0)
        def _():
            heads_across()

    with jax.named_scope("out_ones"):
        project_out(1)

    with jax.named_scope("gather_zeros"):

        @pl.when(core == 0)
        def _():
            nb_take()

        @pl.when(core == 1)
        def _():
            heads_across()

    with jax.named_scope("out_zeros"):
        project_out(0)

    with jax.named_scope("drain"):
        all_of(nb.at[0:3], nb_send.at[0], nb_recv.at[0]).wait_send()
        all_of(nb.at[0:4], nb_dsend.at[0], nb_drecv.at[0]).wait_send()


def shards(
    hidden_in, query_one, query_two, key_one, key_two, value_proj, lambdas, norm_gain, out_proj
):
    rows, depth = hidden_in.shape
    head_qk = query_one.shape[1]
    head_v = value_proj.shape[1]
    half = rows // 2
    heads = 2 * NX
    dma = pltpu.SemaphoreType.DMA
    scratch = [
        pltpu.VMEM((rows, depth), BF16),
        pltpu.VMEM((2, head_qk, depth), BF16),
        pltpu.VMEM((2, head_qk, depth), BF16),
        pltpu.VMEM((depth, head_v), BF16),
        pltpu.SMEM((1,), F32),
        pltpu.VMEM((head_v,), F32),
        dma((9,)),
        pltpu.VMEM((2, NZ, CHUNKS, half, head_v), BF16),
        dma((2, CHUNKS)),
        dma((2, HALF, CHUNKS)),
        dma((2, CHUNKS)),
        dma((2, HALF // 2, CHUNKS)),
        pltpu.VMEM((NY, 2 * head_qk, rows), BF16),
        pltpu.VMEM((2, NY, 4 * head_qk, rows), BF16),
        dma((1,)),
        dma((3,)),
        pltpu.VMEM((2, NY, 8, rows), F32),
        pltpu.VMEM((2, NY, 8, rows), F32),
        pltpu.VMEM((2, NY, head_v, rows), F32),
        pltpu.VMEM((2, rows, rows), F32),
        pltpu.VMEM((8, rows), F32),
        pltpu.VMEM((NY, 2, 2 * head_v, half), BF16),
        pltpu.VMEM((NY, 8, rows), F32),
        pltpu.VMEM((2, 3, 2 * head_v, half), BF16),
        pltpu.VMEM((NY, 8, rows), F32),
        pltpu.VMEM((2, 2, 2 * head_v, half), BF16),
        dma((1,)),
        dma((2,)),
        dma((2,)),
        dma((2, 2)),
        dma((1,)),
        dma((1,)),
        pltpu.VMEM((heads, 2, head_v // 2, out_proj.shape[1]), BF16),
        dma((1,)),
        dma((3,)),
        dma((1,)),
        dma((1,)),
        pltpu.VMEM((heads, 2, half, head_v), BF16),
        dma((1,)),
        dma((3,)),
        dma((1,)),
        dma((1,)),
        pltpu.VMEM((rows, out_proj.shape[1]), F32),
    ]
    return pl.pallas_call(
        kernel,
        out_shape=pltpu.VMEM((rows, out_proj.shape[1]), BF16),
        in_specs=[pl.BlockSpec(memory_space=pltpu.HBM)] * 9,
        out_specs=pl.BlockSpec(memory_space=pltpu.VMEM),
        scratch_shapes=scratch,
        compiler_params=pltpu.CompilerParams(
            collective_id=0, has_side_effects=True, vmem_limit_bytes=60 * 1024 * 1024
        ),
    )(
        hidden_in, query_one.T, query_two.T, key_one.T, key_two.T, value_proj, lambdas, norm_gain,
        out_proj.reshape(2, head_v // 2, out_proj.shape[1]),
    )


def solution(mesh):
    torus = Mesh(mesh.devices.reshape(NZ, NY, mesh.shape["tp"]), ("sp_0", "sp_1", "tp"))
    placed = (
        P(SP, None),
        P(None, "tp"),
        P(None, "tp"),
        P(None, "tp"),
        P(None, "tp"),
        P(None, "tp"),
        P("tp"),
        P(),
        P("tp", None),
    )
    return jax.shard_map(
        shards, mesh=torus, in_specs=placed, out_specs=P(SP, None), check_vma=False
    )
```

```python
import math

import jax
import jax.numpy as jnp
from jax import lax
from jax.experimental import pallas as pl
from jax.experimental.pallas import tpu as pltpu
from jax.sharding import Mesh
from jax.sharding import PartitionSpec as P

SP = ("sp_0", "sp_1")
F32 = jnp.float32
BF16 = jnp.bfloat16
MESH = pl.DeviceIdType.MESH

epsilon = 1e-06
masked_score = -1e30

NZ = 16
NY = 4
NX = 4
HALF = NZ // 2
CHUNKS = 4
FAR = 2


def kernel(
    hidden_hbm, wq1_hbm, wq2_hbm, wk1_hbm, wk2_hbm, wv_hbm, lam_hbm, gain_hbm, wo_hbm,
    out_ref,
    hid, wq, wk, wv, lam_ref, gain_ref, load_sem,
    kv, kv_send, kv_recv,
    qbuf, qz, q_send, q_recv,
    m_ref, l_ref, acc_ref, ahead_ref, ahead_max,
    opart, stats, orecv, strecv, relay, o_send, o_recv, rel_send, rel_recv, st_send, st_recv,
    wo, wo_send, wo_recv, wo_dsend, wo_drecv,
    nb, nb_send, nb_recv, nb_dsend, nb_drecv, far_send, far_recv,
    out_acc,
):
    z = lax.axis_index("sp_0")
    y = lax.axis_index("sp_1")
    t = lax.axis_index("tp")
    x = t // 2
    core = t % 2
    rows = hid.shape[0]
    head_qk = wq.shape[1]
    head_v = wv.shape[1]
    half_rows = rows // 2
    scale = 1.75 * head_qk ** (-0.5) * math.log2(math.e)

    z_up, z_down = (z + 1) % NZ, (z + NZ - 1) % NZ
    y_at = [y, (y + 1) % NY, (y + 2) % NY, (y + 3) % NY]
    x_at = [x, (x + 1) % NX, (x + 2) % NX, (x + 3) % NX]
    tp_at = [2 * xx + core for xx in x_at]
    sibling = 2 * x + (1 - core)

    loads = [
        pltpu.make_async_copy(hidden_hbm, hid, load_sem.at[0]),
        pltpu.make_async_copy(wk1_hbm, wk.at[0], load_sem.at[1]),
        pltpu.make_async_copy(wk2_hbm, wk.at[1], load_sem.at[2]),
        pltpu.make_async_copy(wv_hbm, wv, load_sem.at[3]),
        pltpu.make_async_copy(wq1_hbm, wq.at[0], load_sem.at[4]),
        pltpu.make_async_copy(wq2_hbm, wq.at[1], load_sem.at[5]),
        pltpu.make_async_copy(wo_hbm, wo.at[t], load_sem.at[6]),
        pltpu.make_async_copy(gain_hbm, gain_ref, load_sem.at[7]),
        pltpu.make_async_copy(lam_hbm, lam_ref, load_sem.at[8]),
    ]
    for load in loads[:3]:
        load.start()

    barrier = pltpu.get_barrier_semaphore()
    partners = [
        {"sp_0": z_up}, {"sp_0": z_down},
        {"sp_1": y_at[1]}, {"sp_1": y_at[2]}, {"sp_1": y_at[3]},
        {"sp_1": y_at[1], "tp": sibling}, {"sp_1": y_at[3], "tp": sibling},
        {"tp": tp_at[1]}, {"tp": tp_at[2]}, {"tp": tp_at[3]}, {"tp": sibling},
    ]
    for partner in partners:
        pl.semaphore_signal(barrier, inc=1, device_id=partner, device_id_type=MESH)
    for load in loads[3:]:
        load.start()

    def remote(src, dst, send_sem, recv_sem, device):
        return pltpu.make_async_remote_copy(
            src_ref=src, dst_ref=dst, send_sem=send_sem, recv_sem=recv_sem,
            device_id=device, device_id_type=MESH,
        )

    def dot(a, b, dims=((1,), (0,))):
        return lax.dot_general(a, b, (dims, ((), ())), preferred_element_type=F32)

    def up(step, chunk, slot):
        ref = kv.at[slot, chunk]
        return remote(
            ref, ref, kv_send.at[0, chunk], kv_recv.at[0, step - 1, chunk], {"sp_0": z_up}
        )

    def down(step, chunk, slot):
        ref = kv.at[slot, chunk]
        return remote(
            ref, ref, kv_send.at[1, chunk], kv_recv.at[1, step - 1, chunk], {"sp_0": z_down}
        )

    def start_ring(chunks):
        @pl.when(z < NZ - 1)
        def _():
            for chunk in chunks:
                up(1, chunk, z).start()

        @pl.when(z < HALF)
        def _():
            for chunk in chunks:
                down(1, chunk, z).start()

    with jax.named_scope("load_kv"):
        for load in loads[:3]:
            load.wait()
    with jax.named_scope("proj_k"):
        h = hid[...]
        k = dot(h, wk[...].reshape(2 * head_qk, wk.shape[2]), ((1,), (1,))).astype(BF16)
        kv[z, 0] = k[:half_rows]
        kv[z, 1] = k[half_rows:]
    with jax.named_scope("entry_barrier"):
        pl.semaphore_wait(barrier, len(partners))
    start_ring((0, 1))
    with jax.named_scope("proj_v"):
        loads[3].wait()
        v = dot(h, wv[...]).T.astype(BF16)
        kv[z, 2] = v[:, :half_rows]
        kv[z, 3] = v[:, half_rows:]
    start_ring((2, 3))

    with jax.named_scope("proj_q"):
        loads[4].wait()
        loads[5].wait()
        qbuf[y] = dot(wq[...].reshape(2 * head_qk, wq.shape[2]), h, ((1,), (1,))).astype(BF16)

    def q_copy(off, slot):
        return remote(
            qbuf.at[slot], qbuf.at[slot], q_send.at[0], q_recv.at[off - 1], {"sp_1": y_at[off]}
        )

    def all_of(ref, send_sem, recv_sem):
        return remote(ref, ref, send_sem, recv_sem, {"tp": sibling})

    for off in (3, 2, 1):
        q_copy(off, y).start()

    def gather_ops(buf, send, recv, dsend, drecv):
        def piece_of(direction, order):
            return direction if order != 1 else 1 - direction

        def hop(direction, order, slot):
            ref = buf.at[slot, piece_of(direction, order)]
            to = tp_at[1] if direction == 0 else tp_at[3]
            return remote(ref, ref, send.at[0], recv.at[order], {"tp": to})

        def across(piece, slot):
            ref = buf.at[slot, piece]
            return remote(ref, ref, dsend.at[0], drecv.at[0], {"tp": sibling})

        def came(direction):
            return tp_at[3] if direction == 0 else tp_at[1]

        def start_own():
            for order in range(2):
                for direction in range(2):
                    hop(direction, order, t).start()
            for piece in range(2):
                across(piece, t).start()

        def take(order):
            all_of(buf.at[0], send.at[0], recv.at[order]).wait_recv()
            for direction in range(2):
                slot = tp_at[2] if order == 2 else came(direction)
                if order == 0:
                    hop(direction, 2, slot).start()
                across(piece_of(direction, order), slot).start()

        def take_across():
            all_of(buf.at[0:4], dsend.at[0], drecv.at[0]).wait_recv()

        def drain():
            all_of(buf.at[0:3], send.at[0], recv.at[0]).wait_send()
            all_of(buf.at[0:4], dsend.at[0], drecv.at[0]).wait_send()

        return start_own, take, take_across, drain

    wo_start, wo_take, wo_take_across, wo_drain = gather_ops(wo, wo_send, wo_recv, wo_dsend, wo_drecv)

    def nb_copy(off, slot):
        ref = nb.at[slot]
        return remote(ref, ref, nb_send.at[0], nb_recv.at[off - 1], {"tp": tp_at[off]})

    def nb_across(kind, slot):
        ref = nb.at[slot]
        return remote(ref, ref, nb_dsend.at[0], nb_drecv.at[kind], {"tp": sibling})

    def nb_far(slot):
        ref = nb.at[slot]
        return remote(ref, ref, far_send.at[0], far_recv.at[0], {"tp": 2 * x_at[2] + 1})

    def nb_start():
        nb_across(0, t).start()

        @pl.when(core == 1)
        def _():
            nb_copy(2, t).start()

        for off in (1, 3):
            nb_copy(off, t).start()

    def nb_take(offs):
        for off in offs:
            slot = tp_at[(NX - off) % NX]
            nb_copy(off, slot).wait_recv()
            nb_across(1, slot).start()

    loads[6].wait()
    wo_start()

    def pass_on(step, chunk):
        low, high = (z + NZ - step) % NZ, (z + step) % NZ

        @pl.when(z >= step)
        def _():
            up(step, chunk, low).wait_recv()

            @pl.when((z < NZ - 1) & ((step < HALF - 1) | (chunk < CHUNKS // 2)))
            def _():
                up(step, chunk, low).wait_send()
                up(step + 1, chunk, low).start()

        @pl.when(high < HALF)
        def _():
            down(step, chunk, high).wait_recv()

            @pl.when((step < HALF - 1) | (chunk >= CHUNKS // 2))
            def _():
                @pl.when((z + step - 1) % NZ < HALF)
                def _():
                    down(step, chunk, high).wait_send()

                down(step + 1, chunk, high).start()

    with jax.named_scope("first_pass"):
        for chunk in range(CHUNKS):
            pass_on(1, chunk)

    def split_queries(block):
        q = qbuf[block].astype(F32) * scale
        high = q.astype(BF16)
        low = (q - high.astype(F32)).astype(BF16)
        nothing = jnp.zeros((head_qk, rows), BF16)
        qz[0, block] = jnp.concatenate((high[:head_qk], nothing, low[:head_qk], nothing), axis=0)
        qz[1, block] = jnp.concatenate((nothing, high[head_qk:], nothing, low[head_qk:]), axis=0)

    def take_queries(first):
        if first:
            q_copy(3, y_at[1]).wait_recv()
        else:
            q_copy(2, y_at[2]).wait_recv()
            q_copy(1, y_at[3]).wait_recv()
        for off in (0, 1) if first else (2, 3):
            split_queries(y_at[off])


    def block_of(slot):
        keys = jnp.concatenate((kv[slot, 0], kv[slot, 1]), axis=0)
        return (
            jnp.concatenate((keys, keys), axis=1),
            jnp.concatenate((kv[slot, 2], kv[slot, 3]), axis=1),
        )

    groups = rows // 8

    def allowed(block):
        k_pos = y * rows + lax.broadcasted_iota(jnp.int32, (rows, rows), 0)
        q_pos = block * rows + lax.broadcasted_iota(jnp.int32, (rows, rows), 1)
        return k_pos <= q_pos

    def score(unit, keys, own=False):
        pick, block = unit
        found = [dot(one, qz[pick, block]) for one in keys]
        if own:
            found = [jnp.where(allowed(block), one, masked_score) for one in found]
        highest = None
        for one in found:
            top = jnp.max(one.reshape(groups, 8, rows), axis=0)
            highest = top if highest is None else jnp.maximum(highest, top)
        return found, highest

    def keep(ahead):
        found, highest = ahead
        for index, one in enumerate(found):
            ahead_ref[index] = one
        ahead_max[...] = highest

    def absorb(unit, vals, found, highest, own=False):
        pick, block = unit
        now = jnp.broadcast_to(jnp.max(highest, axis=0, keepdims=True), (8, rows))
        if not own:
            before = m_ref[pick, block]
            now = jnp.maximum(before, now)
            rescale = jnp.exp2(before - now)
        total = None
        parts = []
        for one in found:
            part = jnp.exp2(one.reshape(groups, 8, rows) - now[None])
            if own:
                part = jnp.where(allowed(block).reshape(groups, 8, rows), part, 0.0)
            summed = jnp.sum(part, axis=0)
            total = summed if total is None else total + summed
            parts.append(part.reshape(rows, rows).astype(BF16))
        added = dot(vals, jnp.concatenate(parts, axis=0))
        m_ref[pick, block] = now
        if own:
            l_ref[pick, block] = total
            acc_ref[pick, block] = added
        else:
            l_ref[pick, block] = l_ref[pick, block] * rescale + total
            kept = acc_ref[pick, block].reshape(head_v // 8, 8, rows) * rescale[None]
            acc_ref[pick, block] = kept.reshape(head_v, rows) + added

    def attend(blocks, slots, own=False, carried=False, then=None):
        keys, vals = zip(*[block_of(slot) for slot in slots])
        vals = jnp.concatenate(vals, axis=1)
        units = [(pick, block) for block in blocks for pick in range(2)]
        if carried:
            ahead = ([ahead_ref[index] for index in range(len(slots))], ahead_max[...])
        else:
            ahead = score(units[0], keys, own)
        for index, unit in enumerate(units):
            here = ahead
            if index + 1 < len(units):
                ahead = score(units[index + 1], keys, own)
            elif then is not None:
                next_block, next_slots = then
                keep(score((0, next_block), [block_of(slot)[0] for slot in next_slots]))
            absorb(unit, vals, *here, own)

    def attend_pair(step, part):
        low, high = (z + NZ - step) % NZ, (z + step) % NZ
        blocks = ((y + 2 * part) % NY, (y + 2 * part + 1) % NY)
        final = (step == HALF - 1) & (part == 1)

        @pl.when(z >= NZ - step)
        def _():
            @pl.when((z == NZ - step) & (part == 0))
            def _():
                keep(score((0, blocks[0]), [block_of(low)[0], block_of(high)[0]]))

            @pl.when(jnp.logical_not(final))
            def _():
                next_slots = ((z + NZ - step - part) % NZ, (z + step + part) % NZ)
                attend(blocks, (low, high), carried=True, then=((y + 2 - 2 * part) % NY, next_slots))

            @pl.when(final)
            def _():
                attend(blocks, (low, high), carried=True)

        @pl.when((z >= step) & (z < NZ - step))
        def _():
            attend(blocks, (low,))

    opposite = (z + HALF) % NZ

    def o_copy(direction, piece, slot):
        to = y_at[1] if direction == 0 else y_at[3]
        return remote(
            opart.at[slot, piece], orecv.at[piece, direction],
            o_send.at[0], o_recv.at[piece], {"sp_1": to},
        )

    def rel_copy(head, direction, slot):
        to = y_at[1] if direction == 0 else y_at[3]
        return remote(
            opart.at[slot, direction], relay.at[head, direction],
            o_send.at[0], rel_recv.at[head, direction], {"sp_1": to, "tp": 2 * x + 1},
        )

    def rel_forward(head, direction):
        to = y_at[1] if direction == 0 else y_at[3]
        return remote(
            relay.at[head, direction], orecv.at[direction, 2],
            rel_send.at[head], o_recv.at[direction], {"sp_1": to, "tp": 2 * x + head},
        )

    def st_copy(off, slot):
        return remote(
            stats.at[slot], strecv.at[off], st_send.at[0], st_recv.at[0], {"sp_1": y_at[off]}
        )

    def pack(block):
        table = []
        for pick in range(2):
            table.append(m_ref[pick, block][:1])
            table.append(jnp.sum(l_ref[pick, block], axis=0, keepdims=True))
            part = acc_ref[pick, block].astype(BF16)
            for piece in range(2):
                span = slice(piece * half_rows, (piece + 1) * half_rows)
                opart[block, piece, pick * head_v : (pick + 1) * head_v] = part[:, span]
        table.append(jnp.zeros((4, rows), F32))
        stats[block] = jnp.concatenate(table, axis=0)

    def finish_send(late):
        def absorb_last(blocks):
            if late:

                @pl.when(z >= HALF)
                def _():
                    attend(blocks, (opposite,))

        absorb_last((y_at[2],))
        pack(y_at[2])
        rel_copy(core, 0, y_at[2]).start()
        rel_copy(core, 1, y_at[2]).start()
        st_copy(2, y_at[2]).start()
        absorb_last((y_at[1], y_at[3]))
        pack(y_at[1])
        o_copy(0, 0, y_at[1]).start()
        o_copy(0, 1, y_at[1]).start()
        st_copy(1, y_at[1]).start()
        pack(y_at[3])
        o_copy(1, 0, y_at[3]).start()
        o_copy(1, 1, y_at[3]).start()
        st_copy(3, y_at[3]).start()
        absorb_last((y_at[0],))
        pack(y_at[0])

    def finish_relay(head):
        @pl.when(core == 1)
        def _():
            for direction in range(2):
                rel_copy(head, direction, y_at[2]).wait_recv()
                rel_forward(head, direction).start()

    def finish_combine():
        all_of(strecv.at[1:NY], st_send.at[0], st_recv.at[0]).wait_recv()
        lam = lam_ref[0]
        tables = [stats[y], strecv[1], strecv[3], strecv[2]]
        coefs = []
        for pick in range(2):
            maxima = [table[2 * pick : 2 * pick + 1] for table in tables]
            sums = [table[2 * pick + 1 : 2 * pick + 2] for table in tables]
            highest = maxima[0]
            for other in maxima[1:]:
                highest = jnp.maximum(highest, other)
            shares = [jnp.exp2(one - highest) for one in maxima]
            total = shares[0] * sums[0]
            for share, one in zip(shares[1:], sums[1:]):
                total = total + share * one
            factor = (1.0 if pick == 0 else -lam) / total
            coefs.append([share * factor for share in shares])
        gain = gain_ref[...].reshape(1, head_v)
        for piece in range(2):
            all_of(orecv.at[piece], o_send.at[0], o_recv.at[piece]).wait_recv()
            span = slice(piece * half_rows, (piece + 1) * half_rows)
            mixed = None
            for pick in range(2):
                parts = [acc_ref[pick, y][:, span]]
                for source in range(3):
                    one = orecv[piece, source, pick * head_v : (pick + 1) * head_v]
                    parts.append(one.astype(F32))
                for part, coef in zip(parts, coefs[pick]):
                    term = part * coef[:, span]
                    mixed = term if mixed is None else mixed + term
            spread = lax.rsqrt(jnp.mean(mixed * mixed, axis=0, keepdims=True) + epsilon)
            nb[t, piece] = ((mixed * spread).T * gain).astype(BF16)
        nb_start()

    loads[7].wait()
    loads[8].wait()

    def ring_step(index, _):
        step, part = index // 2, index % 2

        def pass_one(chunk):
            @pl.when(step < HALF)
            def _():
                with jax.named_scope("pass_on"):
                    pass_on(step, chunk)

        pass_one(2 * part)

        @pl.when(step == 2)
        def _():
            @pl.when(part == 0)
            def _():
                with jax.named_scope("take_q"):
                    take_queries(True)

            attend(((y + 2 * part) % NY, (y + 2 * part + 1) % NY), (z,), own=True)

        pass_one(2 * part + 1)

        @pl.when(index == 4)
        def _():
            with jax.named_scope("take_more_q"):
                take_queries(False)

        with jax.named_scope("attend_pair"):
            attend_pair(step - 1, part)

        @pl.when(index == 8)
        def _():
            wo_take(0)

        @pl.when(index == 12)
        def _():
            wo_take(1)

        @pl.when(index == 16)
        def _():
            wo_take(2)

        @pl.when((z == 0) & (index == 6))
        def _():
            finish_send(False)

        @pl.when((z == 0) & (index == 15))
        def _():
            finish_relay(1)
            finish_relay(0)

        return 0

    with jax.named_scope("ring"):
        lax.fori_loop(4, 2 * HALF + 2, ring_step, 0)

    with jax.named_scope("last_wait"):

        @pl.when(z >= HALF)
        def _():
            for chunk in range(CHUNKS):
                if chunk < CHUNKS // 2:
                    up(HALF, chunk, opposite).wait_recv()
                else:
                    down(HALF, chunk, opposite).wait_recv()

    @pl.when(z > 0)
    def _():
        with jax.named_scope("finish_send"):
            finish_send(True)
        with jax.named_scope("finish_relay"):
            finish_relay(1)

    with jax.named_scope("drain_ring"):
        for chunk in range(CHUNKS):

            @pl.when(z < NZ - 1)
            def _(chunk=chunk):
                up(1, chunk, z).wait_send()

            @pl.when((z < HALF) | (z > HALF + 1) | ((z == HALF + 1) & (chunk >= CHUNKS // 2)))
            def _(chunk=chunk):
                down(1, chunk, z).wait_send()

        all_of(qbuf.at[0 : NY - 1], q_send.at[0], q_recv.at[0]).wait_send()

    with jax.named_scope("finish_combine"):
        finish_combine()

    @pl.when(z > 0)
    def _():
        with jax.named_scope("relay_other"):
            finish_relay(0)

    with jax.named_scope("drain_parts"):
        all_of(stats.at[0 : NY - 1], st_send.at[0], st_recv.at[0]).wait_send()
        all_of(opart.at[0:3], o_send.at[0], o_recv.at[0]).wait_send()

        @pl.when(core == 1)
        def _():
            for head in range(2):
                all_of(relay.at[head], rel_send.at[head], o_recv.at[0]).wait_send()

        wo_take_across()
        wo_drain()

    def project_out(heads, first=False, last=False):
        lhs = jnp.concatenate([nb[head].reshape(rows, head_v) for head in heads], axis=1)
        width = 256
        for left in range(0, out_ref.shape[1], width):
            span = slice(left, left + width)
            rhs = jnp.concatenate([wo[head, :, :, span].reshape(head_v, width) for head in heads], axis=0)
            found = dot(lhs, rhs)
            if not first:
                found = out_acc[:, span] + found
            if last:
                out_ref[:, span] = found.astype(BF16)
            else:
                out_acc[:, span] = found

    with jax.named_scope("gather_ones"):

        @pl.when(core == 1)
        def _():
            nb_take((1, 3, 2))

        @pl.when(core == 0)
        def _():
            nb_across(0, 2 * x + 1).wait_recv()
            all_of(nb.at[0:3], nb_dsend.at[0], nb_drecv.at[1]).wait_recv()

    with jax.named_scope("out_ones"):
        project_out([1, 3, 5, 7], first=True)

    @pl.when(core == 1)
    def _():
        with jax.named_scope("far_start"):
            nb_across(0, 2 * x).wait_recv()
            nb_far(2 * x).start()
        with jax.named_scope("far_wait"):
            nb_far(2 * x_at[2]).wait_recv()
            nb_across(2, 2 * x_at[2]).start()
        with jax.named_scope("zeros_wait"):
            all_of(nb.at[0:2], nb_dsend.at[0], nb_drecv.at[1]).wait_recv()
        with jax.named_scope("out_zeros"):
            project_out([0, 2, 4, 6], last=True)
        all_of(nb.at[0:3], nb_send.at[0], nb_recv.at[0]).wait_send()
        all_of(nb.at[0:5], nb_dsend.at[0], nb_drecv.at[0]).wait_send()
        nb_far(2 * x).wait_send()

    @pl.when(core == 0)
    def _():
        with jax.named_scope("near_wait"):
            nb_take((1, 3))
        with jax.named_scope("out_near"):
            project_out([2 * x_at[0], 2 * x_at[1], 2 * x_at[3]])
        with jax.named_scope("far_wait0"):
            nb_across(2, 2 * x_at[2]).wait_recv()
        with jax.named_scope("out_far"):
            project_out([2 * x_at[2]], last=True)
        all_of(nb.at[0:2], nb_send.at[0], nb_recv.at[0]).wait_send()
        all_of(nb.at[0:3], nb_dsend.at[0], nb_drecv.at[0]).wait_send()


def shards(
    hidden_in, query_one, query_two, key_one, key_two, value_proj, lambdas, norm_gain, out_proj
):
    rows, depth = hidden_in.shape
    head_qk = query_one.shape[1]
    head_v = value_proj.shape[1]
    half = rows // 2
    heads = 2 * NX
    dma = pltpu.SemaphoreType.DMA
    scratch = [
        pltpu.VMEM((rows, depth), BF16),
        pltpu.VMEM((2, head_qk, depth), BF16),
        pltpu.VMEM((2, head_qk, depth), BF16),
        pltpu.VMEM((depth, head_v), BF16),
        pltpu.SMEM((1,), F32),
        pltpu.VMEM((head_v,), F32),
        dma((9,)),
        pltpu.VMEM((NZ, CHUNKS, half, head_v), BF16),
        dma((2, CHUNKS)),
        dma((2, HALF, CHUNKS)),
        pltpu.VMEM((NY, 2 * head_qk, rows), BF16),
        pltpu.VMEM((2, NY, 4 * head_qk, rows), BF16),
        dma((1,)),
        dma((3,)),
        pltpu.VMEM((2, NY, 8, rows), F32),
        pltpu.VMEM((2, NY, 8, rows), F32),
        pltpu.VMEM((2, NY, head_v, rows), F32),
        pltpu.VMEM((2, rows, rows), F32),
        pltpu.VMEM((8, rows), F32),
        pltpu.VMEM((NY, 2, 2 * head_v, half), BF16),
        pltpu.VMEM((NY, 8, rows), F32),
        pltpu.VMEM((2, 3, 2 * head_v, half), BF16),
        pltpu.VMEM((NY, 8, rows), F32),
        pltpu.VMEM((2, 2, 2 * head_v, half), BF16),
        dma((1,)),
        dma((2,)),
        dma((2,)),
        dma((2, 2)),
        dma((1,)),
        dma((1,)),
        pltpu.VMEM((heads, 2, head_v // 2, out_proj.shape[1]), BF16),
        dma((1,)),
        dma((3,)),
        dma((1,)),
        dma((1,)),
        pltpu.VMEM((heads, 2, half, head_v), BF16),
        dma((1,)),
        dma((3,)),
        dma((1,)),
        dma((3,)),
        dma((1,)),
        dma((1,)),
        pltpu.VMEM((rows, out_proj.shape[1]), F32),
    ]
    return pl.pallas_call(
        kernel,
        out_shape=pltpu.VMEM((rows, out_proj.shape[1]), BF16),
        in_specs=[pl.BlockSpec(memory_space=pltpu.HBM)] * 9,
        out_specs=pl.BlockSpec(memory_space=pltpu.VMEM),
        scratch_shapes=scratch,
        compiler_params=pltpu.CompilerParams(
            collective_id=0, has_side_effects=True, vmem_limit_bytes=60 * 1024 * 1024
        ),
    )(
        hidden_in, query_one.T, query_two.T, key_one.T, key_two.T, value_proj, lambdas, norm_gain,
        out_proj.reshape(2, head_v // 2, out_proj.shape[1]),
    )


def solution(mesh):
    torus = Mesh(mesh.devices.reshape(NZ, NY, mesh.shape["tp"]), ("sp_0", "sp_1", "tp"))
    placed = (
        P(SP, None),
        P(None, "tp"),
        P(None, "tp"),
        P(None, "tp"),
        P(None, "tp"),
        P(None, "tp"),
        P("tp"),
        P(),
        P("tp", None),
    )
    return jax.shard_map(
        shards, mesh=torus, in_specs=placed, out_specs=P(SP, None), check_vma=False
    )
```

```python
import math

import jax
import jax.numpy as jnp
from jax import lax
from jax.experimental import pallas as pl
from jax.experimental.pallas import tpu as pltpu
from jax.sharding import Mesh
from jax.sharding import PartitionSpec as P

SP = ("sp_0", "sp_1")
F32 = jnp.float32
BF16 = jnp.bfloat16
MESH = pl.DeviceIdType.MESH

epsilon = 1e-06
masked_score = -1e30

NZ = 16
NY = 4
NX = 4
HALF = NZ // 2
CHUNKS = 4
FAR = 2


def kernel(
    hidden_hbm, wq1_hbm, wq2_hbm, wk1_hbm, wk2_hbm, wv_hbm, lam_hbm, gain_hbm, wo_hbm,
    out_ref,
    hid, wq, wk, wv, lam_ref, gain_ref, load_sem,
    kv, kv_send, kv_recv, skip_send,
    qbuf, qz, q_send, q_recv,
    m_ref, l_ref, acc_ref, ahead_ref, ahead_max,
    opart, stats, orecv, strecv, relay, o_send, o_recv, rel_send, rel_recv, st_send, st_recv,
    wo, wo_send, wo_recv, wo_dsend, wo_drecv,
    nb, nb_send, nb_recv, nb_dsend, nb_drecv, far_send, far_recv,
    out_acc,
):
    z = lax.axis_index("sp_0")
    y = lax.axis_index("sp_1")
    t = lax.axis_index("tp")
    x = t // 2
    core = t % 2
    rows = hid.shape[0]
    head_qk = wq.shape[1]
    head_v = wv.shape[1]
    half_rows = rows // 2
    scale = 1.75 * head_qk ** (-0.5) * math.log2(math.e)

    z_up, z_down = (z + 1) % NZ, (z + NZ - 1) % NZ
    y_at = [y, (y + 1) % NY, (y + 2) % NY, (y + 3) % NY]
    x_at = [x, (x + 1) % NX, (x + 2) % NX, (x + 3) % NX]
    tp_at = [2 * xx + core for xx in x_at]
    sibling = 2 * x + (1 - core)

    loads = [
        pltpu.make_async_copy(hidden_hbm, hid, load_sem.at[0]),
        pltpu.make_async_copy(wk1_hbm, wk.at[0], load_sem.at[1]),
        pltpu.make_async_copy(wk2_hbm, wk.at[1], load_sem.at[2]),
        pltpu.make_async_copy(wv_hbm, wv, load_sem.at[3]),
        pltpu.make_async_copy(wq1_hbm, wq.at[0], load_sem.at[4]),
        pltpu.make_async_copy(wq2_hbm, wq.at[1], load_sem.at[5]),
        pltpu.make_async_copy(wo_hbm, wo.at[t], load_sem.at[6]),
        pltpu.make_async_copy(gain_hbm, gain_ref, load_sem.at[7]),
        pltpu.make_async_copy(lam_hbm, lam_ref, load_sem.at[8]),
    ]
    for load in loads[:3]:
        load.start()

    barrier = pltpu.get_barrier_semaphore()
    partners = [
        {"sp_0": z_up}, {"sp_0": z_down}, {"sp_0": (z + 2) % NZ}, {"sp_0": (z + NZ - 2) % NZ},
        {"sp_1": y_at[1]}, {"sp_1": y_at[2]}, {"sp_1": y_at[3]},
        {"sp_1": y_at[1], "tp": sibling}, {"sp_1": y_at[3], "tp": sibling},
        {"tp": tp_at[1]}, {"tp": tp_at[2]}, {"tp": tp_at[3]}, {"tp": sibling},
    ]
    for partner in partners:
        pl.semaphore_signal(barrier, inc=1, device_id=partner, device_id_type=MESH)
    for load in loads[3:]:
        load.start()

    def remote(src, dst, send_sem, recv_sem, device):
        return pltpu.make_async_remote_copy(
            src_ref=src, dst_ref=dst, send_sem=send_sem, recv_sem=recv_sem,
            device_id=device, device_id_type=MESH,
        )

    def dot(a, b, dims=((1,), (0,))):
        return lax.dot_general(a, b, (dims, ((), ())), preferred_element_type=F32)

    def up(step, chunk, slot):
        ref = kv.at[slot, chunk]
        return remote(
            ref, ref, kv_send.at[0, chunk], kv_recv.at[0, step - 1, chunk], {"sp_0": z_up}
        )

    def down(step, chunk, slot):
        ref = kv.at[slot, chunk]
        return remote(
            ref, ref, kv_send.at[1, chunk], kv_recv.at[1, step - 1, chunk], {"sp_0": z_down}
        )

    def skip(direction, chunk):
        ref = kv.at[z, chunk]
        to = (z + 2) % NZ if direction == 0 else (z + NZ - 2) % NZ
        return remote(
            ref, ref, skip_send.at[direction], kv_recv.at[direction, 1, chunk], {"sp_0": to}
        )

    def start_ring(chunks):
        @pl.when((core == 0) & (z < NZ - 2))
        def _():
            for chunk in chunks:
                skip(0, chunk).start()

        @pl.when((core == 0) & (z < HALF))
        def _():
            for chunk in chunks:
                skip(1, chunk).start()

        @pl.when(z < NZ - 1)
        def _():
            for chunk in chunks:
                up(1, chunk, z).start()

        @pl.when(z < HALF)
        def _():
            for chunk in chunks:
                down(1, chunk, z).start()

    with jax.named_scope("load_kv"):
        for load in loads[:3]:
            load.wait()
    with jax.named_scope("proj_k"):
        h = hid[...]
        k = dot(h, wk[...].reshape(2 * head_qk, wk.shape[2]), ((1,), (1,))).astype(BF16)
        kv[z, 0] = k[:half_rows]
        kv[z, 1] = k[half_rows:]
    with jax.named_scope("entry_barrier"):
        pl.semaphore_wait(barrier, len(partners))
    start_ring((0, 1))
    with jax.named_scope("proj_v"):
        loads[3].wait()
        v = dot(h, wv[...]).T.astype(BF16)
        kv[z, 2] = v[:, :half_rows]
        kv[z, 3] = v[:, half_rows:]
    start_ring((2, 3))

    with jax.named_scope("proj_q"):
        loads[4].wait()
        loads[5].wait()
        qbuf[y] = dot(wq[...].reshape(2 * head_qk, wq.shape[2]), h, ((1,), (1,))).astype(BF16)

    def q_copy(off, slot):
        return remote(
            qbuf.at[slot], qbuf.at[slot], q_send.at[0], q_recv.at[off - 1], {"sp_1": y_at[off]}
        )

    def all_of(ref, send_sem, recv_sem):
        return remote(ref, ref, send_sem, recv_sem, {"tp": sibling})

    for off in (3, 2, 1):
        q_copy(off, y).start()

    def gather_ops(buf, send, recv, dsend, drecv):
        def piece_of(direction, order):
            return direction if order != 1 else 1 - direction

        def hop(direction, order, slot):
            ref = buf.at[slot, piece_of(direction, order)]
            to = tp_at[1] if direction == 0 else tp_at[3]
            return remote(ref, ref, send.at[0], recv.at[order], {"tp": to})

        def across(piece, slot):
            ref = buf.at[slot, piece]
            return remote(ref, ref, dsend.at[0], drecv.at[0], {"tp": sibling})

        def came(direction):
            return tp_at[3] if direction == 0 else tp_at[1]

        def start_own():
            for order in range(2):
                for direction in range(2):
                    hop(direction, order, t).start()
            for piece in range(2):
                across(piece, t).start()

        def take(order):
            all_of(buf.at[0], send.at[0], recv.at[order]).wait_recv()
            for direction in range(2):
                slot = tp_at[2] if order == 2 else came(direction)
                if order == 0:
                    hop(direction, 2, slot).start()
                across(piece_of(direction, order), slot).start()

        def take_across():
            all_of(buf.at[0:4], dsend.at[0], drecv.at[0]).wait_recv()

        def drain():
            all_of(buf.at[0:3], send.at[0], recv.at[0]).wait_send()
            all_of(buf.at[0:4], dsend.at[0], drecv.at[0]).wait_send()

        return start_own, take, take_across, drain

    wo_start, wo_take, wo_take_across, wo_drain = gather_ops(wo, wo_send, wo_recv, wo_dsend, wo_drecv)

    def nb_copy(off, slot):
        ref = nb.at[slot]
        return remote(ref, ref, nb_send.at[0], nb_recv.at[off - 1], {"tp": tp_at[off]})

    def nb_across(kind, slot):
        ref = nb.at[slot]
        return remote(ref, ref, nb_dsend.at[0], nb_drecv.at[kind], {"tp": sibling})

    def nb_far(slot):
        ref = nb.at[slot]
        return remote(ref, ref, far_send.at[0], far_recv.at[0], {"tp": 2 * x_at[2] + 1})

    def nb_start():
        nb_across(0, t).start()

        @pl.when(core == 1)
        def _():
            nb_copy(2, t).start()

        for off in (1, 3):
            nb_copy(off, t).start()

    def nb_take(offs):
        for off in offs:
            slot = tp_at[(NX - off) % NX]
            nb_copy(off, slot).wait_recv()
            nb_across(1, slot).start()

    loads[6].wait()
    wo_start()

    def pass_on(step, chunk):
        low, high = (z + NZ - step) % NZ, (z + step) % NZ
        onward = (core == 1) | (step > 1)

        @pl.when(z >= step)
        def _():
            up(step, chunk, low).wait_recv()

            @pl.when(onward & (z < NZ - 1) & ((step < HALF - 1) | (chunk < CHUNKS // 2)))
            def _():
                up(step, chunk, low).wait_send()
                up(step + 1, chunk, low).start()

        @pl.when(high < HALF)
        def _():
            down(step, chunk, high).wait_recv()

            @pl.when(onward & ((step < HALF - 1) | (chunk >= CHUNKS // 2)))
            def _():
                sent = ((z + step - 1) % NZ < HALF) & ((core == 1) | (step > 2))

                @pl.when((z < HALF) | sent)
                def _():
                    down(step, chunk, high).wait_send()

                down(step + 1, chunk, high).start()

    with jax.named_scope("first_pass"):
        for chunk in range(CHUNKS):
            pass_on(1, chunk)

    def split_queries(block):
        q = qbuf[block].astype(F32) * scale
        high = q.astype(BF16)
        low = (q - high.astype(F32)).astype(BF16)
        nothing = jnp.zeros((head_qk, rows), BF16)
        qz[0, block] = jnp.concatenate((high[:head_qk], nothing, low[:head_qk], nothing), axis=0)
        qz[1, block] = jnp.concatenate((nothing, high[head_qk:], nothing, low[head_qk:]), axis=0)

    def take_queries(first):
        if first:
            q_copy(3, y_at[1]).wait_recv()
        else:
            q_copy(2, y_at[2]).wait_recv()
            q_copy(1, y_at[3]).wait_recv()
        for off in (0, 1) if first else (2, 3):
            split_queries(y_at[off])


    def block_of(slot):
        keys = jnp.concatenate((kv[slot, 0], kv[slot, 1]), axis=0)
        return (
            jnp.concatenate((keys, keys), axis=1),
            jnp.concatenate((kv[slot, 2], kv[slot, 3]), axis=1),
        )

    groups = rows // 8

    def allowed(block):
        k_pos = y * rows + lax.broadcasted_iota(jnp.int32, (rows, rows), 0)
        q_pos = block * rows + lax.broadcasted_iota(jnp.int32, (rows, rows), 1)
        return k_pos <= q_pos

    def score(unit, keys, own=False):
        pick, block = unit
        found = [dot(one, qz[pick, block]) for one in keys]
        if own:
            found = [jnp.where(allowed(block), one, masked_score) for one in found]
        highest = None
        for one in found:
            top = jnp.max(one.reshape(groups, 8, rows), axis=0)
            highest = top if highest is None else jnp.maximum(highest, top)
        return found, highest

    def keep(ahead):
        found, highest = ahead
        for index, one in enumerate(found):
            ahead_ref[index] = one
        ahead_max[...] = highest

    def absorb(unit, vals, found, highest, own=False):
        pick, block = unit
        now = jnp.broadcast_to(jnp.max(highest, axis=0, keepdims=True), (8, rows))
        if not own:
            before = m_ref[pick, block]
            now = jnp.maximum(before, now)
            rescale = jnp.exp2(before - now)
        total = None
        parts = []
        for one in found:
            part = jnp.exp2(one.reshape(groups, 8, rows) - now[None])
            if own:
                part = jnp.where(allowed(block).reshape(groups, 8, rows), part, 0.0)
            summed = jnp.sum(part, axis=0)
            total = summed if total is None else total + summed
            parts.append(part.reshape(rows, rows).astype(BF16))
        added = dot(vals, jnp.concatenate(parts, axis=0))
        m_ref[pick, block] = now
        if own:
            l_ref[pick, block] = total
            acc_ref[pick, block] = added
        else:
            l_ref[pick, block] = l_ref[pick, block] * rescale + total
            kept = acc_ref[pick, block].reshape(head_v // 8, 8, rows) * rescale[None]
            acc_ref[pick, block] = kept.reshape(head_v, rows) + added

    def attend(blocks, slots, own=False, carried=False, then=None):
        keys, vals = zip(*[block_of(slot) for slot in slots])
        vals = jnp.concatenate(vals, axis=1)
        units = [(pick, block) for block in blocks for pick in range(2)]
        if carried:
            ahead = ([ahead_ref[index] for index in range(len(slots))], ahead_max[...])
        else:
            ahead = score(units[0], keys, own)
        for index, unit in enumerate(units):
            here = ahead
            if index + 1 < len(units):
                ahead = score(units[index + 1], keys, own)
            elif then is not None:
                next_block, next_slots = then
                keep(score((0, next_block), [block_of(slot)[0] for slot in next_slots]))
            absorb(unit, vals, *here, own)

    def attend_pair(step, part):
        low, high = (z + NZ - step) % NZ, (z + step) % NZ
        blocks = ((y + 2 * part) % NY, (y + 2 * part + 1) % NY)
        final = (step == HALF - 1) & (part == 1)

        @pl.when(z >= NZ - step)
        def _():
            @pl.when((z == NZ - step) & (part == 0))
            def _():
                keep(score((0, blocks[0]), [block_of(low)[0], block_of(high)[0]]))

            @pl.when(jnp.logical_not(final))
            def _():
                next_slots = ((z + NZ - step - part) % NZ, (z + step + part) % NZ)
                attend(blocks, (low, high), carried=True, then=((y + 2 - 2 * part) % NY, next_slots))

            @pl.when(final)
            def _():
                attend(blocks, (low, high), carried=True)

        @pl.when((z >= step) & (z < NZ - step))
        def _():
            attend(blocks, (low,))

    opposite = (z + HALF) % NZ

    def o_copy(direction, piece, slot):
        to = y_at[1] if direction == 0 else y_at[3]
        return remote(
            opart.at[slot, piece], orecv.at[piece, direction],
            o_send.at[0], o_recv.at[piece], {"sp_1": to},
        )

    def rel_copy(head, direction, slot):
        to = y_at[1] if direction == 0 else y_at[3]
        return remote(
            opart.at[slot, direction], relay.at[head, direction],
            o_send.at[0], rel_recv.at[head, direction], {"sp_1": to, "tp": 2 * x + 1},
        )

    def rel_forward(head, direction):
        to = y_at[1] if direction == 0 else y_at[3]
        return remote(
            relay.at[head, direction], orecv.at[direction, 2],
            rel_send.at[head], o_recv.at[2 + direction], {"sp_1": to, "tp": 2 * x + head},
        )

    def st_copy(off, slot):
        return remote(
            stats.at[slot], strecv.at[off], st_send.at[0], st_recv.at[0], {"sp_1": y_at[off]}
        )

    def pack(block):
        table = []
        for pick in range(2):
            table.append(m_ref[pick, block][:1])
            table.append(jnp.sum(l_ref[pick, block], axis=0, keepdims=True))
            part = acc_ref[pick, block].astype(BF16)
            for piece in range(2):
                span = slice(piece * half_rows, (piece + 1) * half_rows)
                opart[block, piece, pick * head_v : (pick + 1) * head_v] = part[:, span]
        table.append(jnp.zeros((4, rows), F32))
        stats[block] = jnp.concatenate(table, axis=0)

    def finish_send(late):
        def absorb_last(blocks):
            if late:

                @pl.when(z >= HALF)
                def _():
                    attend(blocks, (opposite,))

        absorb_last((y_at[2],))
        pack(y_at[2])
        rel_copy(core, 0, y_at[2]).start()
        rel_copy(core, 1, y_at[2]).start()
        st_copy(2, y_at[2]).start()
        absorb_last((y_at[1], y_at[3]))
        pack(y_at[1])
        o_copy(0, 0, y_at[1]).start()
        o_copy(0, 1, y_at[1]).start()
        st_copy(1, y_at[1]).start()
        pack(y_at[3])
        o_copy(1, 0, y_at[3]).start()
        o_copy(1, 1, y_at[3]).start()
        st_copy(3, y_at[3]).start()
        absorb_last((y_at[0],))
        pack(y_at[0])

    def finish_relay(head):
        @pl.when(core == 1)
        def _():
            for direction in range(2):
                rel_copy(head, direction, y_at[2]).wait_recv()
                rel_forward(head, direction).start()

    def finish_combine():
        all_of(strecv.at[1:NY], st_send.at[0], st_recv.at[0]).wait_recv()
        lam = lam_ref[0]
        tables = [stats[y], strecv[1], strecv[3], strecv[2]]
        coefs = []
        for pick in range(2):
            maxima = [table[2 * pick : 2 * pick + 1] for table in tables]
            sums = [table[2 * pick + 1 : 2 * pick + 2] for table in tables]
            highest = maxima[0]
            for other in maxima[1:]:
                highest = jnp.maximum(highest, other)
            shares = [jnp.exp2(one - highest) for one in maxima]
            total = shares[0] * sums[0]
            for share, one in zip(shares[1:], sums[1:]):
                total = total + share * one
            factor = (1.0 if pick == 0 else -lam) / total
            coefs.append([share * factor for share in shares])
        gain = gain_ref[...].reshape(1, head_v)
        spans = [slice(piece * half_rows, (piece + 1) * half_rows) for piece in range(2)]

        def shares_of(part_of, index, span):
            terms = [part_of(pick).astype(F32) * coefs[pick][index][:, span] for pick in range(2)]
            return terms[0] + terms[1]

        def arrived(piece, source):
            return lambda pick: orecv[piece, source, pick * head_v : (pick + 1) * head_v]

        near = []
        for piece, span in enumerate(spans):
            all_of(orecv.at[piece, 0:2], o_send.at[0], o_recv.at[piece]).wait_recv()
            mixed = shares_of(lambda pick, span=span: acc_ref[pick, y][:, span], 0, span)
            for source in range(2):
                mixed = mixed + shares_of(arrived(piece, source), 1 + source, span)
            near.append(mixed)
        for piece, span in enumerate(spans):
            all_of(orecv.at[piece, 2], o_send.at[0], o_recv.at[2 + piece]).wait_recv()
            mixed = near[piece] + shares_of(arrived(piece, 2), 3, span)
            spread = lax.rsqrt(jnp.mean(mixed * mixed, axis=0, keepdims=True) + epsilon)
            nb[t, piece] = ((mixed * spread).T * gain).astype(BF16)
        nb_start()

    loads[7].wait()
    loads[8].wait()

    def ring_step(index, _):
        step, part = index // 2, index % 2

        def pass_one(chunk):
            @pl.when(step < HALF)
            def _():
                with jax.named_scope("pass_on"):
                    pass_on(step, chunk)

        pass_one(2 * part)

        @pl.when(step == 2)
        def _():
            @pl.when(part == 0)
            def _():
                with jax.named_scope("take_q"):
                    take_queries(True)

            attend(((y + 2 * part) % NY, (y + 2 * part + 1) % NY), (z,), own=True)

        pass_one(2 * part + 1)

        @pl.when(index == 4)
        def _():
            with jax.named_scope("take_more_q"):
                take_queries(False)

        with jax.named_scope("attend_pair"):
            attend_pair(step - 1, part)

        @pl.when(index == 8)
        def _():
            wo_take(0)

        @pl.when(index == 12)
        def _():
            wo_take(1)

        @pl.when(index == 16)
        def _():
            wo_take(2)

        @pl.when((z == 0) & (index == 6))
        def _():
            finish_send(False)

        @pl.when((z == 0) & (index == 15))
        def _():
            finish_relay(1)
            finish_relay(0)

        return 0

    with jax.named_scope("ring"):
        lax.fori_loop(4, 2 * HALF + 2, ring_step, 0)

    with jax.named_scope("last_wait"):

        @pl.when(z >= HALF)
        def _():
            for chunk in range(CHUNKS):
                if chunk < CHUNKS // 2:
                    up(HALF, chunk, opposite).wait_recv()
                else:
                    down(HALF, chunk, opposite).wait_recv()

    @pl.when(z > 0)
    def _():
        with jax.named_scope("finish_send"):
            finish_send(True)
        with jax.named_scope("finish_relay"):
            finish_relay(1)

    with jax.named_scope("drain_ring"):
        for chunk in range(CHUNKS):

            @pl.when(z < NZ - 1)
            def _(chunk=chunk):
                up(1, chunk, z).wait_send()

            @pl.when((z < HALF) | (z > HALF + 1) | ((z == HALF + 1) & (chunk >= CHUNKS // 2)))
            def _(chunk=chunk):
                down(1, chunk, z).wait_send()

        @pl.when((core == 0) & (z < NZ - 2))
        def _():
            all_of(kv.at[0], skip_send.at[0], kv_recv.at[0, 1, 0]).wait_send()

        @pl.when((core == 0) & (z < HALF))
        def _():
            all_of(kv.at[0], skip_send.at[1], kv_recv.at[1, 1, 0]).wait_send()

        all_of(qbuf.at[0 : NY - 1], q_send.at[0], q_recv.at[0]).wait_send()

    with jax.named_scope("finish_combine"):
        finish_combine()

    @pl.when(z > 0)
    def _():
        with jax.named_scope("relay_other"):
            finish_relay(0)

    with jax.named_scope("drain_parts"):
        all_of(stats.at[0 : NY - 1], st_send.at[0], st_recv.at[0]).wait_send()
        all_of(opart.at[0:3], o_send.at[0], o_recv.at[0]).wait_send()

        @pl.when(core == 1)
        def _():
            for head in range(2):
                all_of(relay.at[head], rel_send.at[head], o_recv.at[0]).wait_send()

        wo_take_across()
        wo_drain()

    def project_out(heads, first=False, last=False):
        lhs = jnp.concatenate([nb[head].reshape(rows, head_v) for head in heads], axis=1)
        width = 256
        for left in range(0, out_ref.shape[1], width):
            span = slice(left, left + width)
            rhs = jnp.concatenate([wo[head, :, :, span].reshape(head_v, width) for head in heads], axis=0)
            found = dot(lhs, rhs)
            if not first:
                found = out_acc[:, span] + found
            if last:
                out_ref[:, span] = found.astype(BF16)
            else:
                out_acc[:, span] = found

    with jax.named_scope("gather_ones"):

        @pl.when(core == 1)
        def _():
            nb_take((1, 3, 2))

        @pl.when(core == 0)
        def _():
            nb_across(0, 2 * x + 1).wait_recv()
            all_of(nb.at[0:3], nb_dsend.at[0], nb_drecv.at[1]).wait_recv()

    with jax.named_scope("out_ones"):
        project_out([1, 3, 5, 7], first=True)

    @pl.when(core == 1)
    def _():
        with jax.named_scope("far_start"):
            nb_across(0, 2 * x).wait_recv()
            nb_far(2 * x).start()
        with jax.named_scope("far_wait"):
            nb_far(2 * x_at[2]).wait_recv()
            nb_across(2, 2 * x_at[2]).start()
        with jax.named_scope("zeros_wait"):
            all_of(nb.at[0:2], nb_dsend.at[0], nb_drecv.at[1]).wait_recv()
        with jax.named_scope("out_zeros"):
            project_out([0, 2, 4, 6], last=True)
        all_of(nb.at[0:3], nb_send.at[0], nb_recv.at[0]).wait_send()
        all_of(nb.at[0:5], nb_dsend.at[0], nb_drecv.at[0]).wait_send()
        nb_far(2 * x).wait_send()

    @pl.when(core == 0)
    def _():
        with jax.named_scope("near_wait"):
            nb_take((1, 3))
        with jax.named_scope("out_near"):
            project_out([2 * x_at[0], 2 * x_at[1], 2 * x_at[3]])
        with jax.named_scope("far_wait0"):
            nb_across(2, 2 * x_at[2]).wait_recv()
        with jax.named_scope("out_far"):
            project_out([2 * x_at[2]], last=True)
        all_of(nb.at[0:2], nb_send.at[0], nb_recv.at[0]).wait_send()
        all_of(nb.at[0:3], nb_dsend.at[0], nb_drecv.at[0]).wait_send()


def shards(
    hidden_in, query_one, query_two, key_one, key_two, value_proj, lambdas, norm_gain, out_proj
):
    rows, depth = hidden_in.shape
    head_qk = query_one.shape[1]
    head_v = value_proj.shape[1]
    half = rows // 2
    heads = 2 * NX
    dma = pltpu.SemaphoreType.DMA
    scratch = [
        pltpu.VMEM((rows, depth), BF16),
        pltpu.VMEM((2, head_qk, depth), BF16),
        pltpu.VMEM((2, head_qk, depth), BF16),
        pltpu.VMEM((depth, head_v), BF16),
        pltpu.SMEM((1,), F32),
        pltpu.VMEM((head_v,), F32),
        dma((9,)),
        pltpu.VMEM((NZ, CHUNKS, half, head_v), BF16),
        dma((2, CHUNKS)),
        dma((2, HALF, CHUNKS)),
        dma((2,)),
        pltpu.VMEM((NY, 2 * head_qk, rows), BF16),
        pltpu.VMEM((2, NY, 4 * head_qk, rows), BF16),
        dma((1,)),
        dma((3,)),
        pltpu.VMEM((2, NY, 8, rows), F32),
        pltpu.VMEM((2, NY, 8, rows), F32),
        pltpu.VMEM((2, NY, head_v, rows), F32),
        pltpu.VMEM((2, rows, rows), F32),
        pltpu.VMEM((8, rows), F32),
        pltpu.VMEM((NY, 2, 2 * head_v, half), BF16),
        pltpu.VMEM((NY, 8, rows), F32),
        pltpu.VMEM((2, 3, 2 * head_v, half), BF16),
        pltpu.VMEM((NY, 8, rows), F32),
        pltpu.VMEM((2, 2, 2 * head_v, half), BF16),
        dma((1,)),
        dma((4,)),
        dma((2,)),
        dma((2, 2)),
        dma((1,)),
        dma((1,)),
        pltpu.VMEM((heads, 2, head_v // 2, out_proj.shape[1]), BF16),
        dma((1,)),
        dma((3,)),
        dma((1,)),
        dma((1,)),
        pltpu.VMEM((heads, 2, half, head_v), BF16),
        dma((1,)),
        dma((3,)),
        dma((1,)),
        dma((3,)),
        dma((1,)),
        dma((1,)),
        pltpu.VMEM((rows, out_proj.shape[1]), F32),
    ]
    return pl.pallas_call(
        kernel,
        out_shape=pltpu.VMEM((rows, out_proj.shape[1]), BF16),
        in_specs=[pl.BlockSpec(memory_space=pltpu.HBM)] * 9,
        out_specs=pl.BlockSpec(memory_space=pltpu.VMEM),
        scratch_shapes=scratch,
        compiler_params=pltpu.CompilerParams(
            collective_id=0, has_side_effects=True, vmem_limit_bytes=60 * 1024 * 1024
        ),
    )(
        hidden_in, query_one.T, query_two.T, key_one.T, key_two.T, value_proj, lambdas, norm_gain,
        out_proj.reshape(2, head_v // 2, out_proj.shape[1]),
    )


def solution(mesh):
    torus = Mesh(mesh.devices.reshape(NZ, NY, mesh.shape["tp"]), ("sp_0", "sp_1", "tp"))
    placed = (
        P(SP, None),
        P(None, "tp"),
        P(None, "tp"),
        P(None, "tp"),
        P(None, "tp"),
        P(None, "tp"),
        P("tp"),
        P(),
        P("tp", None),
    )
    return jax.shard_map(
        shards, mesh=torus, in_specs=placed, out_specs=P(SP, None), check_vma=False
    )
```

```python
import math

import jax
import jax.numpy as jnp
from jax import lax
from jax.experimental import pallas as pl
from jax.experimental.pallas import tpu as pltpu
from jax.sharding import Mesh
from jax.sharding import PartitionSpec as P

SP = ("sp_0", "sp_1")
F32 = jnp.float32
BF16 = jnp.bfloat16
MESH = pl.DeviceIdType.MESH

epsilon = 1e-06
masked_score = -1e30

NZ = 16
NY = 4
NX = 4
HALF = NZ // 2
CHUNKS = 4
FAR = 2


def kernel(
    hidden_hbm, wq1_hbm, wq2_hbm, wk1_hbm, wk2_hbm, wv_hbm, lam_hbm, gain_hbm, wo_hbm,
    out_ref,
    hid, wq, wk, wv, lam_ref, gain_ref, load_sem,
    kv, kv_send, kv_recv,
    qbuf, qz, q_send, q_recv,
    m_ref, l_ref, acc_ref, ahead_ref, ahead_max,
    opart, stats, orecv, strecv, o_send, o_recv, st_send, st_recv,
    wo, wo_send, wo_recv, wo_dsend, wo_drecv,
    nb, nb_send, nb_recv, nb_dsend, nb_drecv, far_send, far_recv,
    out_acc,
):
    z = lax.axis_index("sp_0")
    y = lax.axis_index("sp_1")
    t = lax.axis_index("tp")
    x = t // 2
    core = t % 2
    rows = hid.shape[0]
    head_qk = wq.shape[1]
    head_v = wv.shape[1]
    half_rows = rows // 2
    scale = 1.75 * head_qk ** (-0.5) * math.log2(math.e)

    z_up, z_down = (z + 1) % NZ, (z + NZ - 1) % NZ
    y_at = [y, (y + 1) % NY, (y + 2) % NY, (y + 3) % NY]
    x_at = [x, (x + 1) % NX, (x + 2) % NX, (x + 3) % NX]
    tp_at = [2 * xx + core for xx in x_at]
    sibling = 2 * x + (1 - core)

    loads = [
        pltpu.make_async_copy(hidden_hbm, hid, load_sem.at[0]),
        pltpu.make_async_copy(wk1_hbm, wk.at[0], load_sem.at[1]),
        pltpu.make_async_copy(wk2_hbm, wk.at[1], load_sem.at[2]),
        pltpu.make_async_copy(wv_hbm, wv, load_sem.at[3]),
        pltpu.make_async_copy(wq1_hbm, wq.at[0], load_sem.at[4]),
        pltpu.make_async_copy(wq2_hbm, wq.at[1], load_sem.at[5]),
        pltpu.make_async_copy(wo_hbm, wo.at[t], load_sem.at[6]),
        pltpu.make_async_copy(gain_hbm, gain_ref, load_sem.at[7]),
        pltpu.make_async_copy(lam_hbm, lam_ref, load_sem.at[8]),
    ]
    for load in loads[:3]:
        load.start()

    barrier = pltpu.get_barrier_semaphore()
    partners = [
        {"sp_0": z_up}, {"sp_0": z_down},
        {"sp_1": y_at[1]}, {"sp_1": y_at[2]}, {"sp_1": y_at[3]},
        {"tp": tp_at[1]}, {"tp": tp_at[2]}, {"tp": tp_at[3]}, {"tp": sibling},
    ]
    for partner in partners:
        pl.semaphore_signal(barrier, inc=1, device_id=partner, device_id_type=MESH)
    for load in loads[3:]:
        load.start()

    def remote(src, dst, send_sem, recv_sem, device):
        return pltpu.make_async_remote_copy(
            src_ref=src, dst_ref=dst, send_sem=send_sem, recv_sem=recv_sem,
            device_id=device, device_id_type=MESH,
        )

    def dot(a, b, dims=((1,), (0,))):
        return lax.dot_general(a, b, (dims, ((), ())), preferred_element_type=F32)

    def up(step, chunk, slot):
        ref = kv.at[slot, chunk]
        return remote(
            ref, ref, kv_send.at[0, chunk], kv_recv.at[0, step - 1, chunk], {"sp_0": z_up}
        )

    def down(step, chunk, slot):
        ref = kv.at[slot, chunk]
        return remote(
            ref, ref, kv_send.at[1, chunk], kv_recv.at[1, step - 1, chunk], {"sp_0": z_down}
        )

    def start_ring(chunks):
        @pl.when(z < NZ - 1)
        def _():
            for chunk in chunks:
                up(1, chunk, z).start()

        @pl.when(z < HALF)
        def _():
            for chunk in chunks:
                down(1, chunk, z).start()

    with jax.named_scope("load_kv"):
        for load in loads[:3]:
            load.wait()
    with jax.named_scope("proj_k"):
        h = hid[...]
        k = dot(h, wk[...].reshape(2 * head_qk, wk.shape[2]), ((1,), (1,))).astype(BF16)
        kv[z, 0] = k[:half_rows]
        kv[z, 1] = k[half_rows:]
    with jax.named_scope("entry_barrier"):
        pl.semaphore_wait(barrier, len(partners))
    start_ring((0, 1))
    with jax.named_scope("proj_v"):
        loads[3].wait()
        v = dot(h, wv[...]).T.astype(BF16)
        kv[z, 2] = v[:, :half_rows]
        kv[z, 3] = v[:, half_rows:]
    start_ring((2, 3))

    with jax.named_scope("proj_q"):
        loads[4].wait()
        loads[5].wait()
        qbuf[y] = dot(wq[...].reshape(2 * head_qk, wq.shape[2]), h, ((1,), (1,))).astype(BF16)

    def q_copy(off, slot):
        return remote(
            qbuf.at[slot], qbuf.at[slot], q_send.at[0], q_recv.at[off - 1], {"sp_1": y_at[off]}
        )

    def all_of(ref, send_sem, recv_sem):
        return remote(ref, ref, send_sem, recv_sem, {"tp": sibling})

    for off in (3, 2, 1):
        q_copy(off, y).start()

    def gather_ops(buf, send, recv, dsend, drecv):
        def piece_of(direction, order):
            return direction if order != 1 else 1 - direction

        def hop(direction, order, slot):
            ref = buf.at[slot, piece_of(direction, order)]
            to = tp_at[1] if direction == 0 else tp_at[3]
            return remote(ref, ref, send.at[0], recv.at[order], {"tp": to})

        def across(piece, slot):
            ref = buf.at[slot, piece]
            return remote(ref, ref, dsend.at[0], drecv.at[0], {"tp": sibling})

        def came(direction):
            return tp_at[3] if direction == 0 else tp_at[1]

        def start_own():
            for order in range(2):
                for direction in range(2):
                    hop(direction, order, t).start()
            for piece in range(2):
                across(piece, t).start()

        def take(order):
            all_of(buf.at[0], send.at[0], recv.at[order]).wait_recv()
            for direction in range(2):
                slot = tp_at[2] if order == 2 else came(direction)
                if order == 0:
                    hop(direction, 2, slot).start()
                across(piece_of(direction, order), slot).start()

        def take_across():
            all_of(buf.at[0:4], dsend.at[0], drecv.at[0]).wait_recv()

        def drain():
            all_of(buf.at[0:3], send.at[0], recv.at[0]).wait_send()
            all_of(buf.at[0:4], dsend.at[0], drecv.at[0]).wait_send()

        return start_own, take, take_across, drain

    wo_start, wo_take, wo_take_across, wo_drain = gather_ops(wo, wo_send, wo_recv, wo_dsend, wo_drecv)

    def nb_copy(off, slot):
        ref = nb.at[slot]
        return remote(ref, ref, nb_send.at[0], nb_recv.at[off - 1], {"tp": tp_at[off]})

    def nb_across(kind, slot):
        ref = nb.at[slot]
        return remote(ref, ref, nb_dsend.at[0], nb_drecv.at[kind], {"tp": sibling})

    def nb_far(slot):
        ref = nb.at[slot]
        return remote(ref, ref, far_send.at[0], far_recv.at[0], {"tp": 2 * x_at[2] + 1})

    def nb_start():
        nb_across(0, t).start()

        @pl.when(core == 1)
        def _():
            nb_copy(2, t).start()

        for off in (1, 3):
            nb_copy(off, t).start()

    def nb_take(offs):
        for off in offs:
            slot = tp_at[(NX - off) % NX]
            nb_copy(off, slot).wait_recv()
            nb_across(1, slot).start()

    loads[6].wait()
    wo_start()

    def pass_on(step, chunk):
        low, high = (z + NZ - step) % NZ, (z + step) % NZ

        @pl.when(z >= step)
        def _():
            up(step, chunk, low).wait_recv()

            @pl.when((z < NZ - 1) & ((step < HALF - 1) | (chunk < CHUNKS // 2)))
            def _():
                up(step, chunk, low).wait_send()
                up(step + 1, chunk, low).start()

        @pl.when(high < HALF)
        def _():
            down(step, chunk, high).wait_recv()

            @pl.when((step < HALF - 1) | (chunk >= CHUNKS // 2))
            def _():
                @pl.when((z + step - 1) % NZ < HALF)
                def _():
                    down(step, chunk, high).wait_send()

                down(step + 1, chunk, high).start()

    with jax.named_scope("first_pass"):
        for chunk in range(CHUNKS):
            pass_on(1, chunk)

    def split_queries(block):
        q = qbuf[block].astype(F32) * scale
        high = q.astype(BF16)
        low = (q - high.astype(F32)).astype(BF16)
        nothing = jnp.zeros((head_qk, rows), BF16)
        qz[0, block] = jnp.concatenate((high[:head_qk], nothing, low[:head_qk], nothing), axis=0)
        qz[1, block] = jnp.concatenate((nothing, high[head_qk:], nothing, low[head_qk:]), axis=0)

    def take_queries(first):
        if first:
            q_copy(3, y_at[1]).wait_recv()
        else:
            q_copy(2, y_at[2]).wait_recv()
            q_copy(1, y_at[3]).wait_recv()
        for off in (0, 1) if first else (2, 3):
            split_queries(y_at[off])


    def block_of(slot):
        keys = jnp.concatenate((kv[slot, 0], kv[slot, 1]), axis=0)
        return (
            jnp.concatenate((keys, keys), axis=1),
            jnp.concatenate((kv[slot, 2], kv[slot, 3]), axis=1),
        )

    groups = rows // 8

    def allowed(block):
        k_pos = y * rows + lax.broadcasted_iota(jnp.int32, (rows, rows), 0)
        q_pos = block * rows + lax.broadcasted_iota(jnp.int32, (rows, rows), 1)
        return k_pos <= q_pos

    def score(unit, keys, own=False):
        pick, block = unit
        found = [dot(one, qz[pick, block]) for one in keys]
        if own:
            found = [jnp.where(allowed(block), one, masked_score) for one in found]
        highest = None
        for one in found:
            top = jnp.max(one.reshape(groups, 8, rows), axis=0)
            highest = top if highest is None else jnp.maximum(highest, top)
        return found, highest

    def keep(ahead):
        found, highest = ahead
        for index, one in enumerate(found):
            ahead_ref[index] = one
        ahead_max[...] = highest

    def absorb(unit, vals, found, highest, own=False):
        pick, block = unit
        now = jnp.broadcast_to(jnp.max(highest, axis=0, keepdims=True), (8, rows))
        if not own:
            before = m_ref[pick, block]
            now = jnp.maximum(before, now)
            rescale = jnp.exp2(before - now)
        total = None
        parts = []
        for one in found:
            part = jnp.exp2(one.reshape(groups, 8, rows) - now[None])
            if own:
                part = jnp.where(allowed(block).reshape(groups, 8, rows), part, 0.0)
            summed = jnp.sum(part, axis=0)
            total = summed if total is None else total + summed
            parts.append(part.reshape(rows, rows).astype(BF16))
        added = dot(vals, jnp.concatenate(parts, axis=0))
        m_ref[pick, block] = now
        if own:
            l_ref[pick, block] = total
            acc_ref[pick, block] = added
        else:
            l_ref[pick, block] = l_ref[pick, block] * rescale + total
            kept = acc_ref[pick, block].reshape(head_v // 8, 8, rows) * rescale[None]
            acc_ref[pick, block] = kept.reshape(head_v, rows) + added

    def attend(blocks, slots, own=False, carried=False, then=None):
        keys, vals = zip(*[block_of(slot) for slot in slots])
        vals = jnp.concatenate(vals, axis=1)
        units = [(pick, block) for block in blocks for pick in range(2)]
        if carried:
            ahead = ([ahead_ref[index] for index in range(len(slots))], ahead_max[...])
        else:
            ahead = score(units[0], keys, own)
        for index, unit in enumerate(units):
            here = ahead
            if index + 1 < len(units):
                ahead = score(units[index + 1], keys, own)
            elif then is not None:
                next_block, next_slots = then
                keep(score((0, next_block), [block_of(slot)[0] for slot in next_slots]))
            absorb(unit, vals, *here, own)

    def attend_pair(step, part):
        low, high = (z + NZ - step) % NZ, (z + step) % NZ
        blocks = ((y + 2 * part) % NY, (y + 2 * part + 1) % NY)
        final = (step == HALF - 1) & (part == 1)

        @pl.when(z >= NZ - step)
        def _():
            @pl.when((z == NZ - step) & (part == 0))
            def _():
                keep(score((0, blocks[0]), [block_of(low)[0], block_of(high)[0]]))

            @pl.when(jnp.logical_not(final))
            def _():
                next_slots = ((z + NZ - step - part) % NZ, (z + step + part) % NZ)
                attend(blocks, (low, high), carried=True, then=((y + 2 - 2 * part) % NY, next_slots))

            @pl.when(final)
            def _():
                attend(blocks, (low, high), carried=True)

        @pl.when((z >= step) & (z < NZ - step))
        def _():
            attend(blocks, (low,))

    opposite = (z + HALF) % NZ

    def o_copy(direction, piece, slot):
        to = y_at[1] if direction == 0 else y_at[3]
        return remote(
            opart.at[slot, piece], orecv.at[piece, direction],
            o_send.at[0], o_recv.at[piece], {"sp_1": to},
        )

    def far_copy(piece, slot):
        return remote(
            opart.at[slot, piece], orecv.at[piece, 2],
            o_send.at[0], o_recv.at[2 + piece], {"sp_1": y_at[2]},
        )

    def st_copy(off, slot):
        return remote(
            stats.at[slot], strecv.at[off], st_send.at[0], st_recv.at[0], {"sp_1": y_at[off]}
        )

    def pack(block):
        table = []
        for pick in range(2):
            table.append(m_ref[pick, block][:1])
            table.append(jnp.sum(l_ref[pick, block], axis=0, keepdims=True))
            part = acc_ref[pick, block].astype(BF16)
            for piece in range(2):
                span = slice(piece * half_rows, (piece + 1) * half_rows)
                opart[block, piece, pick * head_v : (pick + 1) * head_v] = part[:, span]
        table.append(jnp.zeros((4, rows), F32))
        stats[block] = jnp.concatenate(table, axis=0)

    def finish_send(late):
        def absorb_last(blocks):
            if late:

                @pl.when(z >= HALF)
                def _():
                    attend(blocks, (opposite,))

        absorb_last((y_at[2],))
        pack(y_at[2])
        far_copy(0, y_at[2]).start()
        far_copy(1, y_at[2]).start()
        st_copy(2, y_at[2]).start()
        absorb_last((y_at[1], y_at[3]))
        pack(y_at[1])
        o_copy(0, 0, y_at[1]).start()
        o_copy(0, 1, y_at[1]).start()
        st_copy(1, y_at[1]).start()
        pack(y_at[3])
        o_copy(1, 0, y_at[3]).start()
        o_copy(1, 1, y_at[3]).start()
        st_copy(3, y_at[3]).start()
        absorb_last((y_at[0],))
        pack(y_at[0])

    def finish_combine():
        all_of(strecv.at[1:NY], st_send.at[0], st_recv.at[0]).wait_recv()
        lam = lam_ref[0]
        tables = [stats[y], strecv[1], strecv[3], strecv[2]]
        coefs = []
        for pick in range(2):
            maxima = [table[2 * pick : 2 * pick + 1] for table in tables]
            sums = [table[2 * pick + 1 : 2 * pick + 2] for table in tables]
            highest = maxima[0]
            for other in maxima[1:]:
                highest = jnp.maximum(highest, other)
            shares = [jnp.exp2(one - highest) for one in maxima]
            total = shares[0] * sums[0]
            for share, one in zip(shares[1:], sums[1:]):
                total = total + share * one
            factor = (1.0 if pick == 0 else -lam) / total
            coefs.append([share * factor for share in shares])
        gain = gain_ref[...].reshape(1, head_v)
        spans = [slice(piece * half_rows, (piece + 1) * half_rows) for piece in range(2)]

        def shares_of(part_of, index, span):
            terms = [part_of(pick).astype(F32) * coefs[pick][index][:, span] for pick in range(2)]
            return terms[0] + terms[1]

        def arrived(piece, source):
            return lambda pick: orecv[piece, source, pick * head_v : (pick + 1) * head_v]

        near = []
        for piece, span in enumerate(spans):
            all_of(orecv.at[piece, 0:2], o_send.at[0], o_recv.at[piece]).wait_recv()
            mixed = shares_of(lambda pick, span=span: acc_ref[pick, y][:, span], 0, span)
            for source in range(2):
                mixed = mixed + shares_of(arrived(piece, source), 1 + source, span)
            near.append(mixed)
        for piece, span in enumerate(spans):
            all_of(orecv.at[piece, 2], o_send.at[0], o_recv.at[2 + piece]).wait_recv()
            mixed = near[piece] + shares_of(arrived(piece, 2), 3, span)
            spread = lax.rsqrt(jnp.mean(mixed * mixed, axis=0, keepdims=True) + epsilon)
            nb[t, piece] = ((mixed * spread).T * gain).astype(BF16)
        nb_start()

    loads[7].wait()
    loads[8].wait()

    def ring_step(index, _):
        step, part = index // 2, index % 2

        def pass_one(chunk):
            @pl.when(step < HALF)
            def _():
                with jax.named_scope("pass_on"):
                    pass_on(step, chunk)

        pass_one(2 * part)

        @pl.when(step == 2)
        def _():
            @pl.when(part == 0)
            def _():
                with jax.named_scope("take_q"):
                    take_queries(True)

            attend(((y + 2 * part) % NY, (y + 2 * part + 1) % NY), (z,), own=True)

        pass_one(2 * part + 1)

        @pl.when(index == 4)
        def _():
            with jax.named_scope("take_more_q"):
                take_queries(False)

        with jax.named_scope("attend_pair"):
            attend_pair(step - 1, part)

        @pl.when(index == 8)
        def _():
            wo_take(0)

        @pl.when(index == 12)
        def _():
            wo_take(1)

        @pl.when(index == 16)
        def _():
            wo_take(2)

        @pl.when((z == 0) & (index == 6))
        def _():
            finish_send(False)

        return 0

    with jax.named_scope("ring"):
        lax.fori_loop(4, 2 * HALF + 2, ring_step, 0)

    with jax.named_scope("last_wait"):

        @pl.when(z >= HALF)
        def _():
            for chunk in range(CHUNKS):
                if chunk < CHUNKS // 2:
                    up(HALF, chunk, opposite).wait_recv()
                else:
                    down(HALF, chunk, opposite).wait_recv()

    @pl.when(z > 0)
    def _():
        with jax.named_scope("finish_send"):
            finish_send(True)

    with jax.named_scope("drain_ring"):
        for chunk in range(CHUNKS):

            @pl.when(z < NZ - 1)
            def _(chunk=chunk):
                up(1, chunk, z).wait_send()

            @pl.when((z < HALF) | (z > HALF + 1) | ((z == HALF + 1) & (chunk >= CHUNKS // 2)))
            def _(chunk=chunk):
                down(1, chunk, z).wait_send()

        all_of(qbuf.at[0 : NY - 1], q_send.at[0], q_recv.at[0]).wait_send()

    with jax.named_scope("finish_combine"):
        finish_combine()

    with jax.named_scope("drain_parts"):
        all_of(stats.at[0 : NY - 1], st_send.at[0], st_recv.at[0]).wait_send()
        all_of(opart.at[0:3], o_send.at[0], o_recv.at[0]).wait_send()

        wo_take_across()
        wo_drain()

    def project_out(heads, first=False, last=False):
        lhs = jnp.concatenate([nb[head].reshape(rows, head_v) for head in heads], axis=1)
        width = 256
        for left in range(0, out_ref.shape[1], width):
            span = slice(left, left + width)
            rhs = jnp.concatenate([wo[head, :, :, span].reshape(head_v, width) for head in heads], axis=0)
            found = dot(lhs, rhs)
            if not first:
                found = out_acc[:, span] + found
            if last:
                out_ref[:, span] = found.astype(BF16)
            else:
                out_acc[:, span] = found

    with jax.named_scope("gather_ones"):

        @pl.when(core == 1)
        def _():
            nb_take((1, 3, 2))

        @pl.when(core == 0)
        def _():
            nb_across(0, 2 * x + 1).wait_recv()
            all_of(nb.at[0:3], nb_dsend.at[0], nb_drecv.at[1]).wait_recv()

    with jax.named_scope("out_ones"):
        project_out([1, 3, 5, 7], first=True)

    @pl.when(core == 1)
    def _():
        with jax.named_scope("far_start"):
            nb_across(0, 2 * x).wait_recv()
            nb_far(2 * x).start()
        with jax.named_scope("far_wait"):
            nb_far(2 * x_at[2]).wait_recv()
            nb_across(2, 2 * x_at[2]).start()
        with jax.named_scope("zeros_wait"):
            all_of(nb.at[0:2], nb_dsend.at[0], nb_drecv.at[1]).wait_recv()
        with jax.named_scope("out_zeros"):
            project_out([0, 2, 4, 6], last=True)
        all_of(nb.at[0:3], nb_send.at[0], nb_recv.at[0]).wait_send()
        all_of(nb.at[0:5], nb_dsend.at[0], nb_drecv.at[0]).wait_send()
        nb_far(2 * x).wait_send()

    @pl.when(core == 0)
    def _():
        with jax.named_scope("near_wait"):
            nb_take((1, 3))
        with jax.named_scope("out_near"):
            project_out([2 * x_at[0], 2 * x_at[1], 2 * x_at[3]])
        with jax.named_scope("far_wait0"):
            nb_across(2, 2 * x_at[2]).wait_recv()
        with jax.named_scope("out_far"):
            project_out([2 * x_at[2]], last=True)
        all_of(nb.at[0:2], nb_send.at[0], nb_recv.at[0]).wait_send()
        all_of(nb.at[0:3], nb_dsend.at[0], nb_drecv.at[0]).wait_send()


def shards(
    hidden_in, query_one, query_two, key_one, key_two, value_proj, lambdas, norm_gain, out_proj
):
    rows, depth = hidden_in.shape
    head_qk = query_one.shape[1]
    head_v = value_proj.shape[1]
    half = rows // 2
    heads = 2 * NX
    dma = pltpu.SemaphoreType.DMA
    scratch = [
        pltpu.VMEM((rows, depth), BF16),
        pltpu.VMEM((2, head_qk, depth), BF16),
        pltpu.VMEM((2, head_qk, depth), BF16),
        pltpu.VMEM((depth, head_v), BF16),
        pltpu.SMEM((1,), F32),
        pltpu.VMEM((head_v,), F32),
        dma((9,)),
        pltpu.VMEM((NZ, CHUNKS, half, head_v), BF16),
        dma((2, CHUNKS)),
        dma((2, HALF, CHUNKS)),
        pltpu.VMEM((NY, 2 * head_qk, rows), BF16),
        pltpu.VMEM((2, NY, 4 * head_qk, rows), BF16),
        dma((1,)),
        dma((3,)),
        pltpu.VMEM((2, NY, 8, rows), F32),
        pltpu.VMEM((2, NY, 8, rows), F32),
        pltpu.VMEM((2, NY, head_v, rows), F32),
        pltpu.VMEM((2, rows, rows), F32),
        pltpu.VMEM((8, rows), F32),
        pltpu.VMEM((NY, 2, 2 * head_v, half), BF16),
        pltpu.VMEM((NY, 8, rows), F32),
        pltpu.VMEM((2, 3, 2 * head_v, half), BF16),
        pltpu.VMEM((NY, 8, rows), F32),
        dma((1,)),
        dma((4,)),
        dma((1,)),
        dma((1,)),
        pltpu.VMEM((heads, 2, head_v // 2, out_proj.shape[1]), BF16),
        dma((1,)),
        dma((3,)),
        dma((1,)),
        dma((1,)),
        pltpu.VMEM((heads, 2, half, head_v), BF16),
        dma((1,)),
        dma((3,)),
        dma((1,)),
        dma((3,)),
        dma((1,)),
        dma((1,)),
        pltpu.VMEM((rows, out_proj.shape[1]), F32),
    ]
    return pl.pallas_call(
        kernel,
        out_shape=pltpu.VMEM((rows, out_proj.shape[1]), BF16),
        in_specs=[pl.BlockSpec(memory_space=pltpu.HBM)] * 9,
        out_specs=pl.BlockSpec(memory_space=pltpu.VMEM),
        scratch_shapes=scratch,
        compiler_params=pltpu.CompilerParams(
            collective_id=0, has_side_effects=True, vmem_limit_bytes=60 * 1024 * 1024
        ),
    )(
        hidden_in, query_one.T, query_two.T, key_one.T, key_two.T, value_proj, lambdas, norm_gain,
        out_proj.reshape(2, head_v // 2, out_proj.shape[1]),
    )


def solution(mesh):
    torus = Mesh(mesh.devices.reshape(NZ, NY, mesh.shape["tp"]), ("sp_0", "sp_1", "tp"))
    placed = (
        P(SP, None),
        P(None, "tp"),
        P(None, "tp"),
        P(None, "tp"),
        P(None, "tp"),
        P(None, "tp"),
        P("tp"),
        P(),
        P("tp", None),
    )
    return jax.shard_map(
        shards, mesh=torus, in_specs=placed, out_specs=P(SP, None), check_vma=False
    )
```

```python
import math

import jax
import jax.numpy as jnp
from jax import lax
from jax.experimental import pallas as pl
from jax.experimental.pallas import tpu as pltpu
from jax.sharding import Mesh
from jax.sharding import PartitionSpec as P

SP = ("sp_0", "sp_1")
F32 = jnp.float32
BF16 = jnp.bfloat16
MESH = pl.DeviceIdType.MESH

epsilon = 1e-06
masked_score = -1e30

NZ = 16
NY = 4
NX = 4
HALF = NZ // 2
CHUNKS = 4
FAR = 2


def kernel(
    hidden_hbm, wq1_hbm, wq2_hbm, wk1_hbm, wk2_hbm, wv_hbm, lam_hbm, gain_hbm, wo_hbm,
    out_ref,
    hid, wq, wk, wv, lam_ref, gain_ref, load_sem,
    kv, kv_send, kv_recv,
    qbuf, qz, q_send, q_recv,
    m_ref, l_ref, acc_ref, ahead_ref, ahead_max,
    opart, stats, orecv, strecv, o_send, o_recv, st_send, st_recv,
    wo, wo_send, wo_recv, wo_dsend, wo_drecv,
    nb, nb_send, nb_recv, nb_dsend, nb_drecv, far_send, far_recv,
    out_acc,
):
    z = lax.axis_index("sp_0")
    y = lax.axis_index("sp_1")
    t = lax.axis_index("tp")
    x = t // 2
    core = t % 2
    rows = hid.shape[0]
    head_qk = wq.shape[1]
    head_v = wv.shape[1]
    half_rows = rows // 2
    scale = 1.75 * head_qk ** (-0.5) * math.log2(math.e)

    z_up, z_down = (z + 1) % NZ, (z + NZ - 1) % NZ
    y_at = [y, (y + 1) % NY, (y + 2) % NY, (y + 3) % NY]
    x_at = [x, (x + 1) % NX, (x + 2) % NX, (x + 3) % NX]
    tp_at = [2 * xx + core for xx in x_at]
    sibling = 2 * x + (1 - core)

    loads = [
        pltpu.make_async_copy(hidden_hbm, hid, load_sem.at[0]),
        pltpu.make_async_copy(wk1_hbm, wk.at[0], load_sem.at[1]),
        pltpu.make_async_copy(wk2_hbm, wk.at[1], load_sem.at[2]),
        pltpu.make_async_copy(wv_hbm, wv, load_sem.at[3]),
        pltpu.make_async_copy(wq1_hbm, wq.at[0], load_sem.at[4]),
        pltpu.make_async_copy(wq2_hbm, wq.at[1], load_sem.at[5]),
        pltpu.make_async_copy(wo_hbm, wo.at[t], load_sem.at[6]),
        pltpu.make_async_copy(gain_hbm, gain_ref, load_sem.at[7]),
        pltpu.make_async_copy(lam_hbm, lam_ref, load_sem.at[8]),
    ]
    for load in loads[:3]:
        load.start()

    barrier = pltpu.get_barrier_semaphore()
    partners = [
        {"sp_0": z_up}, {"sp_0": z_down},
        {"sp_1": y_at[1]}, {"sp_1": y_at[2]}, {"sp_1": y_at[3]},
        {"tp": tp_at[1]}, {"tp": tp_at[2]}, {"tp": tp_at[3]}, {"tp": sibling},
    ]
    for partner in partners:
        pl.semaphore_signal(barrier, inc=1, device_id=partner, device_id_type=MESH)
    for load in loads[3:]:
        load.start()

    def remote(src, dst, send_sem, recv_sem, device):
        return pltpu.make_async_remote_copy(
            src_ref=src, dst_ref=dst, send_sem=send_sem, recv_sem=recv_sem,
            device_id=device, device_id_type=MESH,
        )

    def dot(a, b, dims=((1,), (0,))):
        return lax.dot_general(a, b, (dims, ((), ())), preferred_element_type=F32)

    def up(step, chunk, slot):
        ref = kv.at[slot, chunk]
        return remote(
            ref, ref, kv_send.at[0, chunk], kv_recv.at[0, step - 1, chunk], {"sp_0": z_up}
        )

    def down(step, chunk, slot):
        ref = kv.at[slot, chunk]
        return remote(
            ref, ref, kv_send.at[1, chunk], kv_recv.at[1, step - 1, chunk], {"sp_0": z_down}
        )

    def start_ring(chunks):
        @pl.when(z < NZ - 1)
        def _():
            for chunk in chunks:
                up(1, chunk, z).start()

        @pl.when(z < HALF)
        def _():
            for chunk in chunks:
                down(1, chunk, z).start()

    with jax.named_scope("load_kv"):
        for load in loads[:3]:
            load.wait()
    with jax.named_scope("proj_k"):
        h = hid[...]
        k = dot(h, wk[...].reshape(2 * head_qk, wk.shape[2]), ((1,), (1,))).astype(BF16)
        kv[z, 0] = k[:half_rows]
        kv[z, 1] = k[half_rows:]
    with jax.named_scope("entry_barrier"):
        pl.semaphore_wait(barrier, len(partners))
    start_ring((0, 1))
    with jax.named_scope("proj_v"):
        loads[3].wait()
        v = dot(h, wv[...]).T.astype(BF16)
        kv[z, 2] = v[:, :half_rows]
        kv[z, 3] = v[:, half_rows:]
    start_ring((2, 3))

    with jax.named_scope("proj_q"):
        loads[4].wait()
        loads[5].wait()
        qbuf[y] = dot(wq[...].reshape(2 * head_qk, wq.shape[2]), h, ((1,), (1,))).astype(BF16)

    def q_copy(off, slot):
        return remote(
            qbuf.at[slot], qbuf.at[slot], q_send.at[0], q_recv.at[off - 1], {"sp_1": y_at[off]}
        )

    def all_of(ref, send_sem, recv_sem):
        return remote(ref, ref, send_sem, recv_sem, {"tp": sibling})

    for off in (3, 2, 1):
        q_copy(off, y).start()

    def gather_ops(buf, send, recv, dsend, drecv):
        def piece_of(direction, order):
            return direction if order != 1 else 1 - direction

        def hop(direction, order, slot):
            ref = buf.at[slot, piece_of(direction, order)]
            to = tp_at[1] if direction == 0 else tp_at[3]
            return remote(ref, ref, send.at[0], recv.at[order], {"tp": to})

        def across(piece, slot):
            ref = buf.at[slot, piece]
            return remote(ref, ref, dsend.at[0], drecv.at[0], {"tp": sibling})

        def came(direction):
            return tp_at[3] if direction == 0 else tp_at[1]

        def start_own():
            for order in range(2):
                for direction in range(2):
                    hop(direction, order, t).start()
            for piece in range(2):
                across(piece, t).start()

        def take(order):
            all_of(buf.at[0], send.at[0], recv.at[order]).wait_recv()
            for direction in range(2):
                slot = tp_at[2] if order == 2 else came(direction)
                if order == 0:
                    hop(direction, 2, slot).start()
                across(piece_of(direction, order), slot).start()

        def take_across():
            all_of(buf.at[0:4], dsend.at[0], drecv.at[0]).wait_recv()

        def drain():
            all_of(buf.at[0:3], send.at[0], recv.at[0]).wait_send()
            all_of(buf.at[0:4], dsend.at[0], drecv.at[0]).wait_send()

        return start_own, take, take_across, drain

    wo_start, wo_take, wo_take_across, wo_drain = gather_ops(wo, wo_send, wo_recv, wo_dsend, wo_drecv)

    def nb_copy(off, slot):
        ref = nb.at[slot]
        return remote(ref, ref, nb_send.at[0], nb_recv.at[off - 1], {"tp": tp_at[off]})

    def nb_across(kind, slot):
        ref = nb.at[slot]
        return remote(ref, ref, nb_dsend.at[0], nb_drecv.at[kind], {"tp": sibling})

    def nb_far(slot):
        ref = nb.at[slot]
        return remote(ref, ref, far_send.at[0], far_recv.at[0], {"tp": 2 * x_at[2] + 1})

    def nb_start():
        nb_across(0, t).start()

        @pl.when(core == 1)
        def _():
            nb_copy(2, t).start()

        for off in (1, 3):
            nb_copy(off, t).start()

    def nb_take(offs):
        for off in offs:
            slot = tp_at[(NX - off) % NX]
            nb_copy(off, slot).wait_recv()
            nb_across(1, slot).start()

    loads[6].wait()
    wo_start()

    def pass_on(step, chunk):
        low, high = (z + NZ - step) % NZ, (z + step) % NZ

        @pl.when(z >= step)
        def _():
            up(step, chunk, low).wait_recv()

            @pl.when((z < NZ - 1) & ((step < HALF - 1) | (chunk < CHUNKS // 2)))
            def _():
                up(step, chunk, low).wait_send()
                up(step + 1, chunk, low).start()

        @pl.when(high < HALF)
        def _():
            down(step, chunk, high).wait_recv()

            @pl.when((step < HALF - 1) | (chunk >= CHUNKS // 2))
            def _():
                @pl.when((z + step - 1) % NZ < HALF)
                def _():
                    down(step, chunk, high).wait_send()

                down(step + 1, chunk, high).start()

    with jax.named_scope("first_pass"):
        for chunk in range(CHUNKS):
            pass_on(1, chunk)

    def split_queries(block):
        q = qbuf[block].astype(F32) * scale
        high = q.astype(BF16)
        low = (q - high.astype(F32)).astype(BF16)
        nothing = jnp.zeros((head_qk, rows), BF16)
        qz[0, block] = jnp.concatenate((high[:head_qk], nothing, low[:head_qk], nothing), axis=0)
        qz[1, block] = jnp.concatenate((nothing, high[head_qk:], nothing, low[head_qk:]), axis=0)

    def take_queries(first):
        if first:
            q_copy(3, y_at[1]).wait_recv()
        else:
            q_copy(2, y_at[2]).wait_recv()
            q_copy(1, y_at[3]).wait_recv()
        for off in (0, 1) if first else (2, 3):
            split_queries(y_at[off])


    def block_of(slot):
        keys = jnp.concatenate((kv[slot, 0], kv[slot, 1]), axis=0)
        return (
            jnp.concatenate((keys, keys), axis=1),
            jnp.concatenate((kv[slot, 2], kv[slot, 3]), axis=1),
        )

    groups = rows // 8

    def allowed(block):
        k_pos = y * rows + lax.broadcasted_iota(jnp.int32, (rows, rows), 0)
        q_pos = block * rows + lax.broadcasted_iota(jnp.int32, (rows, rows), 1)
        return k_pos <= q_pos

    def score(unit, keys, own=False):
        pick, block = unit
        found = [dot(one, qz[pick, block]) for one in keys]
        if own:
            found = [jnp.where(allowed(block), one, masked_score) for one in found]
        highest = None
        for one in found:
            top = jnp.max(one.reshape(groups, 8, rows), axis=0)
            highest = top if highest is None else jnp.maximum(highest, top)
        return found, highest

    def keep(ahead):
        found, highest = ahead
        for index, one in enumerate(found):
            ahead_ref[index] = one
        ahead_max[...] = highest

    def absorb(unit, vals, found, highest, own=False):
        pick, block = unit
        now = jnp.broadcast_to(jnp.max(highest, axis=0, keepdims=True), (8, rows))
        if not own:
            before = m_ref[pick, block]
            now = jnp.maximum(before, now)
            rescale = jnp.exp2(before - now)
        total = None
        parts = []
        for one in found:
            part = jnp.exp2(one.reshape(groups, 8, rows) - now[None])
            if own:
                part = jnp.where(allowed(block).reshape(groups, 8, rows), part, 0.0)
            summed = jnp.sum(part, axis=0)
            total = summed if total is None else total + summed
            parts.append(part.reshape(rows, rows).astype(BF16))
        added = dot(vals, jnp.concatenate(parts, axis=0))
        m_ref[pick, block] = now
        if own:
            l_ref[pick, block] = total
            acc_ref[pick, block] = added
        else:
            l_ref[pick, block] = l_ref[pick, block] * rescale + total
            kept = acc_ref[pick, block].reshape(head_v // 8, 8, rows) * rescale[None]
            acc_ref[pick, block] = kept.reshape(head_v, rows) + added

    def attend(blocks, slots, own=False, carried=False, then=None):
        keys, vals = zip(*[block_of(slot) for slot in slots])
        vals = jnp.concatenate(vals, axis=1)
        units = [(pick, block) for block in blocks for pick in range(2)]
        if carried:
            ahead = ([ahead_ref[index] for index in range(len(slots))], ahead_max[...])
        else:
            ahead = score(units[0], keys, own)
        for index, unit in enumerate(units):
            here = ahead
            if index + 1 < len(units):
                ahead = score(units[index + 1], keys, own)
            elif then is not None:
                next_block, next_slots = then
                keep(score((0, next_block), [block_of(slot)[0] for slot in next_slots]))
            absorb(unit, vals, *here, own)

    def attend_pair(step, part):
        low, high = (z + NZ - step) % NZ, (z + step) % NZ
        blocks = ((y + 2 * part) % NY, (y + 2 * part + 1) % NY)
        final = (step == HALF - 1) & (part == 1)

        @pl.when(z >= NZ - step)
        def _():
            @pl.when((z == NZ - step) & (part == 0))
            def _():
                keep(score((0, blocks[0]), [block_of(low)[0], block_of(high)[0]]))

            @pl.when(jnp.logical_not(final))
            def _():
                next_slots = ((z + NZ - step - part) % NZ, (z + step + part) % NZ)
                attend(blocks, (low, high), carried=True, then=((y + 2 - 2 * part) % NY, next_slots))

            @pl.when(final)
            def _():
                attend(blocks, (low, high), carried=True)

        @pl.when((z >= step) & (z < NZ - step))
        def _():
            attend(blocks, (low,))

    opposite = (z + HALF) % NZ

    def o_copy(direction, piece, slot):
        to = y_at[1] if direction == 0 else y_at[3]
        return remote(
            opart.at[slot, piece], orecv.at[piece, direction],
            o_send.at[0], o_recv.at[piece], {"sp_1": to},
        )

    def far_copy(piece, slot):
        return remote(
            opart.at[slot, piece], orecv.at[piece, 2],
            o_send.at[0], o_recv.at[2 + piece], {"sp_1": y_at[2]},
        )

    def st_copy(off, slot):
        return remote(
            stats.at[slot], strecv.at[off], st_send.at[0], st_recv.at[0], {"sp_1": y_at[off]}
        )

    def pack(block):
        table = []
        for pick in range(2):
            table.append(m_ref[pick, block][:1])
            table.append(jnp.sum(l_ref[pick, block], axis=0, keepdims=True))
            part = acc_ref[pick, block].astype(BF16)
            for piece in range(2):
                span = slice(piece * half_rows, (piece + 1) * half_rows)
                opart[block, piece, pick * head_v : (pick + 1) * head_v] = part[:, span]
        table.append(jnp.zeros((4, rows), F32))
        stats[block] = jnp.concatenate(table, axis=0)

    def finish_send(late):
        def absorb_last(blocks):
            if late:

                @pl.when(z >= HALF)
                def _():
                    attend(blocks, (opposite,))

        absorb_last((y_at[2],))
        pack(y_at[2])
        far_copy(0, y_at[2]).start()
        far_copy(1, y_at[2]).start()
        st_copy(2, y_at[2]).start()
        absorb_last((y_at[1], y_at[3]))
        pack(y_at[1])
        o_copy(0, 0, y_at[1]).start()
        o_copy(0, 1, y_at[1]).start()
        st_copy(1, y_at[1]).start()
        pack(y_at[3])
        o_copy(1, 0, y_at[3]).start()
        o_copy(1, 1, y_at[3]).start()
        st_copy(3, y_at[3]).start()
        absorb_last((y_at[0],))
        pack(y_at[0])

    def finish_combine():
        all_of(strecv.at[1:NY], st_send.at[0], st_recv.at[0]).wait_recv()
        lam = lam_ref[0]
        tables = [stats[y], strecv[1], strecv[3], strecv[2]]
        coefs = []
        for pick in range(2):
            maxima = [table[2 * pick : 2 * pick + 1] for table in tables]
            sums = [table[2 * pick + 1 : 2 * pick + 2] for table in tables]
            highest = maxima[0]
            for other in maxima[1:]:
                highest = jnp.maximum(highest, other)
            shares = [jnp.exp2(one - highest) for one in maxima]
            total = shares[0] * sums[0]
            for share, one in zip(shares[1:], sums[1:]):
                total = total + share * one
            factor = (1.0 if pick == 0 else -lam) / total
            coefs.append([share * factor for share in shares])
        gain = gain_ref[...].reshape(1, head_v)
        spans = [slice(piece * half_rows, (piece + 1) * half_rows) for piece in range(2)]

        def shares_of(part_of, index, span):
            terms = [part_of(pick).astype(F32) * coefs[pick][index][:, span] for pick in range(2)]
            return terms[0] + terms[1]

        def arrived(piece, source):
            return lambda pick: orecv[piece, source, pick * head_v : (pick + 1) * head_v]

        near = []
        for piece, span in enumerate(spans):
            all_of(orecv.at[piece, 0:2], o_send.at[0], o_recv.at[piece]).wait_recv()
            mixed = shares_of(lambda pick, span=span: acc_ref[pick, y][:, span], 0, span)
            for source in range(2):
                mixed = mixed + shares_of(arrived(piece, source), 1 + source, span)
            near.append(mixed)
        for piece, span in enumerate(spans):
            all_of(orecv.at[piece, 2], o_send.at[0], o_recv.at[2 + piece]).wait_recv()
            mixed = near[piece] + shares_of(arrived(piece, 2), 3, span)
            spread = lax.rsqrt(jnp.mean(mixed * mixed, axis=0, keepdims=True) + epsilon)
            nb[t, piece] = ((mixed * spread).T * gain).astype(BF16)
        nb_start()

    loads[7].wait()
    loads[8].wait()

    def ring_step(index, _):
        step, part = index // 2, index % 2

        def pass_one(chunk):
            @pl.when(step < HALF)
            def _():
                with jax.named_scope("pass_on"):
                    pass_on(step, chunk)

        pass_one(2 * part)

        @pl.when(step == 2)
        def _():
            @pl.when(part == 0)
            def _():
                with jax.named_scope("take_q"):
                    take_queries(True)

            attend(((y + 2 * part) % NY, (y + 2 * part + 1) % NY), (z,), own=True)

        pass_one(2 * part + 1)

        @pl.when(index == 4)
        def _():
            with jax.named_scope("take_more_q"):
                take_queries(False)

        with jax.named_scope("attend_pair"):
            attend_pair(step - 1, part)

        @pl.when(index == 8)
        def _():
            wo_take(0)

        @pl.when(index == 12)
        def _():
            wo_take(1)

        @pl.when(index == 16)
        def _():
            wo_take(2)

        @pl.when((z == 0) & (index == 6))
        def _():
            finish_send(False)

        return 0

    with jax.named_scope("ring"):
        lax.fori_loop(4, 2 * HALF + 2, ring_step, 0)

    with jax.named_scope("last_wait"):

        @pl.when(z >= HALF)
        def _():
            for chunk in range(CHUNKS):
                if chunk < CHUNKS // 2:
                    up(HALF, chunk, opposite).wait_recv()
                else:
                    down(HALF, chunk, opposite).wait_recv()

    @pl.when(z > 0)
    def _():
        with jax.named_scope("finish_send"):
            finish_send(True)

    with jax.named_scope("drain_ring"):
        for chunk in range(CHUNKS):

            @pl.when(z < NZ - 1)
            def _(chunk=chunk):
                up(1, chunk, z).wait_send()

            @pl.when((z < HALF) | (z > HALF + 1) | ((z == HALF + 1) & (chunk >= CHUNKS // 2)))
            def _(chunk=chunk):
                down(1, chunk, z).wait_send()

        all_of(qbuf.at[0 : NY - 1], q_send.at[0], q_recv.at[0]).wait_send()

    with jax.named_scope("finish_combine"):
        finish_combine()

    with jax.named_scope("drain_parts"):
        all_of(stats.at[0 : NY - 1], st_send.at[0], st_recv.at[0]).wait_send()
        all_of(opart.at[0:3], o_send.at[0], o_recv.at[0]).wait_send()

        wo_take_across()
        wo_drain()

    def project_out(heads, first=False, last=False):
        lhs = jnp.concatenate([nb[head].reshape(rows, head_v) for head in heads], axis=1)
        width = 256
        for left in range(0, out_ref.shape[1], width):
            span = slice(left, left + width)
            rhs = jnp.concatenate([wo[head, :, :, span].reshape(head_v, width) for head in heads], axis=0)
            found = dot(lhs, rhs)
            if not first:
                found = out_acc[:, span] + found
            if last:
                out_ref[:, span] = found.astype(BF16)
            else:
                out_acc[:, span] = found

    with jax.named_scope("gather_ones"):

        @pl.when(core == 1)
        def _():
            nb_take((1, 3, 2))

        @pl.when(core == 0)
        def _():
            nb_across(0, 2 * x + 1).wait_recv()
            all_of(nb.at[0:3], nb_dsend.at[0], nb_drecv.at[1]).wait_recv()

    with jax.named_scope("out_ones"):
        project_out([1, 3, 5, 7], first=True)

    @pl.when(core == 1)
    def _():
        with jax.named_scope("far_start"):
            nb_across(0, 2 * x).wait_recv()
            nb_far(2 * x).start()
        with jax.named_scope("far_wait"):
            nb_far(2 * x_at[2]).wait_recv()
            nb_across(2, 2 * x_at[2]).start()
        with jax.named_scope("out_far1"):
            project_out([2 * x_at[0], 2 * x_at[2]])
        with jax.named_scope("zeros_wait"):
            all_of(nb.at[0:2], nb_dsend.at[0], nb_drecv.at[1]).wait_recv()
        with jax.named_scope("out_zeros"):
            project_out([2 * x_at[1], 2 * x_at[3]], last=True)
        all_of(nb.at[0:3], nb_send.at[0], nb_recv.at[0]).wait_send()
        all_of(nb.at[0:5], nb_dsend.at[0], nb_drecv.at[0]).wait_send()
        nb_far(2 * x).wait_send()

    @pl.when(core == 0)
    def _():
        with jax.named_scope("near_wait"):
            nb_take((1, 3))
        with jax.named_scope("out_near"):
            project_out([2 * x_at[0], 2 * x_at[1], 2 * x_at[3]])
        with jax.named_scope("far_wait0"):
            nb_across(2, 2 * x_at[2]).wait_recv()
        with jax.named_scope("out_far"):
            project_out([2 * x_at[2]], last=True)
        all_of(nb.at[0:2], nb_send.at[0], nb_recv.at[0]).wait_send()
        all_of(nb.at[0:3], nb_dsend.at[0], nb_drecv.at[0]).wait_send()


def shards(
    hidden_in, query_one, query_two, key_one, key_two, value_proj, lambdas, norm_gain, out_proj
):
    rows, depth = hidden_in.shape
    head_qk = query_one.shape[1]
    head_v = value_proj.shape[1]
    half = rows // 2
    heads = 2 * NX
    dma = pltpu.SemaphoreType.DMA
    scratch = [
        pltpu.VMEM((rows, depth), BF16),
        pltpu.VMEM((2, head_qk, depth), BF16),
        pltpu.VMEM((2, head_qk, depth), BF16),
        pltpu.VMEM((depth, head_v), BF16),
        pltpu.SMEM((1,), F32),
        pltpu.VMEM((head_v,), F32),
        dma((9,)),
        pltpu.VMEM((NZ, CHUNKS, half, head_v), BF16),
        dma((2, CHUNKS)),
        dma((2, HALF, CHUNKS)),
        pltpu.VMEM((NY, 2 * head_qk, rows), BF16),
        pltpu.VMEM((2, NY, 4 * head_qk, rows), BF16),
        dma((1,)),
        dma((3,)),
        pltpu.VMEM((2, NY, 8, rows), F32),
        pltpu.VMEM((2, NY, 8, rows), F32),
        pltpu.VMEM((2, NY, head_v, rows), F32),
        pltpu.VMEM((2, rows, rows), F32),
        pltpu.VMEM((8, rows), F32),
        pltpu.VMEM((NY, 2, 2 * head_v, half), BF16),
        pltpu.VMEM((NY, 8, rows), F32),
        pltpu.VMEM((2, 3, 2 * head_v, half), BF16),
        pltpu.VMEM((NY, 8, rows), F32),
        dma((1,)),
        dma((4,)),
        dma((1,)),
        dma((1,)),
        pltpu.VMEM((heads, 2, head_v // 2, out_proj.shape[1]), BF16),
        dma((1,)),
        dma((3,)),
        dma((1,)),
        dma((1,)),
        pltpu.VMEM((heads, 2, half, head_v), BF16),
        dma((1,)),
        dma((3,)),
        dma((1,)),
        dma((3,)),
        dma((1,)),
        dma((1,)),
        pltpu.VMEM((rows, out_proj.shape[1]), F32),
    ]
    return pl.pallas_call(
        kernel,
        out_shape=pltpu.VMEM((rows, out_proj.shape[1]), BF16),
        in_specs=[pl.BlockSpec(memory_space=pltpu.HBM)] * 9,
        out_specs=pl.BlockSpec(memory_space=pltpu.VMEM),
        scratch_shapes=scratch,
        compiler_params=pltpu.CompilerParams(
            collective_id=0, has_side_effects=True, vmem_limit_bytes=60 * 1024 * 1024
        ),
    )(
        hidden_in, query_one.T, query_two.T, key_one.T, key_two.T, value_proj, lambdas, norm_gain,
        out_proj.reshape(2, head_v // 2, out_proj.shape[1]),
    )


def solution(mesh):
    torus = Mesh(mesh.devices.reshape(NZ, NY, mesh.shape["tp"]), ("sp_0", "sp_1", "tp"))
    placed = (
        P(SP, None),
        P(None, "tp"),
        P(None, "tp"),
        P(None, "tp"),
        P(None, "tp"),
        P(None, "tp"),
        P("tp"),
        P(),
        P("tp", None),
    )
    return jax.shard_map(
        shards, mesh=torus, in_specs=placed, out_specs=P(SP, None), check_vma=False
    )
```
